128 devices in a mesh: rep: 4 (over z), fs: 4 (over y), tp: 8 (over x, core).
Axes of the slice: x: 4, y: 4, z: 4, core: 2. Of those that a mesh axis runs over, the one named last changes fastest.
Arguments:
- tokens_in: bfloat16 [12288, 1024], P(('rep', 'fs', 'tp')), may hold values from -6 to 6
- out_grad: bfloat16 [12288, 1024], P(('rep', 'fs', 'tp')), may hold values from -24 to 24
- gate_weight: bfloat16 [1024, 2816], P('fs', 'tp'), may hold values from -0.1875 to 0.1875
- up_weight: bfloat16 [1024, 2816], P('fs', 'tp'), may hold values from -0.1875 to 0.1875
- down_weight: bfloat16 [2816, 1024], P('tp', 'fs'), may hold values from -0.109375 to 0.109375
Outputs:
- grad_in: bfloat16 [12288, 1024], P(('rep', 'fs', 'tp'))
- grad_gate_w: float32 [1024, 2816], P('fs', 'tp')
- grad_up_w: float32 [1024, 2816], P('fs', 'tp')
- grad_down_w: float32 [2816, 1024], P('tp', 'fs')
The draws below stay inside these ranges and needn't reach their ends.
All inputs are finite; a program needn't handle non-finite values.
Results may differ from the reference program's by a relative error of at most 0.02.
Values may be sent and summed in bfloat16 or wider, within the bound.
A program may use at most 64 MiB of HBM per device.

```python
import jax
import jax.numpy as jnp

D = 1024
FF = 2816
TOKENS = 12288


def raised(result, rng, source, target, shards_of, factor):
    def block_of(dim):
        return (jnp.arange(result.shape[dim]) // (result.shape[dim] // shards_of)).reshape((-1,) + (1,) * (result.ndim - 1 - dim))

    first = jax.random.permutation(rng, shards_of)[block_of(target)]
    other_side = (block_of(target) + shards_of // 2) % shards_of
    return jnp.where((block_of(source) == first) | (block_of(source) == other_side), factor * result, result)


def steps_of(stream_key, shape, cuts, least, largest):
    factor_of = 1.0
    for axis_at, parts in cuts:
        heights = jax.random.uniform(jax.random.fold_in(jax.random.fold_in(stream_key, 6), axis_at), (parts,), jnp.float32, least / len(cuts), largest / len(cuts))
        factor_of = factor_of * jnp.repeat(jnp.exp(heights), shape[axis_at] // parts).reshape((-1,) + (1,) * (len(shape) - 1 - axis_at))
    return factor_of


def bell_draw(stream_key, dims, scale, limit, pieces=(), dtype=jnp.bfloat16):
    entries = scale * jax.random.normal(stream_key, dims, jnp.float32)
    if pieces:
        entries = entries * steps_of(stream_key, dims, pieces, -0.22, 0.18)
    return jnp.clip(entries, -limit, limit).astype(dtype)


def noise_with(stream_key, extent, deviation, limit, split, heavy, dtype=jnp.bfloat16):
    values = deviation * jax.random.normal(stream_key, extent, jnp.float32)
    if split:
        values = values * steps_of(stream_key, extent, split, -0.22, 0.18)
    return jnp.clip(raised(values, jax.random.fold_in(stream_key, 3), *heavy), -limit, limit).astype(dtype)


def setup_inputs(seed: int = 0) -> dict:
    arg_keys = jax.random.split(jax.random.key(seed), 6)
    tokens_in = bell_draw(arg_keys[0], (TOKENS, D), 1.0, 6.0, ((0, 128),))
    out_grad = noise_with(arg_keys[1], (TOKENS, D), 1.0, 24.0, ((0, 128),), (0, 1, 128, 5.5))
    gate_weight = bell_draw(arg_keys[2], (D, FF), D ** -0.5, 0.1875, ((0, 4), (1, 8)))
    up_weight = bell_draw(arg_keys[3], (D, FF), D ** -0.5, 0.1875, ((0, 4), (1, 8)))
    down_weight = bell_draw(arg_keys[4], (FF, D), FF ** -0.5, 0.109375, ((0, 8), (1, 4)))
    return dict(tokens_in=tokens_in, out_grad=out_grad, gate_weight=gate_weight, up_weight=up_weight, down_weight=down_weight)


def reference(tokens_in, out_grad, gate_weight, up_weight, down_weight):
    gate = jnp.dot(tokens_in, gate_weight, preferred_element_type=jnp.float32).astype(jnp.bfloat16)
    up_proj = jnp.dot(tokens_in, up_weight, preferred_element_type=jnp.float32).astype(jnp.bfloat16)
    gate_wide = gate.astype(jnp.float32)
    up_wide = up_proj.astype(jnp.float32)
    sigmoid = jax.nn.sigmoid(gate_wide)
    activated = gate_wide * sigmoid
    hidden = (activated * up_wide).astype(jnp.bfloat16)
    grad_hidden = jnp.dot(out_grad, down_weight.T, preferred_element_type=jnp.float32).astype(jnp.bfloat16)
    grad_wide = grad_hidden.astype(jnp.float32)
    grad_gate = (grad_wide * up_wide * sigmoid * (1.0 + gate_wide * (1.0 - sigmoid))).astype(jnp.bfloat16)
    grad_up = (grad_wide * activated).astype(jnp.bfloat16)
    grad_in = (jnp.dot(grad_gate, gate_weight.T, preferred_element_type=jnp.float32)
               + jnp.dot(grad_up, up_weight.T, preferred_element_type=jnp.float32)).astype(jnp.bfloat16)
    factor = TOKENS ** -0.5
    grad_gate_w = jnp.dot(tokens_in.T, grad_gate, preferred_element_type=jnp.float32) * factor
    grad_up_w = jnp.dot(tokens_in.T, grad_up, preferred_element_type=jnp.float32) * factor
    grad_down_w = jnp.dot(hidden.T, out_grad, preferred_element_type=jnp.float32) * factor
    return grad_in, grad_gate_w, grad_up_w, grad_down_w
```

```python
import functools

import jax
import jax.numpy as jnp
from jax import lax
from jax.experimental import pallas as pl
from jax.experimental.pallas import tpu as pltpu
from jax.sharding import PartitionSpec as P

BF16 = jnp.bfloat16
F32 = jnp.float32
MESH = pl.DeviceIdType.MESH
COPIES = 112


def nt(left, right):
    return lax.dot_general(left, right, (((1,), (1,)), ((), ())), preferred_element_type=F32)


def tn(left, right):
    return lax.dot_general(left, right, (((0,), (0,)), ((), ())), preferred_element_type=F32)


def nn(left, right):
    return lax.dot_general(left, right, (((1,), (0,)), ((), ())), preferred_element_type=F32)


def eye(n):
    rows = lax.broadcasted_iota(jnp.int32, (n, n), 0)
    cols = lax.broadcasted_iota(jnp.int32, (n, n), 1)
    return jnp.where(rows == cols, 1.0, 0.0).astype(BF16)


def kernel(
    factor, block, width, hid,
    x_in, g_in, wg_in, wu_in, wd_in,
    gin_out, og_out, ou_out, od_out,
    X, G, WT, WG, WU, H, PW, PB, DX, DS, GX, YA1, YA2, ZB, OUTT,
    ring_bufs,
    send_sems, recv_sems, local_sems,
):
    rep = lax.axis_index("rep")
    fs = lax.axis_index("fs")
    tp = lax.axis_index("tp")
    core = lax.rem(tp, 2)
    xpos = tp // 2
    shard = width // 4

    def turn(pos, step):
        return lax.rem(pos + step, 4)

    def at_x(step):
        return {"tp": turn(xpos, step) * 2 + core}

    def at_y(step):
        return {"fs": turn(fs, step)}

    def at_z(step):
        return {"rep": turn(rep, step)}

    sibling = {"tp": tp + 1 - 2 * core}

    def lanes_of(step):
        return pl.ds(pl.multiple_of(turn(fs, step) * shard, shard), shard)

    counter = [0]
    pending = []

    def remote(src, dst, k, where):
        return pltpu.make_async_remote_copy(
            src_ref=src, dst_ref=dst, send_sem=send_sems.at[k], recv_sem=recv_sems.at[k],
            device_id=where, device_id_type=MESH,
        )

    def send(src, dst, where):
        k = counter[0]
        counter[0] += 1
        copy = remote(src, dst, k, where)
        copy.start()
        pending.append(copy)
        return k

    def arrived(k, landing):
        remote(landing, landing, k, sibling).wait_recv()

    own_lanes = lanes_of(0)
    loads = [
        pltpu.make_async_copy(x_in, X.at[pl.ds(0, block)], local_sems.at[0]),
        pltpu.make_async_copy(g_in, G.at[pl.ds(0, block)], local_sems.at[1]),
        pltpu.make_async_copy(wg_in, WG, local_sems.at[2]),
        pltpu.make_async_copy(wu_in, WU, local_sems.at[3]),
        pltpu.make_async_copy(wd_in, WT.at[pl.ds(2 * hid, hid), own_lanes], local_sems.at[4]),
    ]
    for load in loads:
        load.start()

    barrier = pltpu.get_barrier_semaphore()
    for where in (at_x(1), at_x(3), at_y(1), at_y(3), at_z(1), at_z(3), sibling):
        pl.semaphore_signal(barrier, inc=1, device_id=where, device_id_type=MESH)
    pl.semaphore_wait(barrier, 7)

    half = block // 2
    SELF, LEFT, RIGHT, OPP = 0, 1, 2, 3

    def slot(buf, s, start=0, count=block):
        return buf.at[pl.ds(s * 2 * block + start, count)]

    def token_start(buf):
        right = send(slot(buf, SELF), slot(buf, LEFT), at_x(1))
        left = send(slot(buf, SELF), slot(buf, RIGHT), at_x(3))
        across = send(slot(buf, SELF), slot(buf, SELF, block), sibling)
        return right, left, [(across, SELF)]

    def token_relay(buf, state):
        right, left, across = state
        arrived(right, slot(buf, LEFT))
        right = send(slot(buf, LEFT, 0, half), slot(buf, OPP, 0, half), at_x(1))
        arrived(left, slot(buf, RIGHT))
        left = send(slot(buf, RIGHT, half, half), slot(buf, OPP, half, half), at_x(3))
        across.append((send(slot(buf, LEFT), slot(buf, LEFT, block), sibling), LEFT))
        across.append((send(slot(buf, RIGHT), slot(buf, RIGHT, block), sibling), RIGHT))
        return right, left, across

    def token_last(buf, state):
        right, left, across = state
        arrived(right, slot(buf, OPP, 0, half))
        arrived(left, slot(buf, OPP, half, half))
        return [(send(slot(buf, OPP), slot(buf, OPP, block), sibling), OPP)]

    def token_wait(buf, across):
        for k, s in across:
            arrived(k, slot(buf, s, block))

    loads[0].wait()
    x_state = token_start(X)
    loads[1].wait()
    g_state = token_start(G)

    identity = eye(hid)
    loads[3].wait()
    WT[pl.ds(hid, hid), own_lanes] = nt(identity, WU[...]).astype(BF16)
    loads[4].wait()
    loads[2].wait()
    WT[pl.ds(0, hid), own_lanes] = nt(identity, WG[...]).astype(BF16)

    direct = 544
    part = (3 * hid - direct) // 4
    dhalf = direct // 2
    D0, D1 = pl.ds(0, dhalf), pl.ds(dhalf, dhalf)

    def quarter(step, start=0, count=part):
        return pl.ds(pl.multiple_of(direct + turn(rep, step) * part + start, 16), count)

    def w(rows, step):
        return WT.at[rows, lanes_of(step)]

    qa = send(w(quarter(0), 0), w(quarter(0), 0), at_y(1))
    qb = send(w(quarter(0), 0), w(quarter(0), 0), at_y(3))
    d0r = send(w(D0, 0), w(D0, 0), at_y(1))
    d1l = send(w(D1, 0), w(D1, 0), at_y(3))

    qh = part // 2
    arrived(qa, w(quarter(0), 3))
    qc = send(w(quarter(0, 0, qh), 3), w(quarter(0, 0, qh), 3), at_y(1))
    arrived(qb, w(quarter(0), 1))
    qd = send(w(quarter(0, qh, qh), 1), w(quarter(0, qh, qh), 1), at_y(3))
    d1r = send(w(D1, 0), w(D1, 0), at_y(1))
    d0l = send(w(D0, 0), w(D0, 0), at_y(3))

    def share(step):
        return (
            send(w(quarter(0), step), w(quarter(0), step), at_z(1)),
            send(w(quarter(0), step), w(quarter(0), step), at_z(3)),
        )

    def share_relay(state, step):
        arrived(state[0], w(quarter(3), step))
        a = send(w(quarter(3, 0, qh), step), w(quarter(3, 0, qh), step), at_z(1))
        arrived(state[1], w(quarter(1), step))
        b = send(w(quarter(1, qh, qh), step), w(quarter(1, qh, qh), step), at_z(3))
        return a, b

    def share_last(state, step):
        arrived(state[0], w(quarter(2, 0, qh), step))
        arrived(state[1], w(quarter(2, qh, qh), step))

    z3 = share(3)
    z1 = share(1)

    x_state = token_relay(X, x_state)

    arrived(d0r, w(D0, 3))
    dc = send(w(D0, 3), w(D0, 3), at_y(1))
    arrived(d1l, w(D1, 1))
    dd = send(w(D1, 1), w(D1, 1), at_y(3))

    z3 = share_relay(z3, 3)
    arrived(qc, w(quarter(0, 0, qh), 2))
    arrived(qd, w(quarter(0, qh, qh), 2))
    z2 = share(2)
    z1 = share_relay(z1, 1)

    z2 = share_relay(z2, 2)
    g_state = token_relay(G, g_state)
    x_last = token_last(X, x_state)

    arrived(d1r, w(D1, 3))
    arrived(d0l, w(D0, 1))
    for state, step in ((z3, 3), (z1, 1), (z2, 2)):
        share_last(state, step)
    arrived(dc, w(D0, 2))
    arrived(dd, w(D1, 2))

    rows = hid // 2

    def first_stage(c):
        cols = pl.ds(c * 256, 256)
        for p in range(2):
            gate = nt(WT[pl.ds(p * rows, rows), :], X[cols, :]).astype(BF16).astype(F32)
            up = nt(WT[pl.ds(hid + p * rows, rows), :], X[cols, :]).astype(BF16).astype(F32)
            grad = nt(WT[pl.ds(2 * hid + p * rows, rows), :], G[cols, :]).astype(BF16).astype(F32)
            sig = jax.nn.sigmoid(gate)
            act = gate * sig
            H[pl.ds(2 * hid + p * rows, rows), cols] = (act * up).astype(BF16)
            H[pl.ds(p * rows, rows), cols] = (
                grad * up * sig * (1.0 + gate * (1.0 - sig))
            ).astype(BF16)
            H[pl.ds(hid + p * rows, rows), cols] = (grad * act).astype(BF16)

    token_wait(X, x_state[2])
    token_wait(G, g_state[2])
    first_stage(0)
    g_last = token_last(G, g_state)
    first_stage(1)
    token_wait(X, x_last)
    token_wait(G, g_last)
    first_stage(2)

    class Ring:
        def __init__(self, piece, bufs, dest):
            self.piece, self.dest = piece, dest
            self.t0, self.t1, self.fl, self.fr = bufs
            self.h = self.t0.shape[1]

        def side(self, buf, which):
            return buf.at[:, pl.ds(which * self.h, self.h)]

        def start_far(self):
            self.a = send(self.piece(2, 0), self.t0, self.dest(1))
            self.b = send(self.piece(2, 1), self.t1, self.dest(3))

        def start_near(self):
            self.c = send(self.piece(1, 1), self.side(self.fl, 1), self.dest(1))
            self.d = send(self.piece(3, 0), self.side(self.fr, 0), self.dest(3))

        def relay(self):
            arrived(self.a, self.t0)
            self.t0[...] = (self.t0[...].astype(F32) + self.piece(1, 0)[...].astype(F32)).astype(BF16)
            self.e = send(self.t0, self.side(self.fl, 0), self.dest(1))
            arrived(self.b, self.t1)
            self.t1[...] = (self.t1[...].astype(F32) + self.piece(3, 1)[...].astype(F32)).astype(BF16)
            self.f = send(self.t1, self.side(self.fr, 1), self.dest(3))

        def finish(self, store):
            arrived(self.c, self.side(self.fl, 1))
            arrived(self.d, self.side(self.fr, 0))
            arrived(self.e, self.side(self.fl, 0))
            arrived(self.f, self.side(self.fr, 1))
            for which in range(2):
                total = (
                    self.piece(0, which)[...].astype(F32)
                    + self.side(self.fl, which)[...].astype(F32)
                    + self.side(self.fr, which)[...].astype(F32)
                )
                store(which, total.astype(BF16))

    def y_piece(buf, start, count):
        def piece(step, which):
            lane = pl.multiple_of(turn(fs, step) * shard + which * (shard // 2), 128)
            return buf.at[pl.ds(start, count), pl.ds(lane, shard // 2)]
        return piece

    def z_piece(buf, count, lanes):
        def piece(step, which):
            row = pl.multiple_of(turn(rep, step) * count, 16)
            return buf.at[pl.ds(row, count), pl.ds(which * lanes, lanes)]
        return piece

    def x_piece(step, which):
        s = {0: SELF, 1: RIGHT, 3: LEFT, 2: OPP}[step]
        return GX.at[pl.ds(s * block, block), pl.ds(which * (width // 2), width // 2)]

    A1, A2 = 384, 2 * hid - 384
    B = PB.shape[0]
    ya1 = Ring(y_piece(PW, 0, A1), ring_bufs[0:4], at_y)
    ya2 = Ring(y_piece(PW, A1, A2), ring_bufs[4:8], at_y)
    zb = Ring(z_piece(PB, B // 4, width // 2), ring_bufs[8:12], at_z)
    za1 = Ring(z_piece(YA1, A1 // 4, shard // 2), ring_bufs[12:16], at_z)
    za2 = Ring(z_piece(YA2, A2 // 4, shard // 2), ring_bufs[16:20], at_z)
    yb = Ring(y_piece(ZB, 0, B // 4), ring_bufs[20:24], at_y)
    xr = Ring(x_piece, ring_bufs[24:28], at_x)

    def to_rows(buf, start):
        def store(which, value):
            n, h = value.shape
            buf[pl.ds(start, n), pl.ds(which * h, h)] = value
        return store

    class Gather:
        def __init__(self, base, count):
            self.base, self.count = base, count

        def row(self, step):
            return pl.multiple_of(self.base + turn(rep, step) * self.count, 16)

        def region(self, step, which=None):
            if which is None:
                return OUTT.at[pl.ds(self.row(step), self.count)]
            return OUTT.at[pl.ds(self.row(step), self.count), pl.ds(which * (shard // 2), shard // 2)]

        def start(self):
            self.a = send(self.region(0), self.region(0), at_z(1))
            self.b = send(self.region(0), self.region(0), at_z(3))

        def relay(self):
            arrived(self.a, self.region(3))
            self.c = send(self.region(3, 0), self.region(3, 0), at_z(1))
            arrived(self.b, self.region(1))
            self.d = send(self.region(1, 1), self.region(1, 1), at_z(3))

        def finish(self):
            arrived(self.c, self.region(2, 0))
            arrived(self.d, self.region(2, 1))

    ga1, ga2, gb = Gather(0, A1 // 4), Gather(A1, A2 // 4), Gather(2 * hid, B // 4)

    def weight_piece(step, start, count):
        lanes = lanes_of(step)
        PW[pl.ds(start, count), lanes] = (
            factor * nn(H[pl.ds(start, count), :], X[:, lanes])
        ).astype(BF16)

    def input_piece(c):
        DX[pl.ds(c * 256, 256), :] = tn(
            H[pl.ds(0, 2 * hid), pl.ds(c * 256, 256)], WT[pl.ds(0, 2 * hid), :]
        ).astype(BF16)

    def across(s):
        landing = DS.at[pl.ds(s * block, block)]
        return send(slot(DX, s, block), landing, sibling)

    def across_add(k, s):
        arrived(k, DS.at[pl.ds(s * block, block)])
        GX[pl.ds(s * block, block), :] = (
            DX[pl.ds(s * 2 * block, block), :].astype(F32)
            + DS[pl.ds(s * block, block), :].astype(F32)
        ).astype(BF16)

    weight_piece(2, 0, A1)
    ya1.start_far()
    PB[pl.ds(hid, B - hid), :] = jnp.zeros((B - hid, width), BF16)
    for n in range(4):
        PB[pl.ds(0, hid), pl.ds(n * 256, 256)] = (
            factor * nn(H[pl.ds(2 * hid, hid), :], G[:, pl.ds(n * 256, 256)])
        ).astype(BF16)
    zb.start_far()
    zb.start_near()
    weight_piece(1, 0, A1)
    weight_piece(3, 0, A1)
    ya1.start_near()
    input_piece(2)
    opp = across(OPP)
    for step in (2, 1, 3, 0):
        weight_piece(step, A1, A2)
    ya1.relay()
    ya2.start_far()
    ya2.start_near()
    zb.relay()
    weight_piece(0, 0, A1)
    across_add(opp, OPP)
    xr.start_far()
    input_piece(1)
    near = across(LEFT), across(RIGHT)
    input_piece(0)
    mine = across(SELF)
    across_add(near[0], LEFT)
    across_add(near[1], RIGHT)
    xr.start_near()
    ya1.finish(to_rows(YA1, 0))
    za1.start_far()
    za1.start_near()

    def zb_store(which, value):
        ZB[:, pl.ds(which * (width // 2), width // 2)] = value

    zb.finish(zb_store)
    ya2.relay()
    yb.start_far()
    yb.start_near()
    xr.relay()
    across_add(mine, SELF)
    za1.relay()
    za1.finish(to_rows(OUTT, ga1.row(0)))
    ga1.start()
    yb.relay()
    ya2.finish(to_rows(YA2, 0))
    za2.start_far()
    za2.start_near()
    yb.finish(to_rows(OUTT, gb.row(0)))
    gb.start()
    ga1.relay()
    za2.relay()

    def gin_store(which, value):
        gin_out[:, pl.ds(which * (width // 2), width // 2)] = value

    xr.finish(gin_store)
    za2.finish(to_rows(OUTT, ga2.row(0)))
    ga2.start()
    gb.relay()
    ga1.finish()
    turned = eye(shard)
    gb.finish()
    od_out[...] = OUTT[pl.ds(2 * hid, hid), :].astype(F32)
    ga2.relay()
    og_out[...] = nt(turned, OUTT[pl.ds(0, hid), :])
    ga2.finish()
    ou_out[...] = nt(turned, OUTT[pl.ds(hid, hid), :])

    for copy in pending:
        copy.wait_send()


def body(tokens_in, out_grad, gate_weight, up_weight, down_weight):
    block, width = tokens_in.shape
    shard, hid = gate_weight.shape
    devices = lax.axis_size("rep") * lax.axis_size("fs") * lax.axis_size("tp")
    factor = (block * devices) ** (-0.5)
    tokens = block * 8
    A1, A2, B = 384, 2 * hid - 384, 384

    def ring(count, lanes):
        return [
            pltpu.VMEM((count, lanes // 2), BF16),
            pltpu.VMEM((count, lanes // 2), BF16),
            pltpu.VMEM((count, lanes), BF16),
            pltpu.VMEM((count, lanes), BF16),
        ]

    rings = (
        ring(A1, shard) + ring(A2, shard) + ring(B // 4, width)
        + ring(A1 // 4, shard) + ring(A2 // 4, shard) + ring(B // 4, shard)
        + ring(block, width)
    )
    return pl.pallas_call(
        functools.partial(kernel, factor, block, width, hid),
        out_shape=(
            jax.ShapeDtypeStruct((block, width), BF16),
            jax.ShapeDtypeStruct((shard, hid), F32),
            jax.ShapeDtypeStruct((shard, hid), F32),
            jax.ShapeDtypeStruct((hid, shard), F32),
        ),
        in_specs=[pl.BlockSpec(memory_space=pl.ANY)] * 5,
        out_specs=[pl.BlockSpec(memory_space=pltpu.VMEM)] * 4,
        scratch_shapes=[
            pltpu.VMEM((tokens, width), BF16),
            pltpu.VMEM((tokens, width), BF16),
            pltpu.VMEM((3 * hid, width), BF16),
            pltpu.VMEM((shard, hid), BF16),
            pltpu.VMEM((shard, hid), BF16),
            pltpu.VMEM((3 * hid, tokens), BF16),
            pltpu.VMEM((2 * hid, width), BF16),
            pltpu.VMEM((B, width), BF16),
            pltpu.VMEM((tokens, width), BF16),
            pltpu.VMEM((tokens // 2, width), BF16),
            pltpu.VMEM((tokens // 2, width), BF16),
            pltpu.VMEM((A1, shard), BF16),
            pltpu.VMEM((A2, shard), BF16),
            pltpu.VMEM((B // 4, width), BF16),
            pltpu.VMEM((2 * hid + B, shard), BF16),
            rings,
            pltpu.SemaphoreType.DMA((COPIES,)),
            pltpu.SemaphoreType.DMA((COPIES,)),
            pltpu.SemaphoreType.DMA((5,)),
        ],
        compiler_params=pltpu.CompilerParams(
            collective_id=0, has_side_effects=True, vmem_limit_bytes=48 * 1024 * 1024
        ),
    )(tokens_in, out_grad, gate_weight, up_weight, down_weight)


def solution(mesh):
    return jax.shard_map(
        body,
        mesh=mesh,
        in_specs=(
            P(("rep", "fs", "tp"), None),
            P(("rep", "fs", "tp"), None),
            P("fs", "tp"),
            P("fs", "tp"),
            P("tp", "fs"),
        ),
        out_specs=(P(("rep", "fs", "tp"), None), P("fs", "tp"), P("fs", "tp"), P("tp", "fs")),
        check_vma=False,
    )
```

```python
import functools

import jax
import jax.numpy as jnp
from jax import lax
from jax.experimental import pallas as pl
from jax.experimental.pallas import tpu as pltpu
from jax.sharding import PartitionSpec as P

BF16 = jnp.bfloat16
F32 = jnp.float32
MESH = pl.DeviceIdType.MESH
COPIES = 128
SPLIT = (320, 256), (256, 256)


def nt(left, right):
    return lax.dot_general(left, right, (((1,), (1,)), ((), ())), preferred_element_type=F32)


def tn(left, right):
    return lax.dot_general(left, right, (((0,), (0,)), ((), ())), preferred_element_type=F32)


def nn(left, right):
    return lax.dot_general(left, right, (((1,), (0,)), ((), ())), preferred_element_type=F32)


def kernel(
    factor, block, width, hid,
    x_in, g_in, wg_in, wu_in, wd_in,
    gin_out, og_out, ou_out, od_out,
    X, G, WT, H, ACT, SLOPE, PW, DX, DS, GX, YA1, YA2, ZB1, ZB2, OUTT,
    ring_bufs,
    send_sems, recv_sems, local_sems,
):
    rep = lax.axis_index("rep")
    fs = lax.axis_index("fs")
    tp = lax.axis_index("tp")
    core = lax.rem(tp, 2)
    xpos = tp // 2
    shard = width // 4

    def turn(pos, step):
        return lax.rem(pos + step, 4)

    def at_x(step):
        return {"tp": turn(xpos, step) * 2 + core}

    def at_y(step):
        return {"fs": turn(fs, step)}

    def at_z(step):
        return {"rep": turn(rep, step)}

    sibling = {"tp": tp + 1 - 2 * core}

    def lanes_of(step):
        return pl.ds(pl.multiple_of(turn(fs, step) * shard, shard), shard)

    counter = [0]
    pending = []

    def remote(src, dst, k, where):
        return pltpu.make_async_remote_copy(
            src_ref=src, dst_ref=dst, send_sem=send_sems.at[k], recv_sem=recv_sems.at[k],
            device_id=where, device_id_type=MESH,
        )

    def send(src, dst, where):
        k = counter[0]
        counter[0] += 1
        copy = remote(src, dst, k, where)
        copy.start()
        pending.append(copy)
        return k

    def arrived(k, landing):
        remote(landing, landing, k, sibling).wait_recv()

    own_lanes = lanes_of(0)
    loads = [
        pltpu.make_async_copy(x_in, X.at[pl.ds(0, block)], local_sems.at[0]),
        pltpu.make_async_copy(g_in, G.at[pl.ds(0, block)], local_sems.at[1]),
        pltpu.make_async_copy(wg_in, WT.at[pl.ds(0, hid), own_lanes], local_sems.at[2]),
        pltpu.make_async_copy(wu_in, WT.at[pl.ds(hid, hid), own_lanes], local_sems.at[3]),
        pltpu.make_async_copy(wd_in, WT.at[pl.ds(2 * hid, hid), own_lanes], local_sems.at[4]),
    ]
    for load in loads:
        load.start()

    barrier = pltpu.get_barrier_semaphore()
    for where in (at_x(1), at_x(3), at_y(1), at_y(3), at_z(1), at_z(3), sibling):
        pl.semaphore_signal(barrier, inc=1, device_id=where, device_id_type=MESH)
    pl.semaphore_wait(barrier, 7)

    half = block // 2
    SELF, LEFT, RIGHT, OPP = 0, 1, 2, 3

    def slot(buf, s, start=0, count=block):
        return buf.at[pl.ds(s * 2 * block + start, count)]

    def token_start(buf):
        right = send(slot(buf, SELF), slot(buf, LEFT), at_x(1))
        left = send(slot(buf, SELF), slot(buf, RIGHT), at_x(3))
        across = send(slot(buf, SELF), slot(buf, SELF, block), sibling)
        return right, left, [(across, (SELF, block))]

    def token_relay(buf, state):
        right, left, across = state
        arrived(right, slot(buf, LEFT))
        right = send(slot(buf, LEFT, 0, half), slot(buf, OPP, 0, half), at_x(1))
        arrived(left, slot(buf, RIGHT))
        left = send(slot(buf, RIGHT, half, half), slot(buf, OPP, half, half), at_x(3))
        across.append((send(slot(buf, LEFT), slot(buf, LEFT, block), sibling), (LEFT, block)))
        across.append((send(slot(buf, RIGHT), slot(buf, RIGHT, block), sibling), (RIGHT, block)))
        return right, left, across

    def token_last(buf, state):
        out = []
        for k, start in ((state[0], 0), (state[1], half)):
            arrived(k, slot(buf, OPP, start, half))
            landing = (OPP, block + start, half)
            out.append((send(slot(buf, OPP, start, half), slot(buf, *landing), sibling), landing))
        return out

    def token_wait(buf, across):
        for k, landing in across:
            arrived(k, slot(buf, *landing))

    loads[0].wait()
    x_state = token_start(X)
    loads[1].wait()
    g_state = token_start(G)

    for load in loads[2:]:
        load.wait()

    direct = 544
    part = (3 * hid - direct) // 4
    dhalf = direct // 2
    D0, D1 = pl.ds(0, dhalf), pl.ds(dhalf, dhalf)

    def quarter(step, start=0, count=part):
        return pl.ds(pl.multiple_of(direct + turn(rep, step) * part + start, 16), count)

    def w(rows, step):
        return WT.at[rows, lanes_of(step)]

    qa = send(w(quarter(0), 0), w(quarter(0), 0), at_y(1))
    qb = send(w(quarter(0), 0), w(quarter(0), 0), at_y(3))
    d0r = send(w(D0, 0), w(D0, 0), at_y(1))
    d1l = send(w(D1, 0), w(D1, 0), at_y(3))

    qh = part // 2
    arrived(qa, w(quarter(0), 3))
    qc = send(w(quarter(0, 0, qh), 3), w(quarter(0, 0, qh), 3), at_y(1))
    arrived(qb, w(quarter(0), 1))
    qd = send(w(quarter(0, qh, qh), 1), w(quarter(0, qh, qh), 1), at_y(3))
    d1r = send(w(D1, 0), w(D1, 0), at_y(1))
    d0l = send(w(D0, 0), w(D0, 0), at_y(3))

    def share(step):
        return (
            send(w(quarter(0), step), w(quarter(0), step), at_z(1)),
            send(w(quarter(0), step), w(quarter(0), step), at_z(3)),
        )

    def share_relay(state, step):
        arrived(state[0], w(quarter(3), step))
        a = send(w(quarter(3, 0, qh), step), w(quarter(3, 0, qh), step), at_z(1))
        arrived(state[1], w(quarter(1), step))
        b = send(w(quarter(1, qh, qh), step), w(quarter(1, qh, qh), step), at_z(3))
        return a, b

    def share_last(state, step):
        arrived(state[0], w(quarter(2, 0, qh), step))
        arrived(state[1], w(quarter(2, qh, qh), step))

    z3 = share(3)
    z1 = share(1)

    x_state = token_relay(X, x_state)

    arrived(d0r, w(D0, 3))
    dc = send(w(D0, 3), w(D0, 3), at_y(1))
    arrived(d1l, w(D1, 1))
    dd = send(w(D1, 1), w(D1, 1), at_y(3))

    z3 = share_relay(z3, 3)
    arrived(qc, w(quarter(0, 0, qh), 2))
    arrived(qd, w(quarter(0, qh, qh), 2))
    z2 = share(2)
    z1 = share_relay(z1, 1)

    g_state = token_relay(G, g_state)
    x_last = token_last(X, x_state)
    z2 = share_relay(z2, 2)

    token_wait(X, x_state[2])
    token_wait(X, x_last)
    token_wait(G, g_state[2])
    arrived(d1r, w(D1, 3))
    arrived(d0l, w(D0, 1))
    for state, step in ((z3, 3), (z1, 1), (z2, 2)):
        share_last(state, step)
    arrived(dc, w(D0, 2))
    arrived(dd, w(D1, 2))

    rows = hid // 2

    def gate_stage(c):
        cols = pl.ds(c * 256, 256)
        for p in range(2):
            part_rows = pl.ds(p * rows, rows)
            gate = nt(WT[part_rows, :], X[cols, :]).astype(BF16).astype(F32)
            up = nt(WT[pl.ds(hid + p * rows, rows), :], X[cols, :]).astype(BF16).astype(F32)
            sig = jax.nn.sigmoid(gate)
            act = gate * sig
            H[pl.ds(2 * hid + p * rows, rows), cols] = (act * up).astype(BF16)
            ACT[part_rows, cols] = act
            SLOPE[part_rows, cols] = up * sig * (1.0 + gate * (1.0 - sig))

    def grad_stage(c):
        cols = pl.ds(c * 256, 256)
        grad = nt(WT[pl.ds(2 * hid, hid), :], G[cols, :]).astype(BF16).astype(F32)
        H[pl.ds(0, hid), cols] = (grad * SLOPE[:, cols]).astype(BF16)
        H[pl.ds(hid, hid), cols] = (grad * ACT[:, cols]).astype(BF16)

    gate_stage(0)
    gate_stage(1)
    g_last = token_last(G, g_state)
    gate_stage(2)
    grad_stage(0)
    grad_stage(1)
    token_wait(G, g_last)
    grad_stage(2)

    class Ring:
        def __init__(self, piece, bufs, dest):
            self.piece, self.dest = piece, dest
            self.t0, self.t1, self.fl, self.fr = bufs
            self.h = self.t0.shape[1]

        def side(self, buf, which):
            return buf.at[:, pl.ds(which * self.h, self.h)]

        def start_far(self):
            self.a = send(self.piece(2, 0), self.t0, self.dest(1))
            self.b = send(self.piece(2, 1), self.t1, self.dest(3))

        def start_near(self):
            self.c = send(self.piece(1, 1), self.side(self.fl, 1), self.dest(1))
            self.d = send(self.piece(3, 0), self.side(self.fr, 0), self.dest(3))

        def relay(self):
            arrived(self.a, self.t0)
            self.t0[...] = (self.t0[...].astype(F32) + self.piece(1, 0)[...].astype(F32)).astype(BF16)
            self.e = send(self.t0, self.side(self.fl, 0), self.dest(1))
            arrived(self.b, self.t1)
            self.t1[...] = (self.t1[...].astype(F32) + self.piece(3, 1)[...].astype(F32)).astype(BF16)
            self.f = send(self.t1, self.side(self.fr, 1), self.dest(3))

        def finish(self, store):
            arrived(self.c, self.side(self.fl, 1))
            arrived(self.d, self.side(self.fr, 0))
            arrived(self.e, self.side(self.fl, 0))
            arrived(self.f, self.side(self.fr, 1))
            for which in range(2):
                total = (
                    self.piece(0, which)[...].astype(F32)
                    + self.side(self.fl, which)[...].astype(F32)
                    + self.side(self.fr, which)[...].astype(F32)
                )
                store(which, total.astype(BF16))

    def y_piece(buf, start, count):
        def piece(step, which):
            lane = pl.multiple_of(turn(fs, step) * shard + which * (shard // 2), 128)
            return buf.at[pl.ds(start, count), pl.ds(lane, shard // 2)]
        return piece

    def z_piece(buf, start, count, lanes):
        def piece(step, which):
            row = pl.multiple_of(start + turn(rep, step) * count, 16)
            return buf.at[pl.ds(row, count), pl.ds(which * lanes, lanes)]
        return piece

    def x_piece(step, which):
        s = {0: SELF, 1: RIGHT, 3: LEFT, 2: OPP}[step]
        return GX.at[pl.ds(s * block, block), pl.ds(which * (width // 2), width // 2)]

    def strip(buf, count):
        def piece(step):
            row = pl.multiple_of(turn(rep, step) * (count // 4), 16)
            return buf.at[pl.ds(row, count // 4)]
        return piece

    def column(buf):
        def piece(step):
            return buf.at[:, lanes_of(step)]
        return piece

    class Exchange:
        def __init__(self, piece, bufs, dest):
            self.piece, self.bufs, self.dest = piece, bufs, dest

        def start(self):
            self.keys = [
                (send(self.piece(step), self.bufs[step - 1], self.dest(step)), self.bufs[step - 1])
                for step in (2, 1, 3)
            ]

        def finish(self, start):
            for k, landing in self.keys:
                arrived(k, landing)
            total = self.piece(0)[...].astype(F32)
            for buf in self.bufs:
                total = total + buf[...].astype(F32)
            OUTT[pl.ds(start, total.shape[0]), :] = total.astype(BF16)

    class Gather:
        def __init__(self, base, count):
            self.base, self.count = base, count // 4

        def row(self, step):
            return pl.multiple_of(self.base + turn(rep, step) * self.count, 16)

        def region(self, step):
            return OUTT.at[pl.ds(self.row(step), self.count)]

        def start(self):
            self.keys = [
                (send(self.region(0), self.region(0), at_z(step)), 4 - step) for step in (2, 1, 3)
            ]

        def finish(self):
            for k, step in self.keys:
                arrived(k, self.region(step))

    (A1, A2), (B1, B2) = SPLIT
    b1, b2 = A1 + A2, A1 + A2 + B1
    ya1 = Ring(y_piece(PW, 0, A1), ring_bufs[0:4], at_y)
    ya2 = Ring(y_piece(PW, A1, A2), ring_bufs[4:8], at_y)
    zb1 = Ring(z_piece(PW, b1, B1 // 4, width // 2), ring_bufs[8:12], at_z)
    zb2 = Ring(z_piece(PW, b2, B2 // 4, width // 2), ring_bufs[12:16], at_z)
    xr = Ring(x_piece, ring_bufs[16:20], at_x)
    za1 = Exchange(strip(YA1, A1), ring_bufs[20:23], at_z)
    za2 = Exchange(strip(YA2, A2), ring_bufs[23:26], at_z)
    yb1 = Exchange(column(ZB1), ring_bufs[26:29], at_y)
    yb2 = Exchange(column(ZB2), ring_bufs[29:32], at_y)
    ga1, ga2, gb1, gb2 = Gather(0, A1), Gather(A1, A2), Gather(b1, B1), Gather(b2, B2)

    def keep(buf):
        def store(which, value):
            h = value.shape[1]
            buf[:, pl.ds(which * h, h)] = value
        return store

    def weight_piece(step, start, count):
        lanes = lanes_of(step)
        PW[pl.ds(start, count), lanes] = (
            factor * nn(H[pl.ds(start, count), :], X[:, lanes])
        ).astype(BF16)

    def weight_rows(start, count):
        for lo, hi, tokens in ((start, min(start + count, 2 * hid), X), (max(start, 2 * hid), min(start + count, 3 * hid), G)):
            if lo < hi:
                for n in range(4):
                    PW[pl.ds(lo, hi - lo), pl.ds(n * 256, 256)] = (
                        factor * nn(H[pl.ds(lo, hi - lo), :], tokens[:, pl.ds(n * 256, 256)])
                    ).astype(BF16)

    def input_piece(c):
        DX[pl.ds(c * 256, 256), :] = tn(
            H[pl.ds(0, 2 * hid), pl.ds(c * 256, 256)], WT[pl.ds(0, 2 * hid), :]
        ).astype(BF16)

    def across(s):
        landing = DS.at[pl.ds(s * block, block)]
        return send(slot(DX, s, block), landing, sibling)

    def across_add(k, s):
        arrived(k, DS.at[pl.ds(s * block, block)])
        GX[pl.ds(s * block, block), :] = (
            DX[pl.ds(s * 2 * block, block), :].astype(F32)
            + DS[pl.ds(s * block, block), :].astype(F32)
        ).astype(BF16)

    spare = PW.shape[0] - 3 * hid
    PW[pl.ds(3 * hid, spare), :] = jnp.zeros((spare, width), BF16)
    weight_piece(2, 0, A1)
    ya1.start_far()
    weight_rows(b1, B1)
    zb1.start_far()
    zb1.start_near()
    weight_piece(1, 0, A1)
    weight_piece(3, 0, A1)
    ya1.start_near()
    weight_rows(A1, A2)
    ya2.start_far()
    weight_rows(b2, B2)
    zb2.start_far()
    input_piece(2)
    opp = across(OPP)
    input_piece(1)
    near = across(LEFT), across(RIGHT)
    ya1.relay()
    ya2.start_near()
    zb1.relay()
    zb2.start_near()
    across_add(opp, OPP)
    xr.start_far()
    input_piece(0)
    mine = across(SELF)
    across_add(near[0], LEFT)
    across_add(near[1], RIGHT)
    xr.start_near()
    weight_piece(0, 0, A1)
    ya2.relay()
    zb2.relay()
    ya1.finish(keep(YA1))
    za1.start()
    zb1.finish(keep(ZB1))
    yb1.start()
    across_add(mine, SELF)
    xr.relay()
    ya2.finish(keep(YA2))
    za2.start()
    zb2.finish(keep(ZB2))
    yb2.start()
    za1.finish(ga1.row(0))
    ga1.start()
    yb1.finish(gb1.row(0))
    gb1.start()
    za2.finish(ga2.row(0))
    ga2.start()
    yb2.finish(gb2.row(0))
    gb2.start()
    xr.finish(keep(gin_out))
    for gather in (ga1, ga2):
        gather.finish()
    og_out[...] = OUTT[pl.ds(0, hid), :].astype(F32)
    for gather in (gb1, gb2):
        gather.finish()
    ou_out[...] = OUTT[pl.ds(hid, hid), :].astype(F32)
    od_out[...] = OUTT[pl.ds(2 * hid, hid), :].astype(F32)

    for copy in pending:
        copy.wait_send()


def writer(*refs):
    sources, targets, sems = refs[:4], refs[4:8], refs[8]
    copies = [pltpu.make_async_copy(a, b, sems.at[i]) for i, (a, b) in enumerate(zip(sources, targets))]
    for copy in copies:
        copy.start()
    for copy in copies:
        copy.wait()


def body(tokens_in, out_grad, gate_weight, up_weight, down_weight):
    block, width = tokens_in.shape
    shard, hid = gate_weight.shape
    devices = lax.axis_size("rep") * lax.axis_size("fs") * lax.axis_size("tp")
    factor = (block * devices) ** (-0.5)
    tokens = block * 8
    (A1, A2), (B1, B2) = SPLIT
    total_rows = A1 + A2 + B1 + B2

    def ring(count, lanes):
        return [
            pltpu.VMEM((count, lanes // 2), BF16),
            pltpu.VMEM((count, lanes // 2), BF16),
            pltpu.VMEM((count, lanes), BF16),
            pltpu.VMEM((count, lanes), BF16),
        ]

    def exchange(count):
        return [pltpu.VMEM((count // 4, shard), BF16)] * 3

    rings = (
        ring(A1, shard) + ring(A2, shard) + ring(B1 // 4, width) + ring(B2 // 4, width)
        + ring(block, width)
        + exchange(A1) + exchange(A2) + exchange(B1) + exchange(B2)
    )
    outs = (
        jax.ShapeDtypeStruct((block, width), BF16),
        jax.ShapeDtypeStruct((hid, shard), F32),
        jax.ShapeDtypeStruct((hid, shard), F32),
        jax.ShapeDtypeStruct((hid, shard), F32),
    )
    results = pl.pallas_call(
        functools.partial(kernel, factor, block, width, hid),
        out_shape=outs,
        in_specs=[pl.BlockSpec(memory_space=pltpu.HBM)] * 5,
        out_specs=[pl.BlockSpec(memory_space=pltpu.VMEM)] * 4,
        scratch_shapes=[
            pltpu.VMEM((tokens, width), BF16),
            pltpu.VMEM((tokens, width), BF16),
            pltpu.VMEM((3 * hid, width), BF16),
            pltpu.VMEM((3 * hid, tokens), BF16),
            pltpu.VMEM((hid, tokens), F32),
            pltpu.VMEM((hid, tokens), F32),
            pltpu.VMEM((total_rows, width), BF16),
            pltpu.VMEM((tokens, width), BF16),
            pltpu.VMEM((tokens // 2, width), BF16),
            pltpu.VMEM((tokens // 2, width), BF16),
            pltpu.VMEM((A1, shard), BF16),
            pltpu.VMEM((A2, shard), BF16),
            pltpu.VMEM((B1 // 4, width), BF16),
            pltpu.VMEM((B2 // 4, width), BF16),
            pltpu.VMEM((total_rows, shard), BF16),
            rings,
            pltpu.SemaphoreType.DMA((COPIES,)),
            pltpu.SemaphoreType.DMA((COPIES,)),
            pltpu.SemaphoreType.DMA((5,)),
        ],
        compiler_params=pltpu.CompilerParams(
            collective_id=0, has_side_effects=True, vmem_limit_bytes=48 * 1024 * 1024
        ),
    )(tokens_in, out_grad, gate_weight.T, up_weight.T, down_weight)
    grad_in, gate_t, up_t, down_t = pl.pallas_call(
        writer,
        out_shape=outs,
        in_specs=[pl.BlockSpec(memory_space=pl.ANY)] * 4,
        out_specs=[pl.BlockSpec(memory_space=pltpu.HBM)] * 4,
        scratch_shapes=[pltpu.SemaphoreType.DMA((4,))],
        compiler_params=pltpu.CompilerParams(vmem_limit_bytes=1024 * 1024),
    )(*results)
    return grad_in, gate_t.T, up_t.T, down_t


def solution(mesh):
    return jax.shard_map(
        body,
        mesh=mesh,
        in_specs=(
            P(("rep", "fs", "tp"), None),
            P(("rep", "fs", "tp"), None),
            P("fs", "tp"),
            P("fs", "tp"),
            P("tp", "fs"),
        ),
        out_specs=(P(("rep", "fs", "tp"), None), P("fs", "tp"), P("fs", "tp"), P("tp", "fs")),
        check_vma=False,
    )
```

```python
import functools

import jax
import jax.numpy as jnp
from jax import lax
from jax.experimental import pallas as pl
from jax.experimental.pallas import tpu as pltpu
from jax.sharding import PartitionSpec as P

BF16 = jnp.bfloat16
F32 = jnp.float32
MESH = pl.DeviceIdType.MESH
COPIES = 128
SPLIT = (320, 256), (256, 256)


def nt(left, right):
    return lax.dot_general(left, right, (((1,), (1,)), ((), ())), preferred_element_type=F32)


def tn(left, right):
    return lax.dot_general(left, right, (((0,), (0,)), ((), ())), preferred_element_type=F32)


def nn(left, right):
    return lax.dot_general(left, right, (((1,), (0,)), ((), ())), preferred_element_type=F32)


def kernel(
    factor, block, width, hid,
    x_in, g_in, wg_in, wu_in, wd_in,
    gin_out, og_out, ou_out, od_out,
    X, G, WT, H, ACT, SLOPE, PW, DX, DS, GX, YA1, YA2, ZB1, ZB2, OUTT,
    ring_bufs,
    send_sems, recv_sems, local_sems,
):
    rep = lax.axis_index("rep")
    fs = lax.axis_index("fs")
    tp = lax.axis_index("tp")
    core = lax.rem(tp, 2)
    xpos = tp // 2
    shard = width // 4

    def turn(pos, step):
        return lax.rem(pos + step, 4)

    def at_x(step):
        return {"tp": turn(xpos, step) * 2 + core}

    def at_y(step):
        return {"fs": turn(fs, step)}

    def at_z(step):
        return {"rep": turn(rep, step)}

    sibling = {"tp": tp + 1 - 2 * core}

    def lanes_of(step):
        return pl.ds(pl.multiple_of(turn(fs, step) * shard, shard), shard)

    counter = [0]
    pending = []

    def remote(src, dst, k, where):
        return pltpu.make_async_remote_copy(
            src_ref=src, dst_ref=dst, send_sem=send_sems.at[k], recv_sem=recv_sems.at[k],
            device_id=where, device_id_type=MESH,
        )

    def send(src, dst, where):
        k = counter[0]
        counter[0] += 1
        copy = remote(src, dst, k, where)
        copy.start()
        pending.append(copy)
        return k

    def arrived(k, landing):
        remote(landing, landing, k, sibling).wait_recv()

    barrier = pltpu.get_barrier_semaphore()
    partners = [sibling] + [at(step) for at in (at_x, at_y, at_z) for step in (1, 3)]
    partners += [at_y(2), at_z(2)]
    for where in partners:
        pl.semaphore_signal(barrier, inc=1, device_id=where, device_id_type=MESH)

    own_lanes = lanes_of(0)
    loads = [
        pltpu.make_async_copy(x_in, X.at[pl.ds(0, block)], local_sems.at[0]),
        pltpu.make_async_copy(g_in, G.at[pl.ds(0, block)], local_sems.at[1]),
        pltpu.make_async_copy(wg_in, WT.at[pl.ds(0, hid), own_lanes], local_sems.at[2]),
        pltpu.make_async_copy(wu_in, WT.at[pl.ds(hid, hid), own_lanes], local_sems.at[3]),
        pltpu.make_async_copy(wd_in, WT.at[pl.ds(2 * hid, hid), own_lanes], local_sems.at[4]),
    ]
    for load in loads:
        load.start()

    pl.semaphore_wait(barrier, len(partners))

    half = block // 2
    SELF, LEFT, RIGHT, OPP = 0, 1, 2, 3

    def slot(buf, s, start=0, count=block):
        return buf.at[pl.ds(s * 2 * block + start, count)]

    def forward(buf, s, start=0, count=block):
        landing = (s, block + start, count)
        return send(slot(buf, s, start, count), slot(buf, *landing), sibling), landing

    def forwarded(buf, *states):
        for k, landing in states:
            arrived(k, slot(buf, *landing))

    class Tokens:
        def __init__(self, buf):
            self.buf = buf

        def part(self, s, which):
            return slot(self.buf, s, which * half, half)

        def start_first(self):
            self.r0 = send(self.part(SELF, 0), self.part(LEFT, 0), at_x(1))
            self.l1 = send(self.part(SELF, 1), self.part(RIGHT, 1), at_x(3))

        def start_second(self):
            self.r1 = send(self.part(SELF, 1), self.part(LEFT, 1), at_x(1))
            self.l0 = send(self.part(SELF, 0), self.part(RIGHT, 0), at_x(3))

        def relay(self):
            arrived(self.r0, self.part(LEFT, 0))
            self.r2 = send(self.part(LEFT, 0), self.part(OPP, 0), at_x(1))
            arrived(self.l1, self.part(RIGHT, 1))
            self.l2 = send(self.part(RIGHT, 1), self.part(OPP, 1), at_x(3))

        def near(self):
            arrived(self.r1, self.part(LEFT, 1))
            arrived(self.l0, self.part(RIGHT, 0))
            return forward(self.buf, LEFT), forward(self.buf, RIGHT)

        def far(self):
            arrived(self.r2, self.part(OPP, 0))
            first = forward(self.buf, OPP, 0, half)
            arrived(self.l2, self.part(OPP, 1))
            return first, forward(self.buf, OPP, half, half)

    xt, gt = Tokens(X), Tokens(G)
    loads[0].wait()
    xt.start_first()
    xt.start_second()
    loads[1].wait()
    gt.start_first()
    for load in loads[2:]:
        load.wait()

    part, direct, spare = 64, 448, 96
    base1, base2 = direct, 2 * hid + spare
    qh, dhalf = part // 2, direct // 2
    D0, D1 = pl.ds(0, dhalf), pl.ds(dhalf, dhalf)
    D2 = pl.ds(2 * hid, spare)

    def quarter(base, step, start=0, count=part):
        return pl.ds(pl.multiple_of(base + turn(rep, step) * part + start, 16), count)

    def w(rows, step):
        return WT.at[rows, lanes_of(step)]

    def copy_w(rows, step, where):
        return send(w(rows, step), w(rows, step), where)

    class Quarters:
        def __init__(self, base):
            self.base = base

        def start(self):
            own = quarter(self.base, 0)
            self.r, self.l = copy_w(own, 0, at_y(1)), copy_w(own, 0, at_y(3))
            self.shares = {}

        def relay(self):
            arrived(self.r, w(quarter(self.base, 0), 3))
            self.r2 = copy_w(quarter(self.base, 0, 0, qh), 3, at_y(1))
            arrived(self.l, w(quarter(self.base, 0), 1))
            self.l2 = copy_w(quarter(self.base, 0, qh, qh), 1, at_y(3))

        def far(self):
            arrived(self.r2, w(quarter(self.base, 0, 0, qh), 2))
            arrived(self.l2, w(quarter(self.base, 0, qh, qh), 2))

        def share(self, lane):
            self.shares[lane] = [
                (copy_w(quarter(self.base, 0), lane, at_z(step)), 4 - step) for step in (2, 1, 3)
            ]

        def finish(self):
            for lane, keys in self.shares.items():
                for k, step in keys:
                    arrived(k, w(quarter(self.base, step), lane))

    q1, q2 = Quarters(base1), Quarters(base2)
    q1.start()
    q2.start()
    d0r = copy_w(D0, 0, at_y(1))
    d1l = copy_w(D1, 0, at_y(3))
    x_own = forward(X, SELF)
    g_own = forward(G, SELF)

    q1.relay()
    q1.share(3)
    q1.share(1)
    q2.relay()
    d1r = copy_w(D1, 0, at_y(1))
    d0l = copy_w(D0, 0, at_y(3))

    xt.relay()
    gt.start_second()
    arrived(d0r, w(D0, 3))
    dc = copy_w(D0, 3, at_y(1))
    arrived(d1l, w(D1, 1))
    dd = copy_w(D1, 1, at_y(3))
    x_near = xt.near()
    q1.far()
    q1.share(2)
    q2.share(3)
    q2.share(1)
    q2.far()
    q2.share(2)
    d2 = [(copy_w(D2, 0, at_y(step)), 4 - step) for step in (2, 1, 3)]
    gt.relay()
    x_far = xt.far()

    forwarded(X, x_own, *x_near)
    arrived(d1r, w(D1, 3))
    arrived(d0l, w(D0, 1))
    q1.finish()
    arrived(dc, w(D0, 2))
    arrived(dd, w(D1, 2))

    rows = hid // 2

    def gate_stage(c):
        cols = pl.ds(c * 256, 256)
        for p in range(2):
            part_rows = pl.ds(p * rows, rows)
            gate = nt(WT[part_rows, :], X[cols, :]).astype(BF16).astype(F32)
            up = nt(WT[pl.ds(hid + p * rows, rows), :], X[cols, :]).astype(BF16).astype(F32)
            sig = jax.nn.sigmoid(gate)
            act = gate * sig
            H[pl.ds(2 * hid + p * rows, rows), cols] = (act * up).astype(BF16)
            ACT[part_rows, cols] = act
            SLOPE[part_rows, cols] = up * sig * (1.0 + gate * (1.0 - sig))

    def grad_stage(c):
        cols = pl.ds(c * 256, 256)
        grad = nt(WT[pl.ds(2 * hid, hid), :], G[cols, :]).astype(BF16).astype(F32)
        H[pl.ds(0, hid), cols] = (grad * SLOPE[:, cols]).astype(BF16)
        H[pl.ds(hid, hid), cols] = (grad * ACT[:, cols]).astype(BF16)

    gate_stage(0)
    gate_stage(1)
    g_near = gt.near()
    forwarded(X, *x_far)
    gate_stage(2)
    q2.finish()
    for k, step in d2:
        arrived(k, w(D2, step))
    forwarded(G, g_own, g_near[0])
    grad_stage(0)
    g_far = gt.far()
    forwarded(G, g_near[1])
    grad_stage(1)
    forwarded(G, *g_far)
    grad_stage(2)

    class Ring:
        def __init__(self, piece, bufs, dest):
            self.piece, self.dest = piece, dest
            self.t0, self.t1, self.fl, self.fr = bufs
            self.h = self.t0.shape[1]

        def side(self, buf, which):
            return buf.at[:, pl.ds(which * self.h, self.h)]

        def start_far(self):
            self.a = send(self.piece(2, 0), self.t0, self.dest(1))
            self.b = send(self.piece(2, 1), self.t1, self.dest(3))

        def start_near(self):
            self.c = send(self.piece(1, 1), self.side(self.fl, 1), self.dest(1))
            self.d = send(self.piece(3, 0), self.side(self.fr, 0), self.dest(3))

        def relay(self):
            arrived(self.a, self.t0)
            self.t0[...] = (self.t0[...].astype(F32) + self.piece(1, 0)[...].astype(F32)).astype(BF16)
            self.e = send(self.t0, self.side(self.fl, 0), self.dest(1))
            arrived(self.b, self.t1)
            self.t1[...] = (self.t1[...].astype(F32) + self.piece(3, 1)[...].astype(F32)).astype(BF16)
            self.f = send(self.t1, self.side(self.fr, 1), self.dest(3))

        def finish(self, store):
            arrived(self.c, self.side(self.fl, 1))
            arrived(self.d, self.side(self.fr, 0))
            arrived(self.e, self.side(self.fl, 0))
            arrived(self.f, self.side(self.fr, 1))
            for which in range(2):
                total = (
                    self.piece(0, which)[...].astype(F32)
                    + self.side(self.fl, which)[...].astype(F32)
                    + self.side(self.fr, which)[...].astype(F32)
                )
                store(which, total.astype(BF16))

    def y_piece(buf, start, count):
        def piece(step, which):
            lane = pl.multiple_of(turn(fs, step) * shard + which * (shard // 2), 128)
            return buf.at[pl.ds(start, count), pl.ds(lane, shard // 2)]
        return piece

    def z_piece(buf, start, count, lanes):
        def piece(step, which):
            row = pl.multiple_of(start + turn(rep, step) * count, 16)
            return buf.at[pl.ds(row, count), pl.ds(which * lanes, lanes)]
        return piece

    def x_piece(step, which):
        s = {0: SELF, 1: RIGHT, 3: LEFT, 2: OPP}[step]
        return GX.at[pl.ds(s * block, block), pl.ds(which * (width // 2), width // 2)]

    def strip(buf, count):
        def piece(step):
            row = pl.multiple_of(turn(rep, step) * (count // 4), 16)
            return buf.at[pl.ds(row, count // 4)]
        return piece

    def column(buf):
        def piece(step):
            return buf.at[:, lanes_of(step)]
        return piece

    class Exchange:
        def __init__(self, piece, bufs, dest):
            self.piece, self.bufs, self.dest = piece, bufs, dest

        def start(self):
            self.keys = [
                (send(self.piece(step), self.bufs[step - 1], self.dest(step)), self.bufs[step - 1])
                for step in (2, 1, 3)
            ]

        def finish(self, start):
            for k, landing in self.keys:
                arrived(k, landing)
            total = self.piece(0)[...].astype(F32)
            for buf in self.bufs:
                total = total + buf[...].astype(F32)
            OUTT[pl.ds(start, total.shape[0]), :] = total.astype(BF16)

    class Gather:
        def __init__(self, base, count):
            self.base, self.count = base, count // 4

        def row(self, step):
            return pl.multiple_of(self.base + turn(rep, step) * self.count, 16)

        def region(self, step):
            return OUTT.at[pl.ds(self.row(step), self.count)]

        def start(self):
            self.keys = [
                (send(self.region(0), self.region(0), at_z(step)), 4 - step) for step in (2, 1, 3)
            ]

        def finish(self):
            for k, step in self.keys:
                arrived(k, self.region(step))

    (A1, A2), (B1, B2) = SPLIT
    b1, b2 = A1 + A2, A1 + A2 + B1
    ya1 = Ring(y_piece(PW, 0, A1), ring_bufs[0:4], at_y)
    ya2 = Ring(y_piece(PW, A1, A2), ring_bufs[4:8], at_y)
    zb1 = Ring(z_piece(PW, b1, B1 // 4, width // 2), ring_bufs[8:12], at_z)
    zb2 = Ring(z_piece(PW, b2, B2 // 4, width // 2), ring_bufs[12:16], at_z)
    xr = Ring(x_piece, ring_bufs[16:20], at_x)
    za1 = Exchange(strip(YA1, A1), ring_bufs[20:23], at_z)
    za2 = Exchange(strip(YA2, A2), ring_bufs[23:26], at_z)
    yb1 = Exchange(column(ZB1), ring_bufs[26:29], at_y)
    yb2 = Exchange(column(ZB2), ring_bufs[29:32], at_y)
    ga1, ga2, gb1, gb2 = Gather(0, A1), Gather(A1, A2), Gather(b1, B1), Gather(b2, B2)

    def keep(buf):
        def store(which, value):
            h = value.shape[1]
            buf[:, pl.ds(which * h, h)] = value
        return store

    def weight_piece(step, start, count):
        lanes = lanes_of(step)
        PW[pl.ds(start, count), lanes] = (
            factor * nn(H[pl.ds(start, count), :], X[:, lanes])
        ).astype(BF16)

    def weight_rows(start, count):
        for lo, hi, tokens in ((start, min(start + count, 2 * hid), X), (max(start, 2 * hid), min(start + count, 3 * hid), G)):
            if lo < hi:
                for n in range(4):
                    PW[pl.ds(lo, hi - lo), pl.ds(n * 256, 256)] = (
                        factor * nn(H[pl.ds(lo, hi - lo), :], tokens[:, pl.ds(n * 256, 256)])
                    ).astype(BF16)

    def input_piece(c):
        DX[pl.ds(c * 256, 256), :] = tn(
            H[pl.ds(0, 2 * hid), pl.ds(c * 256, 256)], WT[pl.ds(0, 2 * hid), :]
        ).astype(BF16)

    def across(s):
        landing = DS.at[pl.ds(s * block, block)]
        return send(slot(DX, s, block), landing, sibling)

    def across_add(k, s):
        arrived(k, DS.at[pl.ds(s * block, block)])
        GX[pl.ds(s * block, block), :] = (
            DX[pl.ds(s * 2 * block, block), :].astype(F32)
            + DS[pl.ds(s * block, block), :].astype(F32)
        ).astype(BF16)

    blank = PW.shape[0] - 3 * hid
    PW[pl.ds(3 * hid, blank), :] = jnp.zeros((blank, width), BF16)
    weight_piece(2, 0, A1)
    ya1.start_far()
    weight_rows(b1, B1)
    zb1.start_far()
    zb1.start_near()
    weight_piece(1, 0, A1)
    weight_piece(3, 0, A1)
    ya1.start_near()
    weight_rows(A1, A2)
    ya2.start_far()
    weight_rows(b2, B2)
    zb2.start_far()
    input_piece(2)
    opp = across(OPP)
    input_piece(1)
    near = across(LEFT), across(RIGHT)
    ya1.relay()
    ya2.start_near()
    zb1.relay()
    zb2.start_near()
    across_add(opp, OPP)
    xr.start_far()
    input_piece(0)
    mine = across(SELF)
    across_add(near[0], LEFT)
    across_add(near[1], RIGHT)
    xr.start_near()
    weight_piece(0, 0, A1)
    ya2.relay()
    zb2.relay()
    ya1.finish(keep(YA1))
    za1.start()
    zb1.finish(keep(ZB1))
    yb1.start()
    across_add(mine, SELF)
    xr.relay()
    ya2.finish(keep(YA2))
    za2.start()
    zb2.finish(keep(ZB2))
    yb2.start()
    za1.finish(ga1.row(0))
    ga1.start()
    yb1.finish(gb1.row(0))
    gb1.start()
    za2.finish(ga2.row(0))
    ga2.start()
    yb2.finish(gb2.row(0))
    gb2.start()
    xr.finish(keep(gin_out))
    for gather in (ga1, ga2):
        gather.finish()
    og_out[...] = OUTT[pl.ds(0, hid), :].astype(F32)
    for gather in (gb1, gb2):
        gather.finish()
    ou_out[...] = OUTT[pl.ds(hid, hid), :].astype(F32)
    od_out[...] = OUTT[pl.ds(2 * hid, hid), :].astype(F32)

    for copy in pending:
        copy.wait_send()


def writer(*refs):
    sources, targets, sems = refs[:4], refs[4:8], refs[8]
    copies = [pltpu.make_async_copy(a, b, sems.at[i]) for i, (a, b) in enumerate(zip(sources, targets))]
    for copy in copies:
        copy.start()
    for copy in copies:
        copy.wait()


def body(tokens_in, out_grad, gate_weight, up_weight, down_weight):
    block, width = tokens_in.shape
    shard, hid = gate_weight.shape
    devices = lax.axis_size("rep") * lax.axis_size("fs") * lax.axis_size("tp")
    factor = (block * devices) ** (-0.5)
    tokens = block * 8
    (A1, A2), (B1, B2) = SPLIT
    total_rows = A1 + A2 + B1 + B2

    def ring(count, lanes):
        return [
            pltpu.VMEM((count, lanes // 2), BF16),
            pltpu.VMEM((count, lanes // 2), BF16),
            pltpu.VMEM((count, lanes), BF16),
            pltpu.VMEM((count, lanes), BF16),
        ]

    def exchange(count):
        return [pltpu.VMEM((count // 4, shard), BF16)] * 3

    rings = (
        ring(A1, shard) + ring(A2, shard) + ring(B1 // 4, width) + ring(B2 // 4, width)
        + ring(block, width)
        + exchange(A1) + exchange(A2) + exchange(B1) + exchange(B2)
    )
    outs = (
        jax.ShapeDtypeStruct((block, width), BF16),
        jax.ShapeDtypeStruct((hid, shard), F32),
        jax.ShapeDtypeStruct((hid, shard), F32),
        jax.ShapeDtypeStruct((hid, shard), F32),
    )
    arrays = tokens_in, out_grad, gate_weight.T, up_weight.T, down_weight
    results = pl.pallas_call(
        functools.partial(kernel, factor, block, width, hid),
        out_shape=outs,
        in_specs=[pl.BlockSpec(memory_space=pltpu.HBM)] * 5,
        out_specs=[pl.BlockSpec(memory_space=pltpu.VMEM)] * 4,
        scratch_shapes=[
            pltpu.VMEM((tokens, width), BF16),
            pltpu.VMEM((tokens, width), BF16),
            pltpu.VMEM((3 * hid, width), BF16),
            pltpu.VMEM((3 * hid, tokens), BF16),
            pltpu.VMEM((hid, tokens), F32),
            pltpu.VMEM((hid, tokens), F32),
            pltpu.VMEM((total_rows, width), BF16),
            pltpu.VMEM((tokens, width), BF16),
            pltpu.VMEM((tokens // 2, width), BF16),
            pltpu.VMEM((tokens // 2, width), BF16),
            pltpu.VMEM((A1, shard), BF16),
            pltpu.VMEM((A2, shard), BF16),
            pltpu.VMEM((B1 // 4, width), BF16),
            pltpu.VMEM((B2 // 4, width), BF16),
            pltpu.VMEM((total_rows, shard), BF16),
            rings,
            pltpu.SemaphoreType.DMA((COPIES,)),
            pltpu.SemaphoreType.DMA((COPIES,)),
            pltpu.SemaphoreType.DMA((5,)),
        ],
        compiler_params=pltpu.CompilerParams(
            collective_id=0, has_side_effects=True, vmem_limit_bytes=48 * 1024 * 1024
        ),
    )(*[pltpu.with_memory_space_constraint(a, pltpu.HBM) for a in arrays])
    grad_in, gate_t, up_t, down_t = pl.pallas_call(
        writer,
        out_shape=outs,
        in_specs=[pl.BlockSpec(memory_space=pl.ANY)] * 4,
        out_specs=[pl.BlockSpec(memory_space=pltpu.HBM)] * 4,
        scratch_shapes=[pltpu.SemaphoreType.DMA((4,))],
        compiler_params=pltpu.CompilerParams(vmem_limit_bytes=1024 * 1024),
    )(*results)
    return grad_in, gate_t.T, up_t.T, down_t


def solution(mesh):
    return jax.shard_map(
        body,
        mesh=mesh,
        in_specs=(
            P(("rep", "fs", "tp"), None),
            P(("rep", "fs", "tp"), None),
            P("fs", "tp"),
            P("fs", "tp"),
            P("tp", "fs"),
        ),
        out_specs=(P(("rep", "fs", "tp"), None), P("fs", "tp"), P("fs", "tp"), P("tp", "fs")),
        check_vma=False,
    )
```

```python
import functools

import jax
import jax.numpy as jnp
from jax import lax
from jax.experimental import pallas as pl
from jax.experimental.pallas import tpu as pltpu
from jax.sharding import PartitionSpec as P

BF16 = jnp.bfloat16
F32 = jnp.float32
MESH = pl.DeviceIdType.MESH
COPIES = 144
SPLIT = (128, 256, 192), (128, 192, 192)


def nt(left, right):
    return lax.dot_general(left, right, (((1,), (1,)), ((), ())), preferred_element_type=F32)


def tn(left, right):
    return lax.dot_general(left, right, (((0,), (0,)), ((), ())), preferred_element_type=F32)


def nn(left, right):
    return lax.dot_general(left, right, (((1,), (0,)), ((), ())), preferred_element_type=F32)


def kernel(
    factor, block, width, hid,
    x_in, g_in, wg_in, wu_in, wd_in,
    gin_out, og_out, ou_out, od_out,
    X, G, WT, H, ACT, SLOPE, PW, DX, DS, GX, YA, ZB, OUTT, YA_BUFS, ZB_BUFS, ZA_BUFS, YB_BUFS, XR_BUFS,
    send_sems, recv_sems, local_sems,
):
    rep = lax.axis_index("rep")
    fs = lax.axis_index("fs")
    tp = lax.axis_index("tp")
    core = lax.rem(tp, 2)
    xpos = tp // 2
    shard = width // 4

    def turn(pos, step):
        return lax.rem(pos + step, 4)

    def at_x(step):
        return {"tp": turn(xpos, step) * 2 + core}

    def at_y(step):
        return {"fs": turn(fs, step)}

    def at_z(step):
        return {"rep": turn(rep, step)}

    sibling = {"tp": tp + 1 - 2 * core}

    def lanes_of(step):
        return pl.ds(pl.multiple_of(turn(fs, step) * shard, shard), shard)

    counter = [0]
    pending = []

    def remote(src, dst, k, where):
        return pltpu.make_async_remote_copy(
            src_ref=src, dst_ref=dst, send_sem=send_sems.at[k], recv_sem=recv_sems.at[k],
            device_id=where, device_id_type=MESH,
        )

    def send(src, dst, where):
        k = counter[0]
        counter[0] += 1
        copy = remote(src, dst, k, where)
        copy.start()
        pending.append(copy)
        return k

    def arrived(k, landing):
        remote(landing, landing, k, sibling).wait_recv()

    barrier = pltpu.get_barrier_semaphore()
    partners = [sibling] + [at(step) for at in (at_x, at_y, at_z) for step in (1, 3)]
    partners += [at_y(2), at_z(2)]
    for where in partners:
        pl.semaphore_signal(barrier, inc=1, device_id=where, device_id_type=MESH)

    own_lanes = lanes_of(0)
    loads = [
        pltpu.make_async_copy(x_in, X.at[pl.ds(0, block)], local_sems.at[0]),
        pltpu.make_async_copy(g_in, G.at[pl.ds(0, block)], local_sems.at[1]),
        pltpu.make_async_copy(wg_in, WT.at[pl.ds(0, hid), own_lanes], local_sems.at[2]),
        pltpu.make_async_copy(wu_in, WT.at[pl.ds(hid, hid), own_lanes], local_sems.at[3]),
        pltpu.make_async_copy(wd_in, WT.at[pl.ds(2 * hid, hid), own_lanes], local_sems.at[4]),
    ]
    for load in loads:
        load.start()

    pl.semaphore_wait(barrier, len(partners))

    half = block // 2
    SELF, LEFT, RIGHT, OPP = 0, 1, 2, 3

    def slot(buf, s, start=0, count=block):
        return buf.at[pl.ds(s * 2 * block + start, count)]

    def forward(buf, s, start=0, count=block):
        landing = (s, block + start, count)
        return send(slot(buf, s, start, count), slot(buf, *landing), sibling), landing

    def forwarded(buf, *states):
        for k, landing in states:
            arrived(k, slot(buf, *landing))

    class Tokens:
        def __init__(self, buf):
            self.buf = buf

        def part(self, s, which):
            return slot(self.buf, s, which * half, half)

        def start_first(self):
            self.r0 = send(self.part(SELF, 0), self.part(LEFT, 0), at_x(1))
            self.l1 = send(self.part(SELF, 1), self.part(RIGHT, 1), at_x(3))

        def start_second(self):
            self.r1 = send(self.part(SELF, 1), self.part(LEFT, 1), at_x(1))
            self.l0 = send(self.part(SELF, 0), self.part(RIGHT, 0), at_x(3))

        def relay(self):
            arrived(self.r0, self.part(LEFT, 0))
            self.r2 = send(self.part(LEFT, 0), self.part(OPP, 0), at_x(1))
            arrived(self.l1, self.part(RIGHT, 1))
            self.l2 = send(self.part(RIGHT, 1), self.part(OPP, 1), at_x(3))

        def near(self):
            arrived(self.r1, self.part(LEFT, 1))
            arrived(self.l0, self.part(RIGHT, 0))
            return forward(self.buf, LEFT), forward(self.buf, RIGHT)

        def far(self):
            arrived(self.r2, self.part(OPP, 0))
            first = forward(self.buf, OPP, 0, half)
            arrived(self.l2, self.part(OPP, 1))
            return first, forward(self.buf, OPP, half, half)

    xt, gt = Tokens(X), Tokens(G)
    loads[0].wait()
    xt.start_first()
    xt.start_second()
    loads[1].wait()
    gt.start_first()
    for load in loads[2:]:
        load.wait()

    direct, spare = 384, 96
    base1, base2 = direct, 2 * hid + spare
    dhalf = direct // 2
    D0, D1 = pl.ds(0, dhalf), pl.ds(dhalf, dhalf)
    D2 = pl.ds(2 * hid, spare)

    def w(rows, step):
        return WT.at[rows, lanes_of(step)]

    def copy_w(rows, step, where):
        return send(w(rows, step), w(rows, step), where)

    class Quarters:
        def __init__(self, base, end):
            self.base, self.part = base, (end - base) // 4
            self.cut = (self.part // 2 + 15) // 16 * 16

        def rows(self, step, which=None):
            start, count = {
                None: (0, self.part), 0: (0, self.cut), 1: (self.cut, self.part - self.cut)
            }[which]
            return pl.ds(pl.multiple_of(self.base + turn(rep, step) * self.part + start, 16), count)

        def start(self):
            self.r, self.l = copy_w(self.rows(0), 0, at_y(1)), copy_w(self.rows(0), 0, at_y(3))
            self.shares = {}

        def relay(self):
            arrived(self.r, w(self.rows(0), 3))
            self.r2 = copy_w(self.rows(0, 0), 3, at_y(1))
            arrived(self.l, w(self.rows(0), 1))
            self.l2 = copy_w(self.rows(0, 1), 1, at_y(3))

        def far(self):
            arrived(self.r2, w(self.rows(0, 0), 2))
            arrived(self.l2, w(self.rows(0, 1), 2))

        def share(self, lane):
            self.shares[lane] = [
                (copy_w(self.rows(0), lane, at_z(step)), 4 - step) for step in (2, 1, 3)
            ]

        def finish(self):
            for lane, keys in self.shares.items():
                for k, step in keys:
                    arrived(k, w(self.rows(step), lane))

    q1, q2 = Quarters(base1, 2 * hid), Quarters(base2, 3 * hid)
    q1.start()
    q2.start()
    d0r = copy_w(D0, 0, at_y(1))
    d1l = copy_w(D1, 0, at_y(3))
    x_own = forward(X, SELF)
    g_own = forward(G, SELF)

    q1.relay()
    q1.share(3)
    q1.share(1)
    q2.relay()
    d1r = copy_w(D1, 0, at_y(1))
    d0l = copy_w(D0, 0, at_y(3))

    xt.relay()
    gt.start_second()
    arrived(d0r, w(D0, 3))
    dc = copy_w(D0, 3, at_y(1))
    arrived(d1l, w(D1, 1))
    dd = copy_w(D1, 1, at_y(3))
    x_near = xt.near()
    q1.far()
    q1.share(2)
    q2.share(3)
    q2.share(1)
    q2.far()
    q2.share(2)
    d2 = [(copy_w(D2, 0, at_y(step)), 4 - step) for step in (2, 1, 3)]
    gt.relay()
    x_far = xt.far()

    forwarded(X, x_own, *x_near)
    arrived(d1r, w(D1, 3))
    arrived(d0l, w(D0, 1))
    q1.finish()
    arrived(dc, w(D0, 2))
    arrived(dd, w(D1, 2))

    rows = hid // 2

    def gate_stage(c):
        cols = pl.ds(c * 256, 256)
        for p in range(2):
            part_rows = pl.ds(p * rows, rows)
            gate = nt(WT[part_rows, :], X[cols, :]).astype(BF16).astype(F32)
            up = nt(WT[pl.ds(hid + p * rows, rows), :], X[cols, :]).astype(BF16).astype(F32)
            sig = jax.nn.sigmoid(gate)
            act = gate * sig
            H[pl.ds(2 * hid + p * rows, rows), cols] = (act * up).astype(BF16)
            ACT[part_rows, cols] = act
            SLOPE[part_rows, cols] = up * sig * (1.0 + gate * (1.0 - sig))

    def grad_stage(c):
        cols = pl.ds(c * 256, 256)
        grad = nt(WT[pl.ds(2 * hid, hid), :], G[cols, :]).astype(BF16).astype(F32)
        H[pl.ds(0, hid), cols] = (grad * SLOPE[:, cols]).astype(BF16)
        H[pl.ds(hid, hid), cols] = (grad * ACT[:, cols]).astype(BF16)

    gate_stage(0)
    gate_stage(1)
    g_near = gt.near()
    forwarded(X, *x_far)
    gate_stage(2)
    q2.finish()
    for k, step in d2:
        arrived(k, w(D2, step))
    forwarded(G, g_own, g_near[0])
    g_far = gt.far()
    grad_stage(0)
    forwarded(G, g_near[1])
    grad_stage(1)
    forwarded(G, *g_far)
    grad_stage(2)

    class Ring:
        def __init__(self, piece, bufs, dest):
            self.piece, self.dest = piece, dest
            self.t0, self.t1, self.fl, self.fr = bufs
            self.h = self.t0.shape[1]

        def side(self, buf, which):
            return buf.at[:, pl.ds(which * self.h, self.h)]

        def start_far(self):
            self.a = send(self.piece(2, 0), self.t0, self.dest(1))
            self.b = send(self.piece(2, 1), self.t1, self.dest(3))

        def start_near(self):
            self.c = send(self.piece(1, 1), self.side(self.fl, 1), self.dest(1))
            self.d = send(self.piece(3, 0), self.side(self.fr, 0), self.dest(3))

        def relay(self):
            arrived(self.a, self.t0)
            self.t0[...] = (self.t0[...].astype(F32) + self.piece(1, 0)[...].astype(F32)).astype(BF16)
            self.e = send(self.t0, self.side(self.fl, 0), self.dest(1))
            arrived(self.b, self.t1)
            self.t1[...] = (self.t1[...].astype(F32) + self.piece(3, 1)[...].astype(F32)).astype(BF16)
            self.f = send(self.t1, self.side(self.fr, 1), self.dest(3))

        def finish(self, store):
            arrived(self.c, self.side(self.fl, 1))
            arrived(self.d, self.side(self.fr, 0))
            arrived(self.e, self.side(self.fl, 0))
            arrived(self.f, self.side(self.fr, 1))
            for which in range(2):
                total = (
                    self.piece(0, which)[...].astype(F32)
                    + self.side(self.fl, which)[...].astype(F32)
                    + self.side(self.fr, which)[...].astype(F32)
                )
                store(which, total.astype(BF16))

    def y_piece(buf, start, count):
        def piece(step, which):
            lane = pl.multiple_of(turn(fs, step) * shard + which * (shard // 2), 128)
            return buf.at[pl.ds(start, count), pl.ds(lane, shard // 2)]
        return piece

    def z_piece(buf, start, count, lanes):
        def piece(step, which):
            row = pl.multiple_of(start + turn(rep, step) * count, 16)
            return buf.at[pl.ds(row, count), pl.ds(which * lanes, lanes)]
        return piece

    def x_piece(step, which):
        s = {0: SELF, 1: RIGHT, 3: LEFT, 2: OPP}[step]
        return GX.at[pl.ds(s * block, block), pl.ds(which * (width // 2), width // 2)]

    def strip(buf, count):
        def piece(step):
            row = pl.multiple_of(turn(rep, step) * (count // 4), 16)
            return buf.at[pl.ds(row, count // 4)]
        return piece

    def column(buf):
        def piece(step):
            return buf.at[:, lanes_of(step)]
        return piece

    class Exchange:
        def __init__(self, piece, bufs, dest):
            self.piece, self.bufs, self.dest = piece, bufs, dest

        def start(self):
            self.keys = [
                (send(self.piece(step), self.bufs[step - 1], self.dest(step)), self.bufs[step - 1])
                for step in (2, 1, 3)
            ]

        def finish(self, start):
            for k, landing in self.keys:
                arrived(k, landing)
            total = self.piece(0)[...].astype(F32)
            for buf in self.bufs:
                total = total + buf[...].astype(F32)
            OUTT[pl.ds(start, total.shape[0]), :] = total.astype(BF16)

    class Gather:
        def __init__(self, base, count):
            self.base, self.count = base, count // 4

        def row(self, step):
            return pl.multiple_of(self.base + turn(rep, step) * self.count, 16)

        def region(self, step):
            return OUTT.at[pl.ds(self.row(step), self.count)]

        def start(self):
            self.keys = [
                (send(self.region(0), self.region(0), at_z(step)), 4 - step) for step in (2, 1, 3)
            ]

        def finish(self):
            for k, step in self.keys:
                arrived(k, self.region(step))

    A, B = SPLIT
    a_at = [sum(A[:i]) for i in range(len(A))]
    b_at = [sum(A) + sum(B[:i]) for i in range(len(B))]
    ya = [Ring(y_piece(PW, r, n), bufs, at_y) for r, n, bufs in zip(a_at, A, YA_BUFS)]
    zb = [Ring(z_piece(PW, r, n // 4, width // 2), bufs, at_z) for r, n, bufs in zip(b_at, B, ZB_BUFS)]
    za = [Exchange(strip(buf, n), bufs, at_z) for buf, n, bufs in zip(YA, A, ZA_BUFS)]
    yb = [Exchange(column(buf), bufs, at_y) for buf, bufs in zip(ZB, YB_BUFS)]
    ga = [Gather(r, n) for r, n in zip(a_at, A)]
    gb = [Gather(r, n) for r, n in zip(b_at, B)]
    xr = Ring(x_piece, XR_BUFS, at_x)

    def keep(buf):
        def store(which, value):
            h = value.shape[1]
            buf[:, pl.ds(which * h, h)] = value
        return store

    def weight_piece(step, start, count):
        lanes = lanes_of(step)
        PW[pl.ds(start, count), lanes] = (
            factor * nn(H[pl.ds(start, count), :], X[:, lanes])
        ).astype(BF16)

    def weight_rows(start, count):
        for lo, hi, tokens in ((start, min(start + count, 2 * hid), X), (max(start, 2 * hid), min(start + count, 3 * hid), G)):
            if lo < hi:
                for n in range(4):
                    PW[pl.ds(lo, hi - lo), pl.ds(n * 256, 256)] = (
                        factor * nn(H[pl.ds(lo, hi - lo), :], tokens[:, pl.ds(n * 256, 256)])
                    ).astype(BF16)

    def input_piece(c):
        DX[pl.ds(c * 256, 256), :] = tn(
            H[pl.ds(0, 2 * hid), pl.ds(c * 256, 256)], WT[pl.ds(0, 2 * hid), :]
        ).astype(BF16)

    def across(s):
        landing = DS.at[pl.ds(s * block, block)]
        return send(slot(DX, s, block), landing, sibling)

    def across_add(k, s):
        arrived(k, DS.at[pl.ds(s * block, block)])
        GX[pl.ds(s * block, block), :] = (
            DX[pl.ds(s * 2 * block, block), :].astype(F32)
            + DS[pl.ds(s * block, block), :].astype(F32)
        ).astype(BF16)

    blank = PW.shape[0] - 3 * hid
    PW[pl.ds(3 * hid, blank), :] = jnp.zeros((blank, width), BF16)
    weight_piece(2, 0, A[0])
    ya[0].start_far()
    weight_rows(b_at[0], B[0])
    zb[0].start_far()
    weight_piece(1, 0, A[0])
    weight_piece(3, 0, A[0])
    ya[0].start_near()
    weight_rows(a_at[1], A[1])
    zb[0].start_near()
    weight_rows(b_at[1], B[1])
    ya[1].start_far()
    weight_rows(a_at[2], A[2])
    zb[1].start_far()
    weight_rows(b_at[2], B[2])
    input_piece(2)
    opp = across(OPP)
    ya[1].start_near()
    zb[1].start_near()
    input_piece(1)
    near = across(LEFT), across(RIGHT)
    ya[0].relay()
    input_piece(0)
    mine = across(SELF)
    zb[0].relay()
    weight_piece(0, 0, A[0])
    across_add(opp, OPP)
    xr.start_far()
    zb[2].start_far()
    ya[2].start_far()
    across_add(near[0], LEFT)
    across_add(near[1], RIGHT)
    xr.start_near()
    ya[1].relay()
    zb[1].relay()
    across_add(mine, SELF)
    zb[2].start_near()
    zb[0].finish(keep(ZB[0]))
    yb[0].start()
    ya[0].finish(keep(YA[0]))
    za[0].start()
    ya[2].start_near()
    zb[2].relay()
    ya[2].relay()
    xr.relay()
    zb[1].finish(keep(ZB[1]))
    yb[1].start()
    ya[1].finish(keep(YA[1]))
    za[1].start()
    yb[0].finish(gb[0].row(0))
    gb[0].start()
    za[0].finish(ga[0].row(0))
    ga[0].start()
    zb[2].finish(keep(ZB[2]))
    yb[2].start()
    ya[2].finish(keep(YA[2]))
    za[2].start()
    xr.finish(keep(gin_out))
    yb[1].finish(gb[1].row(0))
    gb[1].start()
    za[1].finish(ga[1].row(0))
    ga[1].start()
    gb[0].finish()
    ga[0].finish()
    yb[2].finish(gb[2].row(0))
    gb[2].start()
    za[2].finish(ga[2].row(0))
    ga[2].start()
    gb[1].finish()
    ga[1].finish()
    gb[2].finish()
    ga[2].finish()
    og_out[...] = OUTT[pl.ds(0, hid), :].astype(F32)
    ou_out[...] = OUTT[pl.ds(hid, hid), :].astype(F32)
    od_out[...] = OUTT[pl.ds(2 * hid, hid), :].astype(F32)

    for copy in pending:
        copy.wait_send()


def writer(*refs):
    sources, targets, sems = refs[:4], refs[4:8], refs[8]
    copies = [pltpu.make_async_copy(a, b, sems.at[i]) for i, (a, b) in enumerate(zip(sources, targets))]
    for copy in copies:
        copy.start()
    for copy in copies:
        copy.wait()


def body(tokens_in, out_grad, gate_weight, up_weight, down_weight):
    block, width = tokens_in.shape
    shard, hid = gate_weight.shape
    devices = lax.axis_size("rep") * lax.axis_size("fs") * lax.axis_size("tp")
    factor = (block * devices) ** (-0.5)
    tokens = block * 8
    A, B = SPLIT
    total_rows = sum(A) + sum(B)

    def ring(count, lanes):
        return [
            pltpu.VMEM((count, lanes // 2), BF16),
            pltpu.VMEM((count, lanes // 2), BF16),
            pltpu.VMEM((count, lanes), BF16),
            pltpu.VMEM((count, lanes), BF16),
        ]

    def exchange(count):
        return [pltpu.VMEM((count // 4, shard), BF16)] * 3

    outs = (
        jax.ShapeDtypeStruct((block, width), BF16),
        jax.ShapeDtypeStruct((hid, shard), F32),
        jax.ShapeDtypeStruct((hid, shard), F32),
        jax.ShapeDtypeStruct((hid, shard), F32),
    )
    arrays = tokens_in, out_grad, gate_weight.T, up_weight.T, down_weight
    results = pl.pallas_call(
        functools.partial(kernel, factor, block, width, hid),
        out_shape=outs,
        in_specs=[pl.BlockSpec(memory_space=pltpu.HBM)] * 5,
        out_specs=[pl.BlockSpec(memory_space=pltpu.VMEM)] * 4,
        scratch_shapes=[
            pltpu.VMEM((tokens, width), BF16),
            pltpu.VMEM((tokens, width), BF16),
            pltpu.VMEM((3 * hid, width), BF16),
            pltpu.VMEM((3 * hid, tokens), BF16),
            pltpu.VMEM((hid, tokens), F32),
            pltpu.VMEM((hid, tokens), F32),
            pltpu.VMEM((total_rows, width), BF16),
            pltpu.VMEM((tokens, width), BF16),
            pltpu.VMEM((tokens // 2, width), BF16),
            pltpu.VMEM((tokens // 2, width), BF16),
            [pltpu.VMEM((n, shard), BF16) for n in A],
            [pltpu.VMEM((n // 4, width), BF16) for n in B],
            pltpu.VMEM((total_rows, shard), BF16),
            [ring(n, shard) for n in A],
            [ring(n // 4, width) for n in B],
            [exchange(n) for n in A],
            [exchange(n) for n in B],
            ring(block, width),
            pltpu.SemaphoreType.DMA((COPIES,)),
            pltpu.SemaphoreType.DMA((COPIES,)),
            pltpu.SemaphoreType.DMA((5,)),
        ],
        compiler_params=pltpu.CompilerParams(
            collective_id=0, has_side_effects=True, vmem_limit_bytes=48 * 1024 * 1024
        ),
    )(*[pltpu.with_memory_space_constraint(a, pltpu.HBM) for a in arrays])
    grad_in, gate_t, up_t, down_t = pl.pallas_call(
        writer,
        out_shape=outs,
        in_specs=[pl.BlockSpec(memory_space=pl.ANY)] * 4,
        out_specs=[pl.BlockSpec(memory_space=pltpu.HBM)] * 4,
        scratch_shapes=[pltpu.SemaphoreType.DMA((4,))],
        compiler_params=pltpu.CompilerParams(vmem_limit_bytes=1024 * 1024),
    )(*results)
    return grad_in, gate_t.T, up_t.T, down_t


def solution(mesh):
    return jax.shard_map(
        body,
        mesh=mesh,
        in_specs=(
            P(("rep", "fs", "tp"), None),
            P(("rep", "fs", "tp"), None),
            P("fs", "tp"),
            P("fs", "tp"),
            P("tp", "fs"),
        ),
        out_specs=(P(("rep", "fs", "tp"), None), P("fs", "tp"), P("fs", "tp"), P("tp", "fs")),
        check_vma=False,
    )
```

```python
import functools

import jax
import jax.numpy as jnp
from jax import lax
from jax.experimental import pallas as pl
from jax.experimental.pallas import tpu as pltpu
from jax.sharding import PartitionSpec as P

BF16 = jnp.bfloat16
F32 = jnp.float32
MESH = pl.DeviceIdType.MESH
COPIES = 144
SPLIT = (192, 192, 192), (128, 256, 128)


def nt(left, right):
    return lax.dot_general(left, right, (((1,), (1,)), ((), ())), preferred_element_type=F32)


def tn(left, right):
    return lax.dot_general(left, right, (((0,), (0,)), ((), ())), preferred_element_type=F32)


def nn(left, right):
    return lax.dot_general(left, right, (((1,), (0,)), ((), ())), preferred_element_type=F32)


def kernel(
    factor, block, width, hid,
    x_in, g_in, wg_in, wu_in, wd_in,
    gin_out, og_out, ou_out, od_out,
    X, G, WT, H, ACT, SLOPE, PW, DX, DS, GX, YA, ZB, OUTT, YA_BUFS, ZB_BUFS, ZA_BUFS, YB_BUFS, XR_BUFS,
    send_sems, recv_sems, local_sems,
):
    rep = lax.axis_index("rep")
    fs = lax.axis_index("fs")
    tp = lax.axis_index("tp")
    core = lax.rem(tp, 2)
    xpos = tp // 2
    shard = width // 4

    def turn(pos, step):
        return lax.rem(pos + step, 4)

    def at_x(step):
        return {"tp": turn(xpos, step) * 2 + core}

    def at_y(step):
        return {"fs": turn(fs, step)}

    def at_z(step):
        return {"rep": turn(rep, step)}

    sibling = {"tp": tp + 1 - 2 * core}

    def lanes_of(step):
        return pl.ds(pl.multiple_of(turn(fs, step) * shard, shard), shard)

    counter = [0]
    pending = []

    def remote(src, dst, k, where):
        return pltpu.make_async_remote_copy(
            src_ref=src, dst_ref=dst, send_sem=send_sems.at[k], recv_sem=recv_sems.at[k],
            device_id=where, device_id_type=MESH,
        )

    def send(src, dst, where):
        k = counter[0]
        counter[0] += 1
        copy = remote(src, dst, k, where)
        copy.start()
        pending.append(copy)
        return k

    def arrived(k, landing):
        remote(landing, landing, k, sibling).wait_recv()

    barrier = pltpu.get_barrier_semaphore()
    partners = [sibling] + [at(step) for at in (at_x, at_y, at_z) for step in (1, 3)]
    partners += [at_y(2), at_z(2)]
    for where in partners:
        pl.semaphore_signal(barrier, inc=1, device_id=where, device_id_type=MESH)

    own_lanes = lanes_of(0)
    loads = [
        pltpu.make_async_copy(x_in, X.at[pl.ds(0, block)], local_sems.at[0]),
        pltpu.make_async_copy(g_in, G.at[pl.ds(0, block)], local_sems.at[1]),
        pltpu.make_async_copy(wg_in, WT.at[pl.ds(0, hid), own_lanes], local_sems.at[2]),
        pltpu.make_async_copy(wu_in, WT.at[pl.ds(hid, hid), own_lanes], local_sems.at[3]),
        pltpu.make_async_copy(wd_in, WT.at[pl.ds(2 * hid, hid), own_lanes], local_sems.at[4]),
    ]
    for load in loads:
        load.start()

    pl.semaphore_wait(barrier, len(partners))

    half = block // 2
    SELF, LEFT, RIGHT, OPP = 0, 1, 2, 3

    def slot(buf, s, start=0, count=block):
        return buf.at[pl.ds(s * 2 * block + start, count)]

    def forward(buf, s, start=0, count=block):
        landing = (s, block + start, count)
        return send(slot(buf, s, start, count), slot(buf, *landing), sibling), landing

    def forwarded(buf, *states):
        for k, landing in states:
            arrived(k, slot(buf, *landing))

    class Tokens:
        def __init__(self, buf):
            self.buf = buf

        def part(self, s, which):
            return slot(self.buf, s, which * half, half)

        def start_first(self):
            self.r0 = send(self.part(SELF, 0), self.part(LEFT, 0), at_x(1))
            self.l1 = send(self.part(SELF, 1), self.part(RIGHT, 1), at_x(3))

        def start_second(self):
            self.r1 = send(self.part(SELF, 1), self.part(LEFT, 1), at_x(1))
            self.l0 = send(self.part(SELF, 0), self.part(RIGHT, 0), at_x(3))

        def relay(self):
            arrived(self.r0, self.part(LEFT, 0))
            self.r2 = send(self.part(LEFT, 0), self.part(OPP, 0), at_x(1))
            arrived(self.l1, self.part(RIGHT, 1))
            self.l2 = send(self.part(RIGHT, 1), self.part(OPP, 1), at_x(3))

        def near(self):
            arrived(self.r1, self.part(LEFT, 1))
            arrived(self.l0, self.part(RIGHT, 0))
            return forward(self.buf, LEFT), forward(self.buf, RIGHT)

        def far(self):
            arrived(self.r2, self.part(OPP, 0))
            first = forward(self.buf, OPP, 0, half)
            arrived(self.l2, self.part(OPP, 1))
            return first, forward(self.buf, OPP, half, half)

    xt, gt = Tokens(X), Tokens(G)
    loads[0].wait()
    xt.start_first()
    xt.start_second()
    loads[1].wait()
    gt.start_first()
    for load in loads[2:]:
        load.wait()

    direct, spare = 384, 96
    base1, base2 = direct, 2 * hid + spare
    dhalf = direct // 2
    D0, D1 = pl.ds(0, dhalf), pl.ds(dhalf, dhalf)
    D2 = pl.ds(2 * hid, spare)

    def w(rows, step):
        return WT.at[rows, lanes_of(step)]

    def copy_w(rows, step, where):
        return send(w(rows, step), w(rows, step), where)

    class Quarters:
        def __init__(self, base, end):
            self.base, self.part = base, (end - base) // 4
            self.cut = (self.part // 2 + 15) // 16 * 16

        def rows(self, step, which=None):
            start, count = {
                None: (0, self.part), 0: (0, self.cut), 1: (self.cut, self.part - self.cut)
            }[which]
            return pl.ds(pl.multiple_of(self.base + turn(rep, step) * self.part + start, 16), count)

        def start(self):
            self.r, self.l = copy_w(self.rows(0), 0, at_y(1)), copy_w(self.rows(0), 0, at_y(3))
            self.shares = {}

        def relay(self):
            arrived(self.r, w(self.rows(0), 3))
            self.r2 = copy_w(self.rows(0, 0), 3, at_y(1))
            arrived(self.l, w(self.rows(0), 1))
            self.l2 = copy_w(self.rows(0, 1), 1, at_y(3))

        def far(self):
            arrived(self.r2, w(self.rows(0, 0), 2))
            arrived(self.l2, w(self.rows(0, 1), 2))

        def share(self, lane):
            self.shares[lane] = [
                (copy_w(self.rows(0), lane, at_z(step)), 4 - step) for step in (2, 1, 3)
            ]

        def finish(self):
            for lane, keys in self.shares.items():
                for k, step in keys:
                    arrived(k, w(self.rows(step), lane))

    q1, q2 = Quarters(base1, 2 * hid), Quarters(base2, 3 * hid)
    q1.start()
    q2.start()
    d0r = copy_w(D0, 0, at_y(1))
    d1l = copy_w(D1, 0, at_y(3))
    x_own = forward(X, SELF)
    g_own = forward(G, SELF)

    q1.relay()
    q1.share(3)
    q1.share(1)
    q2.relay()
    d1r = copy_w(D1, 0, at_y(1))
    d0l = copy_w(D0, 0, at_y(3))

    xt.relay()
    gt.start_second()
    arrived(d0r, w(D0, 3))
    dc = copy_w(D0, 3, at_y(1))
    arrived(d1l, w(D1, 1))
    dd = copy_w(D1, 1, at_y(3))
    x_near = xt.near()
    q1.far()
    q1.share(2)
    q2.share(3)
    q2.share(1)
    q2.far()
    q2.share(2)
    d2 = [(copy_w(D2, 0, at_y(step)), 4 - step) for step in (2, 1, 3)]
    gt.relay()
    x_far = xt.far()

    forwarded(X, x_own, *x_near)
    arrived(d1r, w(D1, 3))
    arrived(d0l, w(D0, 1))
    q1.finish()
    arrived(dc, w(D0, 2))
    arrived(dd, w(D1, 2))

    rows = hid // 2

    def gate_stage(c):
        cols = pl.ds(c * 256, 256)
        for p in range(2):
            part_rows = pl.ds(p * rows, rows)
            gate = nt(WT[part_rows, :], X[cols, :]).astype(BF16).astype(F32)
            up = nt(WT[pl.ds(hid + p * rows, rows), :], X[cols, :]).astype(BF16).astype(F32)
            sig = jax.nn.sigmoid(gate)
            act = gate * sig
            H[pl.ds(2 * hid + p * rows, rows), cols] = (act * up).astype(BF16)
            ACT[part_rows, cols] = act
            SLOPE[part_rows, cols] = up * sig * (1.0 + gate * (1.0 - sig))

    def grad_stage(c):
        cols = pl.ds(c * 256, 256)
        grad = nt(WT[pl.ds(2 * hid, hid), :], G[cols, :]).astype(BF16).astype(F32)
        H[pl.ds(0, hid), cols] = (grad * SLOPE[:, cols]).astype(BF16)
        H[pl.ds(hid, hid), cols] = (grad * ACT[:, cols]).astype(BF16)

    gate_stage(0)
    gate_stage(1)
    g_near = gt.near()
    forwarded(X, *x_far)
    gate_stage(2)
    q2.finish()
    for k, step in d2:
        arrived(k, w(D2, step))
    forwarded(G, g_own, g_near[0])
    g_far = gt.far()
    grad_stage(0)
    forwarded(G, g_near[1])
    grad_stage(1)
    forwarded(G, *g_far)
    grad_stage(2)

    class Ring:
        def __init__(self, piece, bufs, dest):
            self.piece, self.dest = piece, dest
            self.t0, self.t1, self.fl, self.fr = bufs
            self.h = self.t0.shape[1]

        def side(self, buf, which):
            return buf.at[:, pl.ds(which * self.h, self.h)]

        def start_far(self):
            self.a = send(self.piece(2, 0), self.t0, self.dest(1))
            self.b = send(self.piece(2, 1), self.t1, self.dest(3))

        def start_near(self):
            self.c = send(self.piece(1, 1), self.side(self.fl, 1), self.dest(1))
            self.d = send(self.piece(3, 0), self.side(self.fr, 0), self.dest(3))

        def relay(self):
            arrived(self.a, self.t0)
            self.t0[...] = (self.t0[...].astype(F32) + self.piece(1, 0)[...].astype(F32)).astype(BF16)
            self.e = send(self.t0, self.side(self.fl, 0), self.dest(1))
            arrived(self.b, self.t1)
            self.t1[...] = (self.t1[...].astype(F32) + self.piece(3, 1)[...].astype(F32)).astype(BF16)
            self.f = send(self.t1, self.side(self.fr, 1), self.dest(3))

        def finish(self, store):
            arrived(self.c, self.side(self.fl, 1))
            arrived(self.d, self.side(self.fr, 0))
            arrived(self.e, self.side(self.fl, 0))
            arrived(self.f, self.side(self.fr, 1))
            for which in range(2):
                total = (
                    self.piece(0, which)[...].astype(F32)
                    + self.side(self.fl, which)[...].astype(F32)
                    + self.side(self.fr, which)[...].astype(F32)
                )
                store(which, total.astype(BF16))

    def y_piece(buf, start, count):
        def piece(step, which):
            lane = pl.multiple_of(turn(fs, step) * shard + which * (shard // 2), 128)
            return buf.at[pl.ds(start, count), pl.ds(lane, shard // 2)]
        return piece

    def z_piece(buf, start, count, lanes):
        def piece(step, which):
            row = pl.multiple_of(start + turn(rep, step) * count, 16)
            return buf.at[pl.ds(row, count), pl.ds(which * lanes, lanes)]
        return piece

    def x_piece(step, which):
        s = {0: SELF, 1: RIGHT, 3: LEFT, 2: OPP}[step]
        return GX.at[pl.ds(s * block, block), pl.ds(which * (width // 2), width // 2)]

    def strip(buf, count):
        def piece(step):
            row = pl.multiple_of(turn(rep, step) * (count // 4), 16)
            return buf.at[pl.ds(row, count // 4)]
        return piece

    def column(buf):
        def piece(step):
            return buf.at[:, lanes_of(step)]
        return piece

    class Exchange:
        def __init__(self, piece, bufs, dest):
            self.piece, self.bufs, self.dest = piece, bufs, dest

        def start(self):
            self.keys = [
                (send(self.piece(step), self.bufs[step - 1], self.dest(step)), self.bufs[step - 1])
                for step in (2, 1, 3)
            ]

        def finish(self, start):
            for k, landing in self.keys:
                arrived(k, landing)
            total = self.piece(0)[...].astype(F32)
            for buf in self.bufs:
                total = total + buf[...].astype(F32)
            OUTT[pl.ds(start, total.shape[0]), :] = total.astype(BF16)

    class Gather:
        def __init__(self, base, count):
            self.base, self.count = base, count // 4

        def row(self, step):
            return pl.multiple_of(self.base + turn(rep, step) * self.count, 16)

        def region(self, step):
            return OUTT.at[pl.ds(self.row(step), self.count)]

        def start(self):
            self.keys = [
                (send(self.region(0), self.region(0), at_z(step)), 4 - step) for step in (2, 1, 3)
            ]

        def finish(self):
            for k, step in self.keys:
                arrived(k, self.region(step))

    A, B = SPLIT
    a_at = [sum(A[:i]) for i in range(len(A))]
    b_at = [sum(A) + sum(B[:i]) for i in range(len(B))]
    ya = [Ring(y_piece(PW, r, n), bufs, at_y) for r, n, bufs in zip(a_at, A, YA_BUFS)]
    zb = [Ring(z_piece(PW, r, n // 4, width // 2), bufs, at_z) for r, n, bufs in zip(b_at, B, ZB_BUFS)]
    za = [Exchange(strip(buf, n), bufs, at_z) for buf, n, bufs in zip(YA, A, ZA_BUFS)]
    yb = [Exchange(column(buf), bufs, at_y) for buf, bufs in zip(ZB, YB_BUFS)]
    ga = [Gather(r, n) for r, n in zip(a_at, A)]
    gb = [Gather(r, n) for r, n in zip(b_at, B)]
    xr = Ring(x_piece, XR_BUFS, at_x)

    def keep(buf):
        def store(which, value):
            h = value.shape[1]
            buf[:, pl.ds(which * h, h)] = value
        return store

    def weight_piece(step, start, count):
        lanes = lanes_of(step)
        PW[pl.ds(start, count), lanes] = (
            factor * nn(H[pl.ds(start, count), :], X[:, lanes])
        ).astype(BF16)

    def weight_rows(start, count):
        for lo, hi, tokens in ((start, min(start + count, 2 * hid), X), (max(start, 2 * hid), min(start + count, 3 * hid), G)):
            if lo < hi:
                for n in range(4):
                    PW[pl.ds(lo, hi - lo), pl.ds(n * 256, 256)] = (
                        factor * nn(H[pl.ds(lo, hi - lo), :], tokens[:, pl.ds(n * 256, 256)])
                    ).astype(BF16)

    def input_piece(c):
        DX[pl.ds(c * 256, 256), :] = tn(
            H[pl.ds(0, 2 * hid), pl.ds(c * 256, 256)], WT[pl.ds(0, 2 * hid), :]
        ).astype(BF16)

    def across(s):
        landing = DS.at[pl.ds(s * block, block)]
        return send(slot(DX, s, block), landing, sibling)

    def across_add(k, s):
        arrived(k, DS.at[pl.ds(s * block, block)])
        GX[pl.ds(s * block, block), :] = (
            DX[pl.ds(s * 2 * block, block), :].astype(F32)
            + DS[pl.ds(s * block, block), :].astype(F32)
        ).astype(BF16)

    blank = PW.shape[0] - 3 * hid
    PW[pl.ds(3 * hid, blank), :] = jnp.zeros((blank, width), BF16)
    weight_piece(2, 0, A[0])
    ya[0].start_far()
    weight_rows(b_at[0], B[0])
    zb[0].start_far()
    weight_piece(1, 0, A[0])
    zb[0].start_near()
    weight_piece(3, 0, A[0])
    ya[0].start_near()
    weight_rows(a_at[1], A[1])
    weight_rows(b_at[1], B[1])
    ya[1].start_far()
    zb[1].start_far()
    weight_rows(a_at[2], A[2])
    weight_rows(b_at[2], B[2])
    ya[1].start_near()
    input_piece(2)
    opp = across(OPP)
    ya[0].relay()
    zb[0].relay()
    input_piece(1)
    near = across(LEFT), across(RIGHT)
    zb[1].start_near()
    input_piece(0)
    mine = across(SELF)
    ya[2].start_far()
    weight_piece(0, 0, A[0])
    across_add(opp, OPP)
    xr.start_far()
    zb[2].start_far()
    ya[1].relay()
    zb[1].relay()
    across_add(near[0], LEFT)
    across_add(near[1], RIGHT)
    xr.start_near()
    across_add(mine, SELF)
    zb[0].finish(keep(ZB[0]))
    yb[0].start()
    zb[2].start_near()
    ya[2].start_near()
    ya[0].finish(keep(YA[0]))
    za[0].start()
    ya[2].relay()
    zb[2].relay()
    xr.relay()
    ya[1].finish(keep(YA[1]))
    za[1].start()
    zb[1].finish(keep(ZB[1]))
    yb[1].start()
    yb[0].finish(gb[0].row(0))
    gb[0].start()
    za[0].finish(ga[0].row(0))
    ga[0].start()
    ya[2].finish(keep(YA[2]))
    za[2].start()
    zb[2].finish(keep(ZB[2]))
    yb[2].start()
    za[1].finish(ga[1].row(0))
    ga[1].start()
    yb[1].finish(gb[1].row(0))
    gb[1].start()
    xr.finish(keep(gin_out))
    gb[0].finish()
    ga[0].finish()
    yb[2].finish(gb[2].row(0))
    gb[2].start()
    za[2].finish(ga[2].row(0))
    ga[2].start()
    ga[1].finish()
    gb[1].finish()
    gb[2].finish()
    ga[2].finish()
    og_out[...] = OUTT[pl.ds(0, hid), :].astype(F32)
    ou_out[...] = OUTT[pl.ds(hid, hid), :].astype(F32)
    od_out[...] = OUTT[pl.ds(2 * hid, hid), :].astype(F32)

    for copy in pending:
        copy.wait_send()


def writer(*refs):
    sources, targets, sems = refs[:4], refs[4:8], refs[8]
    copies = [pltpu.make_async_copy(a, b, sems.at[i]) for i, (a, b) in enumerate(zip(sources, targets))]
    for copy in copies:
        copy.start()
    for copy in copies:
        copy.wait()


def body(tokens_in, out_grad, gate_weight, up_weight, down_weight):
    block, width = tokens_in.shape
    shard, hid = gate_weight.shape
    devices = lax.axis_size("rep") * lax.axis_size("fs") * lax.axis_size("tp")
    factor = (block * devices) ** (-0.5)
    tokens = block * 8
    A, B = SPLIT
    total_rows = sum(A) + sum(B)

    def ring(count, lanes):
        return [
            pltpu.VMEM((count, lanes // 2), BF16),
            pltpu.VMEM((count, lanes // 2), BF16),
            pltpu.VMEM((count, lanes), BF16),
            pltpu.VMEM((count, lanes), BF16),
        ]

    def exchange(count):
        return [pltpu.VMEM((count // 4, shard), BF16)] * 3

    outs = (
        jax.ShapeDtypeStruct((block, width), BF16),
        jax.ShapeDtypeStruct((hid, shard), F32),
        jax.ShapeDtypeStruct((hid, shard), F32),
        jax.ShapeDtypeStruct((hid, shard), F32),
    )
    arrays = tokens_in, out_grad, gate_weight.T, up_weight.T, down_weight
    results = pl.pallas_call(
        functools.partial(kernel, factor, block, width, hid),
        out_shape=outs,
        in_specs=[pl.BlockSpec(memory_space=pltpu.HBM)] * 5,
        out_specs=[pl.BlockSpec(memory_space=pltpu.VMEM)] * 4,
        scratch_shapes=[
            pltpu.VMEM((tokens, width), BF16),
            pltpu.VMEM((tokens, width), BF16),
            pltpu.VMEM((3 * hid, width), BF16),
            pltpu.VMEM((3 * hid, tokens), BF16),
            pltpu.VMEM((hid, tokens), F32),
            pltpu.VMEM((hid, tokens), F32),
            pltpu.VMEM((total_rows, width), BF16),
            pltpu.VMEM((tokens, width), BF16),
            pltpu.VMEM((tokens // 2, width), BF16),
            pltpu.VMEM((tokens // 2, width), BF16),
            [pltpu.VMEM((n, shard), BF16) for n in A],
            [pltpu.VMEM((n // 4, width), BF16) for n in B],
            pltpu.VMEM((total_rows, shard), BF16),
            [ring(n, shard) for n in A],
            [ring(n // 4, width) for n in B],
            [exchange(n) for n in A],
            [exchange(n) for n in B],
            ring(block, width),
            pltpu.SemaphoreType.DMA((COPIES,)),
            pltpu.SemaphoreType.DMA((COPIES,)),
            pltpu.SemaphoreType.DMA((5,)),
        ],
        compiler_params=pltpu.CompilerParams(
            collective_id=0, has_side_effects=True, vmem_limit_bytes=48 * 1024 * 1024
        ),
    )(*[pltpu.with_memory_space_constraint(a, pltpu.HBM) for a in arrays])
    grad_in, gate_t, up_t, down_t = pl.pallas_call(
        writer,
        out_shape=outs,
        in_specs=[pl.BlockSpec(memory_space=pl.ANY)] * 4,
        out_specs=[pl.BlockSpec(memory_space=pltpu.HBM)] * 4,
        scratch_shapes=[pltpu.SemaphoreType.DMA((4,))],
        compiler_params=pltpu.CompilerParams(vmem_limit_bytes=1024 * 1024),
    )(*results)
    return grad_in, gate_t.T, up_t.T, down_t


def solution(mesh):
    return jax.shard_map(
        body,
        mesh=mesh,
        in_specs=(
            P(("rep", "fs", "tp"), None),
            P(("rep", "fs", "tp"), None),
            P("fs", "tp"),
            P("fs", "tp"),
            P("tp", "fs"),
        ),
        out_specs=(P(("rep", "fs", "tp"), None), P("fs", "tp"), P("fs", "tp"), P("tp", "fs")),
        check_vma=False,
    )
```

```python
import functools

import jax
import jax.numpy as jnp
from jax import lax
from jax.experimental import pallas as pl
from jax.experimental.pallas import tpu as pltpu
from jax.sharding import PartitionSpec as P

BF16 = jnp.bfloat16
F32 = jnp.float32
MESH = pl.DeviceIdType.MESH
COPIES = 144
SPLIT = (256, 128, 192), (192, 128, 192)


def nt(left, right):
    return lax.dot_general(left, right, (((1,), (1,)), ((), ())), preferred_element_type=F32)


def tn(left, right):
    return lax.dot_general(left, right, (((0,), (0,)), ((), ())), preferred_element_type=F32)


def nn(left, right):
    return lax.dot_general(left, right, (((1,), (0,)), ((), ())), preferred_element_type=F32)


def kernel(
    factor, block, width, hid,
    x_in, g_in, wg_in, wu_in, wd_in,
    gin_out, og_out, ou_out, od_out,
    X, G, WT, H, ACT, SLOPE, PW, DX, DS, GX, YA, ZB, OUTT, YA_BUFS, ZB_BUFS, ZA_BUFS, YB_BUFS, XR_BUFS,
    send_sems, recv_sems, local_sems,
):
    rep = lax.axis_index("rep")
    fs = lax.axis_index("fs")
    tp = lax.axis_index("tp")
    core = lax.rem(tp, 2)
    xpos = tp // 2
    shard = width // 4

    def turn(pos, step):
        return lax.rem(pos + step, 4)

    def at_x(step):
        return {"tp": turn(xpos, step) * 2 + core}

    def at_y(step):
        return {"fs": turn(fs, step)}

    def at_z(step):
        return {"rep": turn(rep, step)}

    sibling = {"tp": tp + 1 - 2 * core}

    def lanes_of(step):
        return pl.ds(pl.multiple_of(turn(fs, step) * shard, shard), shard)

    counter = [0]
    pending = []

    def remote(src, dst, k, where):
        return pltpu.make_async_remote_copy(
            src_ref=src, dst_ref=dst, send_sem=send_sems.at[k], recv_sem=recv_sems.at[k],
            device_id=where, device_id_type=MESH,
        )

    def send(src, dst, where):
        k = counter[0]
        counter[0] += 1
        copy = remote(src, dst, k, where)
        copy.start()
        pending.append(copy)
        return k

    def arrived(k, landing):
        remote(landing, landing, k, sibling).wait_recv()

    barrier = pltpu.get_barrier_semaphore()
    partners = [sibling] + [at(step) for at in (at_x, at_y, at_z) for step in (1, 3)]
    partners += [at_y(2), at_z(2)]
    for where in partners:
        pl.semaphore_signal(barrier, inc=1, device_id=where, device_id_type=MESH)

    own_lanes = lanes_of(0)
    loads = [
        pltpu.make_async_copy(x_in, X.at[pl.ds(0, block)], local_sems.at[0]),
        pltpu.make_async_copy(g_in, G.at[pl.ds(0, block)], local_sems.at[1]),
        pltpu.make_async_copy(wg_in, WT.at[pl.ds(0, hid), own_lanes], local_sems.at[2]),
        pltpu.make_async_copy(wu_in, WT.at[pl.ds(hid, hid), own_lanes], local_sems.at[3]),
        pltpu.make_async_copy(wd_in, WT.at[pl.ds(2 * hid, hid), own_lanes], local_sems.at[4]),
    ]
    for load in loads:
        load.start()

    pl.semaphore_wait(barrier, len(partners))

    half = block // 2
    SELF, LEFT, RIGHT, OPP = 0, 1, 2, 3

    def slot(buf, s, start=0, count=block):
        return buf.at[pl.ds(s * 2 * block + start, count)]

    def forward(buf, s, start=0, count=block):
        landing = (s, block + start, count)
        return send(slot(buf, s, start, count), slot(buf, *landing), sibling), landing

    def forwarded(buf, *states):
        for k, landing in states:
            arrived(k, slot(buf, *landing))

    class Tokens:
        def __init__(self, buf):
            self.buf = buf

        def part(self, s, which):
            return slot(self.buf, s, which * half, half)

        def start_first(self):
            self.r0 = send(self.part(SELF, 0), self.part(LEFT, 0), at_x(1))
            self.l1 = send(self.part(SELF, 1), self.part(RIGHT, 1), at_x(3))

        def start_second(self):
            self.r1 = send(self.part(SELF, 1), self.part(LEFT, 1), at_x(1))
            self.l0 = send(self.part(SELF, 0), self.part(RIGHT, 0), at_x(3))

        def relay(self):
            arrived(self.r0, self.part(LEFT, 0))
            self.r2 = send(self.part(LEFT, 0), self.part(OPP, 0), at_x(1))
            arrived(self.l1, self.part(RIGHT, 1))
            self.l2 = send(self.part(RIGHT, 1), self.part(OPP, 1), at_x(3))

        def near(self):
            arrived(self.r1, self.part(LEFT, 1))
            arrived(self.l0, self.part(RIGHT, 0))
            return forward(self.buf, LEFT), forward(self.buf, RIGHT)

        def far(self):
            arrived(self.r2, self.part(OPP, 0))
            first = forward(self.buf, OPP, 0, half)
            arrived(self.l2, self.part(OPP, 1))
            return first, forward(self.buf, OPP, half, half)

    xt, gt = Tokens(X), Tokens(G)
    loads[0].wait()
    xt.start_first()
    xt.start_second()
    loads[1].wait()
    gt.start_first()
    for load in loads[2:]:
        load.wait()

    direct, spare = 384, 96
    base1, base2 = direct, 2 * hid + spare
    dhalf = direct // 2
    D0, D1 = pl.ds(0, dhalf), pl.ds(dhalf, dhalf)
    D2 = pl.ds(2 * hid, spare)

    def w(rows, step):
        return WT.at[rows, lanes_of(step)]

    def copy_w(rows, step, where):
        return send(w(rows, step), w(rows, step), where)

    class Quarters:
        def __init__(self, base, end):
            self.base, self.part = base, (end - base) // 4
            self.cut = (self.part // 2 + 15) // 16 * 16

        def rows(self, step, which=None):
            start, count = {
                None: (0, self.part), 0: (0, self.cut), 1: (self.cut, self.part - self.cut)
            }[which]
            return pl.ds(pl.multiple_of(self.base + turn(rep, step) * self.part + start, 16), count)

        def start(self):
            self.r, self.l = copy_w(self.rows(0), 0, at_y(1)), copy_w(self.rows(0), 0, at_y(3))
            self.shares = {}

        def relay(self):
            arrived(self.r, w(self.rows(0), 3))
            self.r2 = copy_w(self.rows(0, 0), 3, at_y(1))
            arrived(self.l, w(self.rows(0), 1))
            self.l2 = copy_w(self.rows(0, 1), 1, at_y(3))

        def far(self):
            arrived(self.r2, w(self.rows(0, 0), 2))
            arrived(self.l2, w(self.rows(0, 1), 2))

        def share(self, lane):
            self.shares[lane] = [
                (copy_w(self.rows(0), lane, at_z(step)), 4 - step) for step in (2, 1, 3)
            ]

        def finish(self):
            for lane, keys in self.shares.items():
                for k, step in keys:
                    arrived(k, w(self.rows(step), lane))

    q1, q2 = Quarters(base1, 2 * hid), Quarters(base2, 3 * hid)
    q1.start()
    q2.start()
    d0r = copy_w(D0, 0, at_y(1))
    d1l = copy_w(D1, 0, at_y(3))
    x_own = forward(X, SELF)
    g_own = forward(G, SELF)

    q1.relay()
    q1.share(3)
    q1.share(1)
    q2.relay()
    d1r = copy_w(D1, 0, at_y(1))
    d0l = copy_w(D0, 0, at_y(3))

    xt.relay()
    gt.start_second()
    arrived(d0r, w(D0, 3))
    dc = copy_w(D0, 3, at_y(1))
    arrived(d1l, w(D1, 1))
    dd = copy_w(D1, 1, at_y(3))
    x_near = xt.near()
    q1.far()
    q1.share(2)
    q2.share(3)
    q2.share(1)
    q2.far()
    q2.share(2)
    d2 = [(copy_w(D2, 0, at_y(step)), 4 - step) for step in (2, 1, 3)]
    gt.relay()
    x_far = xt.far()

    forwarded(X, x_own, *x_near)
    arrived(d1r, w(D1, 3))
    arrived(d0l, w(D0, 1))
    q1.finish()
    arrived(dc, w(D0, 2))
    arrived(dd, w(D1, 2))

    rows = hid // 2

    def gate_stage(c):
        cols = pl.ds(c * 256, 256)
        for p in range(2):
            part_rows = pl.ds(p * rows, rows)
            gate = nt(WT[part_rows, :], X[cols, :]).astype(BF16).astype(F32)
            up = nt(WT[pl.ds(hid + p * rows, rows), :], X[cols, :]).astype(BF16).astype(F32)
            sig = jax.nn.sigmoid(gate)
            act = gate * sig
            H[pl.ds(2 * hid + p * rows, rows), cols] = (act * up).astype(BF16)
            ACT[part_rows, cols] = act
            SLOPE[part_rows, cols] = up * sig * (1.0 + gate * (1.0 - sig))

    def grad_stage(c):
        cols = pl.ds(c * 256, 256)
        grad = nt(WT[pl.ds(2 * hid, hid), :], G[cols, :]).astype(BF16).astype(F32)
        H[pl.ds(0, hid), cols] = (grad * SLOPE[:, cols]).astype(BF16)
        H[pl.ds(hid, hid), cols] = (grad * ACT[:, cols]).astype(BF16)

    gate_stage(0)
    gate_stage(1)
    g_near = gt.near()
    forwarded(X, *x_far)
    gate_stage(2)
    q2.finish()
    for k, step in d2:
        arrived(k, w(D2, step))
    forwarded(G, g_own, g_near[0])
    g_far = gt.far()
    grad_stage(0)
    forwarded(G, g_near[1])
    grad_stage(1)
    forwarded(G, *g_far)
    grad_stage(2)

    class Ring:
        def __init__(self, piece, bufs, dest):
            self.piece, self.dest = piece, dest
            self.t0, self.t1, self.fl, self.fr = bufs
            self.h = self.t0.shape[1]

        def side(self, buf, which):
            return buf.at[:, pl.ds(which * self.h, self.h)]

        def start_far(self):
            self.a = send(self.piece(2, 0), self.t0, self.dest(1))
            self.b = send(self.piece(2, 1), self.t1, self.dest(3))

        def start_near(self):
            self.c = send(self.piece(1, 1), self.side(self.fl, 1), self.dest(1))
            self.d = send(self.piece(3, 0), self.side(self.fr, 0), self.dest(3))

        def relay(self):
            arrived(self.a, self.t0)
            self.t0[...] = (self.t0[...].astype(F32) + self.piece(1, 0)[...].astype(F32)).astype(BF16)
            self.e = send(self.t0, self.side(self.fl, 0), self.dest(1))
            arrived(self.b, self.t1)
            self.t1[...] = (self.t1[...].astype(F32) + self.piece(3, 1)[...].astype(F32)).astype(BF16)
            self.f = send(self.t1, self.side(self.fr, 1), self.dest(3))

        def finish(self, store):
            arrived(self.c, self.side(self.fl, 1))
            arrived(self.d, self.side(self.fr, 0))
            arrived(self.e, self.side(self.fl, 0))
            arrived(self.f, self.side(self.fr, 1))
            for which in range(2):
                total = (
                    self.piece(0, which)[...].astype(F32)
                    + self.side(self.fl, which)[...].astype(F32)
                    + self.side(self.fr, which)[...].astype(F32)
                )
                store(which, total.astype(BF16))

    def y_piece(buf, start, count):
        def piece(step, which):
            lane = pl.multiple_of(turn(fs, step) * shard + which * (shard // 2), 128)
            return buf.at[pl.ds(start, count), pl.ds(lane, shard // 2)]
        return piece

    def z_piece(buf, start, count, lanes):
        def piece(step, which):
            row = pl.multiple_of(start + turn(rep, step) * count, 16)
            return buf.at[pl.ds(row, count), pl.ds(which * lanes, lanes)]
        return piece

    def x_piece(step, which):
        s = {0: SELF, 1: RIGHT, 3: LEFT, 2: OPP}[step]
        return GX.at[pl.ds(s * block, block), pl.ds(which * (width // 2), width // 2)]

    def strip(buf, count):
        def piece(step):
            row = pl.multiple_of(turn(rep, step) * (count // 4), 16)
            return buf.at[pl.ds(row, count // 4)]
        return piece

    def column(buf):
        def piece(step):
            return buf.at[:, lanes_of(step)]
        return piece

    class Exchange:
        def __init__(self, piece, bufs, dest):
            self.piece, self.bufs, self.dest = piece, bufs, dest

        def start(self):
            self.keys = [
                (send(self.piece(step), self.bufs[step - 1], self.dest(step)), self.bufs[step - 1])
                for step in (2, 1, 3)
            ]

        def finish(self, start):
            for k, landing in self.keys:
                arrived(k, landing)
            total = self.piece(0)[...].astype(F32)
            for buf in self.bufs:
                total = total + buf[...].astype(F32)
            OUTT[pl.ds(start, total.shape[0]), :] = total.astype(BF16)

    class Gather:
        def __init__(self, base, count, relayed):
            self.base, self.count, self.relayed = base, count // 4, relayed

        def row(self, step):
            return pl.multiple_of(self.base + turn(rep, step) * self.count, 16)

        def region(self, step, which=None):
            rows = pl.ds(self.row(step), self.count)
            if which is None:
                return OUTT.at[rows]
            return OUTT.at[rows, pl.ds(which * (shard // 2), shard // 2)]

        def start(self):
            steps = (1, 3) if self.relayed else (2, 1, 3)
            self.keys = [
                (send(self.region(0), self.region(0), at_z(step)), 4 - step) for step in steps
            ]

        def relay(self):
            (right, _), (left, _) = self.keys
            arrived(right, self.region(3))
            first = send(self.region(3, 0), self.region(3, 0), at_z(1))
            arrived(left, self.region(1))
            second = send(self.region(1, 1), self.region(1, 1), at_z(3))
            self.keys = first, second

        def finish(self):
            if self.relayed:
                for which, k in enumerate(self.keys):
                    arrived(k, self.region(2, which))
            else:
                for k, step in self.keys:
                    arrived(k, self.region(step))

    A, B = SPLIT
    a_at = [sum(A[:i]) for i in range(len(A))]
    b_at = [sum(A) + sum(B[:i]) for i in range(len(B))]
    ya = [Ring(y_piece(PW, r, n), bufs, at_y) for r, n, bufs in zip(a_at, A, YA_BUFS)]
    zb = [Ring(z_piece(PW, r, n // 4, width // 2), bufs, at_z) for r, n, bufs in zip(b_at, B, ZB_BUFS)]
    za = [Exchange(strip(buf, n), bufs, at_z) for buf, n, bufs in zip(YA, A, ZA_BUFS)]
    yb = [Exchange(column(buf), bufs, at_y) for buf, bufs in zip(ZB, YB_BUFS)]
    ga = [Gather(r, n, i < 2) for i, (r, n) in enumerate(zip(a_at, A))]
    gb = [Gather(r, n, i < 2) for i, (r, n) in enumerate(zip(b_at, B))]
    xr = Ring(x_piece, XR_BUFS, at_x)

    def keep(buf):
        def store(which, value):
            h = value.shape[1]
            buf[:, pl.ds(which * h, h)] = value
        return store

    def weight_piece(step, start, count):
        lanes = lanes_of(step)
        PW[pl.ds(start, count), lanes] = (
            factor * nn(H[pl.ds(start, count), :], X[:, lanes])
        ).astype(BF16)

    def weight_rows(start, count):
        for lo, hi, tokens in ((start, min(start + count, 2 * hid), X), (max(start, 2 * hid), min(start + count, 3 * hid), G)):
            if lo < hi:
                for n in range(4):
                    PW[pl.ds(lo, hi - lo), pl.ds(n * 256, 256)] = (
                        factor * nn(H[pl.ds(lo, hi - lo), :], tokens[:, pl.ds(n * 256, 256)])
                    ).astype(BF16)

    def input_piece(c):
        DX[pl.ds(c * 256, 256), :] = tn(
            H[pl.ds(0, 2 * hid), pl.ds(c * 256, 256)], WT[pl.ds(0, 2 * hid), :]
        ).astype(BF16)

    def across(s):
        landing = DS.at[pl.ds(s * block, block)]
        return send(slot(DX, s, block), landing, sibling)

    def across_add(k, s):
        arrived(k, DS.at[pl.ds(s * block, block)])
        GX[pl.ds(s * block, block), :] = (
            DX[pl.ds(s * 2 * block, block), :].astype(F32)
            + DS[pl.ds(s * block, block), :].astype(F32)
        ).astype(BF16)

    blank = PW.shape[0] - 3 * hid
    PW[pl.ds(3 * hid, blank), :] = jnp.zeros((blank, width), BF16)
    weight_piece(2, 0, A[0])
    ya[0].start_far()
    weight_rows(b_at[0], B[0])
    zb[0].start_far()
    weight_piece(1, 0, A[0])
    zb[0].start_near()
    weight_piece(3, 0, A[0])
    ya[0].start_near()
    weight_rows(a_at[1], A[1])
    weight_rows(b_at[1], B[1])
    ya[1].start_far()
    zb[1].start_far()
    weight_rows(a_at[2], A[2])
    zb[1].start_near()
    weight_rows(b_at[2], B[2])
    ya[1].start_near()
    input_piece(2)
    opp = across(OPP)
    ya[2].start_far()
    zb[2].start_far()
    input_piece(1)
    near = across(LEFT), across(RIGHT)
    ya[0].relay()
    zb[0].relay()
    input_piece(0)
    mine = across(SELF)
    across_add(opp, OPP)
    xr.start_far()
    weight_piece(0, 0, A[0])
    zb[2].start_near()
    across_add(near[0], LEFT)
    across_add(near[1], RIGHT)
    zb[1].relay()
    xr.start_near()
    ya[2].start_near()
    ya[1].relay()
    across_add(mine, SELF)
    zb[2].relay()
    ya[2].relay()
    zb[0].finish(keep(ZB[0]))
    yb[0].start()
    ya[0].finish(keep(YA[0]))
    za[0].start()
    xr.relay()
    zb[1].finish(keep(ZB[1]))
    yb[1].start()
    ya[1].finish(keep(YA[1]))
    za[1].start()
    zb[2].finish(keep(ZB[2]))
    yb[2].start()
    ya[2].finish(keep(YA[2]))
    za[2].start()
    yb[0].finish(gb[0].row(0))
    gb[0].start()
    za[0].finish(ga[0].row(0))
    ga[0].start()
    yb[1].finish(gb[1].row(0))
    gb[1].start()
    xr.finish(keep(gin_out))
    za[1].finish(ga[1].row(0))
    ga[1].start()
    yb[2].finish(gb[2].row(0))
    gb[2].start()
    za[2].finish(ga[2].row(0))
    ga[2].start()
    gb[0].relay()
    ga[0].relay()
    gb[1].relay()
    ga[1].relay()
    gb[2].finish()
    ga[2].finish()
    gb[0].finish()
    ga[0].finish()
    gb[1].finish()
    ga[1].finish()
    og_out[...] = OUTT[pl.ds(0, hid), :].astype(F32)
    ou_out[...] = OUTT[pl.ds(hid, hid), :].astype(F32)
    od_out[...] = OUTT[pl.ds(2 * hid, hid), :].astype(F32)

    for copy in pending:
        copy.wait_send()


def writer(*refs):
    sources, targets, sems = refs[:4], refs[4:8], refs[8]
    copies = [pltpu.make_async_copy(a, b, sems.at[i]) for i, (a, b) in enumerate(zip(sources, targets))]
    for copy in copies:
        copy.start()
    for copy in copies:
        copy.wait()


def body(tokens_in, out_grad, gate_weight, up_weight, down_weight):
    block, width = tokens_in.shape
    shard, hid = gate_weight.shape
    devices = lax.axis_size("rep") * lax.axis_size("fs") * lax.axis_size("tp")
    factor = (block * devices) ** (-0.5)
    tokens = block * 8
    A, B = SPLIT
    total_rows = sum(A) + sum(B)

    def ring(count, lanes):
        return [
            pltpu.VMEM((count, lanes // 2), BF16),
            pltpu.VMEM((count, lanes // 2), BF16),
            pltpu.VMEM((count, lanes), BF16),
            pltpu.VMEM((count, lanes), BF16),
        ]

    def exchange(count):
        return [pltpu.VMEM((count // 4, shard), BF16)] * 3

    outs = (
        jax.ShapeDtypeStruct((block, width), BF16),
        jax.ShapeDtypeStruct((hid, shard), F32),
        jax.ShapeDtypeStruct((hid, shard), F32),
        jax.ShapeDtypeStruct((hid, shard), F32),
    )
    arrays = tokens_in, out_grad, gate_weight.T, up_weight.T, down_weight
    results = pl.pallas_call(
        functools.partial(kernel, factor, block, width, hid),
        out_shape=outs,
        in_specs=[pl.BlockSpec(memory_space=pltpu.HBM)] * 5,
        out_specs=[pl.BlockSpec(memory_space=pltpu.VMEM)] * 4,
        scratch_shapes=[
            pltpu.VMEM((tokens, width), BF16),
            pltpu.VMEM((tokens, width), BF16),
            pltpu.VMEM((3 * hid, width), BF16),
            pltpu.VMEM((3 * hid, tokens), BF16),
            pltpu.VMEM((hid, tokens), F32),
            pltpu.VMEM((hid, tokens), F32),
            pltpu.VMEM((total_rows, width), BF16),
            pltpu.VMEM((tokens, width), BF16),
            pltpu.VMEM((tokens // 2, width), BF16),
            pltpu.VMEM((tokens // 2, width), BF16),
            [pltpu.VMEM((n, shard), BF16) for n in A],
            [pltpu.VMEM((n // 4, width), BF16) for n in B],
            pltpu.VMEM((total_rows, shard), BF16),
            [ring(n, shard) for n in A],
            [ring(n // 4, width) for n in B],
            [exchange(n) for n in A],
            [exchange(n) for n in B],
            ring(block, width),
            pltpu.SemaphoreType.DMA((COPIES,)),
            pltpu.SemaphoreType.DMA((COPIES,)),
            pltpu.SemaphoreType.DMA((5,)),
        ],
        compiler_params=pltpu.CompilerParams(
            collective_id=0, has_side_effects=True, vmem_limit_bytes=48 * 1024 * 1024
        ),
    )(*[pltpu.with_memory_space_constraint(a, pltpu.HBM) for a in arrays])
    grad_in, gate_t, up_t, down_t = pl.pallas_call(
        writer,
        out_shape=outs,
        in_specs=[pl.BlockSpec(memory_space=pl.ANY)] * 4,
        out_specs=[pl.BlockSpec(memory_space=pltpu.HBM)] * 4,
        scratch_shapes=[pltpu.SemaphoreType.DMA((4,))],
        compiler_params=pltpu.CompilerParams(vmem_limit_bytes=1024 * 1024),
    )(*results)
    return grad_in, gate_t.T, up_t.T, down_t


def solution(mesh):
    return jax.shard_map(
        body,
        mesh=mesh,
        in_specs=(
            P(("rep", "fs", "tp"), None),
            P(("rep", "fs", "tp"), None),
            P("fs", "tp"),
            P("fs", "tp"),
            P("tp", "fs"),
        ),
        out_specs=(P(("rep", "fs", "tp"), None), P("fs", "tp"), P("fs", "tp"), P("tp", "fs")),
        check_vma=False,
    )
```

```python
import functools

import jax
import jax.numpy as jnp
from jax import lax
from jax.experimental import pallas as pl
from jax.experimental.pallas import tpu as pltpu
from jax.sharding import PartitionSpec as P

BF16 = jnp.bfloat16
F32 = jnp.float32
MESH = pl.DeviceIdType.MESH
COPIES = 144
SPLIT = (192, 192, 192), (128, 256, 128)


def nt(left, right):
    return lax.dot_general(left, right, (((1,), (1,)), ((), ())), preferred_element_type=F32)


def tn(left, right):
    return lax.dot_general(left, right, (((0,), (0,)), ((), ())), preferred_element_type=F32)


def nn(left, right):
    return lax.dot_general(left, right, (((1,), (0,)), ((), ())), preferred_element_type=F32)


def kernel(
    factor, block, width, hid,
    x_in, g_in, wg_in, wu_in, wd_in,
    gin_out, og_out, ou_out, od_out,
    X, G, WT, H, ACT, SLOPE, SUM, PW, DX, DS, GX, YA, ZB, OUTT, YA_BUFS, ZB_BUFS, ZA_BUFS, YB_BUFS, XR_BUFS,
    send_sems, recv_sems, local_sems,
):
    rep = lax.axis_index("rep")
    fs = lax.axis_index("fs")
    tp = lax.axis_index("tp")
    core = lax.rem(tp, 2)
    xpos = tp // 2
    shard = width // 4

    def turn(pos, step):
        return lax.rem(pos + step, 4)

    def at_x(step):
        return {"tp": turn(xpos, step) * 2 + core}

    def at_y(step):
        return {"fs": turn(fs, step)}

    def at_z(step):
        return {"rep": turn(rep, step)}

    sibling = {"tp": tp + 1 - 2 * core}

    def lanes_of(step):
        return pl.ds(pl.multiple_of(turn(fs, step) * shard, shard), shard)

    counter = [0]
    pending = []

    def remote(src, dst, k, where):
        return pltpu.make_async_remote_copy(
            src_ref=src, dst_ref=dst, send_sem=send_sems.at[k], recv_sem=recv_sems.at[k],
            device_id=where, device_id_type=MESH,
        )

    def send(src, dst, where):
        k = counter[0]
        counter[0] += 1
        copy = remote(src, dst, k, where)
        copy.start()
        pending.append(copy)
        return k

    def arrived(k, landing):
        remote(landing, landing, k, sibling).wait_recv()

    barrier = pltpu.get_barrier_semaphore()
    partners = [sibling] + [at(step) for at in (at_x, at_y, at_z) for step in (1, 3)]
    partners += [at_y(2), at_z(2)]
    for where in partners:
        pl.semaphore_signal(barrier, inc=1, device_id=where, device_id_type=MESH)

    own_lanes = lanes_of(0)
    loads = [
        pltpu.make_async_copy(x_in, X.at[pl.ds(0, block)], local_sems.at[0]),
        pltpu.make_async_copy(g_in, G.at[pl.ds(0, block)], local_sems.at[1]),
        pltpu.make_async_copy(wg_in, WT.at[pl.ds(0, hid), own_lanes], local_sems.at[2]),
        pltpu.make_async_copy(wu_in, WT.at[pl.ds(hid, hid), own_lanes], local_sems.at[3]),
        pltpu.make_async_copy(wd_in, WT.at[pl.ds(2 * hid, hid), own_lanes], local_sems.at[4]),
    ]
    for load in loads:
        load.start()

    pl.semaphore_wait(barrier, len(partners))

    half = block // 2
    SELF, LEFT, RIGHT, OPP = 0, 1, 2, 3

    def slot(buf, s, start=0, count=block):
        return buf.at[pl.ds(s * 2 * block + start, count)]

    def forward(buf, s, start=0, count=block):
        landing = (s, block + start, count)
        return send(slot(buf, s, start, count), slot(buf, *landing), sibling), landing

    def forwarded(buf, *states):
        for k, landing in states:
            arrived(k, slot(buf, *landing))

    class Tokens:
        def __init__(self, buf):
            self.buf = buf

        def part(self, s, which):
            return slot(self.buf, s, which * half, half)

        def start_first(self):
            self.r0 = send(self.part(SELF, 0), self.part(LEFT, 0), at_x(1))
            self.l1 = send(self.part(SELF, 1), self.part(RIGHT, 1), at_x(3))

        def start_second(self):
            self.r1 = send(self.part(SELF, 1), self.part(LEFT, 1), at_x(1))
            self.l0 = send(self.part(SELF, 0), self.part(RIGHT, 0), at_x(3))

        def relay(self):
            arrived(self.r0, self.part(LEFT, 0))
            self.r2 = send(self.part(LEFT, 0), self.part(OPP, 0), at_x(1))
            arrived(self.l1, self.part(RIGHT, 1))
            self.l2 = send(self.part(RIGHT, 1), self.part(OPP, 1), at_x(3))

        def near(self):
            arrived(self.r1, self.part(LEFT, 1))
            arrived(self.l0, self.part(RIGHT, 0))
            return forward(self.buf, LEFT), forward(self.buf, RIGHT)

        def far(self):
            arrived(self.r2, self.part(OPP, 0))
            first = forward(self.buf, OPP, 0, half)
            arrived(self.l2, self.part(OPP, 1))
            return first, forward(self.buf, OPP, half, half)

    xt, gt = Tokens(X), Tokens(G)
    loads[0].wait()
    xt.start_first()
    xt.start_second()
    loads[1].wait()
    gt.start_first()
    for load in loads[2:]:
        load.wait()

    direct, spare = 384, 96
    base1, base2 = direct, 2 * hid + spare
    dhalf = direct // 2
    D0, D1 = pl.ds(0, dhalf), pl.ds(dhalf, dhalf)
    D2 = pl.ds(2 * hid, spare)

    def w(rows, step):
        return WT.at[rows, lanes_of(step)]

    def copy_w(rows, step, where):
        return send(w(rows, step), w(rows, step), where)

    class Quarters:
        def __init__(self, base, end):
            self.base, self.part = base, (end - base) // 4
            self.cut = (self.part // 2 + 15) // 16 * 16

        def rows(self, step, which=None):
            start, count = {
                None: (0, self.part), 0: (0, self.cut), 1: (self.cut, self.part - self.cut)
            }[which]
            return pl.ds(pl.multiple_of(self.base + turn(rep, step) * self.part + start, 16), count)

        def start(self):
            self.r, self.l = copy_w(self.rows(0), 0, at_y(1)), copy_w(self.rows(0), 0, at_y(3))
            self.shares = {}

        def relay(self):
            arrived(self.r, w(self.rows(0), 3))
            self.r2 = copy_w(self.rows(0, 0), 3, at_y(1))
            arrived(self.l, w(self.rows(0), 1))
            self.l2 = copy_w(self.rows(0, 1), 1, at_y(3))

        def far(self):
            arrived(self.r2, w(self.rows(0, 0), 2))
            arrived(self.l2, w(self.rows(0, 1), 2))

        def share(self, lane):
            self.shares[lane] = [
                (copy_w(self.rows(0), lane, at_z(step)), 4 - step) for step in (2, 1, 3)
            ]

        def finish(self):
            for lane, keys in self.shares.items():
                for k, step in keys:
                    arrived(k, w(self.rows(step), lane))

    q1, q2 = Quarters(base1, 2 * hid), Quarters(base2, 3 * hid)
    q1.start()
    q2.start()
    d0r = copy_w(D0, 0, at_y(1))
    d1l = copy_w(D1, 0, at_y(3))
    x_own = forward(X, SELF)
    g_own = forward(G, SELF)

    q1.relay()
    q1.share(3)
    q1.share(1)
    q2.relay()
    d1r = copy_w(D1, 0, at_y(1))
    d0l = copy_w(D0, 0, at_y(3))

    xt.relay()
    gt.start_second()
    arrived(d0r, w(D0, 3))
    dc = copy_w(D0, 3, at_y(1))
    arrived(d1l, w(D1, 1))
    dd = copy_w(D1, 1, at_y(3))
    x_near = xt.near()
    q1.far()
    q1.share(2)
    q2.share(3)
    q2.share(1)
    q2.far()
    q2.share(2)
    d2 = [(copy_w(D2, 0, at_y(step)), 4 - step) for step in (2, 1, 3)]
    gt.relay()
    x_far = xt.far()

    forwarded(X, x_own, *x_near)
    arrived(d1r, w(D1, 3))
    arrived(d0l, w(D0, 1))
    q1.finish()
    arrived(dc, w(D0, 2))
    arrived(dd, w(D1, 2))

    rows = hid // 2

    def gate_stage(c):
        cols = pl.ds(c * 256, 256)
        for p in range(2):
            part_rows = pl.ds(p * rows, rows)
            gate = nt(WT[part_rows, :], X[cols, :]).astype(BF16).astype(F32)
            up = nt(WT[pl.ds(hid + p * rows, rows), :], X[cols, :]).astype(BF16).astype(F32)
            sig = jax.nn.sigmoid(gate)
            act = gate * sig
            H[pl.ds(2 * hid + p * rows, rows), cols] = (act * up).astype(BF16)
            ACT[part_rows, cols] = act
            SLOPE[part_rows, cols] = up * sig * (1.0 + gate * (1.0 - sig))

    def grad_stage(c):
        cols = pl.ds(c * 256, 256)
        grad = nt(WT[pl.ds(2 * hid, hid), :], G[cols, :]).astype(BF16).astype(F32)
        H[pl.ds(0, hid), cols] = (grad * SLOPE[:, cols]).astype(BF16)
        H[pl.ds(hid, hid), cols] = (grad * ACT[:, cols]).astype(BF16)

    gate_stage(0)
    gate_stage(1)
    g_near = gt.near()
    forwarded(X, *x_far)
    gate_stage(2)
    q2.finish()
    for k, step in d2:
        arrived(k, w(D2, step))
    forwarded(G, g_own, g_near[0])
    g_far = gt.far()
    grad_stage(0)
    forwarded(G, g_near[1])
    grad_stage(1)
    first = pl.ds(sum(SPLIT[0]), SPLIT[1][0])
    early, late = pl.ds(0, 2 * 256), pl.ds(2 * 256, 256)
    for n in range(4):
        SUM[:, pl.ds(n * 256, 256)] = nn(H[first, early], X[early, pl.ds(n * 256, 256)])
    forwarded(G, *g_far)
    grad_stage(2)

    class Ring:
        def __init__(self, piece, bufs, dest):
            self.piece, self.dest = piece, dest
            self.t0, self.t1, self.fl, self.fr = bufs
            self.h = self.t0.shape[1]

        def side(self, buf, which):
            return buf.at[:, pl.ds(which * self.h, self.h)]

        def start_far(self):
            self.a = send(self.piece(2, 0), self.t0, self.dest(1))
            self.b = send(self.piece(2, 1), self.t1, self.dest(3))

        def start_near(self):
            self.c = send(self.piece(1, 1), self.side(self.fl, 1), self.dest(1))
            self.d = send(self.piece(3, 0), self.side(self.fr, 0), self.dest(3))

        def relay(self):
            arrived(self.a, self.t0)
            self.t0[...] = (self.t0[...].astype(F32) + self.piece(1, 0)[...].astype(F32)).astype(BF16)
            self.e = send(self.t0, self.side(self.fl, 0), self.dest(1))
            arrived(self.b, self.t1)
            self.t1[...] = (self.t1[...].astype(F32) + self.piece(3, 1)[...].astype(F32)).astype(BF16)
            self.f = send(self.t1, self.side(self.fr, 1), self.dest(3))

        def finish(self, store):
            arrived(self.c, self.side(self.fl, 1))
            arrived(self.d, self.side(self.fr, 0))
            arrived(self.e, self.side(self.fl, 0))
            arrived(self.f, self.side(self.fr, 1))
            for which in range(2):
                total = (
                    self.piece(0, which)[...].astype(F32)
                    + self.side(self.fl, which)[...].astype(F32)
                    + self.side(self.fr, which)[...].astype(F32)
                )
                store(which, total.astype(BF16))

    def y_piece(buf, start, count):
        def piece(step, which):
            lane = pl.multiple_of(turn(fs, step) * shard + which * (shard // 2), 128)
            return buf.at[pl.ds(start, count), pl.ds(lane, shard // 2)]
        return piece

    def z_piece(buf, start, count, lanes):
        def piece(step, which):
            row = pl.multiple_of(start + turn(rep, step) * count, 16)
            return buf.at[pl.ds(row, count), pl.ds(which * lanes, lanes)]
        return piece

    def x_piece(step, which):
        s = {0: SELF, 1: RIGHT, 3: LEFT, 2: OPP}[step]
        return GX.at[pl.ds(s * block, block), pl.ds(which * (width // 2), width // 2)]

    def strip(buf, count):
        def piece(step):
            row = pl.multiple_of(turn(rep, step) * (count // 4), 16)
            return buf.at[pl.ds(row, count // 4)]
        return piece

    def column(buf):
        def piece(step):
            return buf.at[:, lanes_of(step)]
        return piece

    class Exchange:
        def __init__(self, piece, bufs, dest):
            self.piece, self.bufs, self.dest = piece, bufs, dest

        def start(self):
            self.keys = [
                (send(self.piece(step), self.bufs[step - 1], self.dest(step)), self.bufs[step - 1])
                for step in (2, 1, 3)
            ]

        def finish(self, start):
            for k, landing in self.keys:
                arrived(k, landing)
            total = self.piece(0)[...].astype(F32)
            for buf in self.bufs:
                total = total + buf[...].astype(F32)
            OUTT[pl.ds(start, total.shape[0]), :] = total.astype(BF16)

    class Gather:
        def __init__(self, base, count):
            self.base, self.count = base, count // 4

        def row(self, step):
            return pl.multiple_of(self.base + turn(rep, step) * self.count, 16)

        def region(self, step):
            return OUTT.at[pl.ds(self.row(step), self.count)]

        def start(self):
            self.keys = [
                (send(self.region(0), self.region(0), at_z(step)), 4 - step) for step in (2, 1, 3)
            ]

        def finish(self):
            for k, step in self.keys:
                arrived(k, self.region(step))

    A, B = SPLIT
    a_at = [sum(A[:i]) for i in range(len(A))]
    b_at = [sum(A) + sum(B[:i]) for i in range(len(B))]
    ya = [Ring(y_piece(PW, r, n), bufs, at_y) for r, n, bufs in zip(a_at, A, YA_BUFS)]
    zb = [Ring(z_piece(PW, r, n // 4, width // 2), bufs, at_z) for r, n, bufs in zip(b_at, B, ZB_BUFS)]
    za = [Exchange(strip(buf, n), bufs, at_z) for buf, n, bufs in zip(YA, A, ZA_BUFS)]
    yb = [Exchange(column(buf), bufs, at_y) for buf, bufs in zip(ZB, YB_BUFS)]
    ga = [Gather(r, n) for r, n in zip(a_at, A)]
    gb = [Gather(r, n) for r, n in zip(b_at, B)]
    xr = Ring(x_piece, XR_BUFS, at_x)

    def keep(buf):
        def store(which, value):
            h = value.shape[1]
            buf[:, pl.ds(which * h, h)] = value
        return store

    def weight_piece(step, start, count):
        lanes = lanes_of(step)
        PW[pl.ds(start, count), lanes] = (
            factor * nn(H[pl.ds(start, count), :], X[:, lanes])
        ).astype(BF16)

    def weight_rows(start, count):
        for lo, hi, tokens in ((start, min(start + count, 2 * hid), X), (max(start, 2 * hid), min(start + count, 3 * hid), G)):
            if lo < hi:
                for n in range(4):
                    PW[pl.ds(lo, hi - lo), pl.ds(n * 256, 256)] = (
                        factor * nn(H[pl.ds(lo, hi - lo), :], tokens[:, pl.ds(n * 256, 256)])
                    ).astype(BF16)

    def first_rows():
        for n in range(4):
            lanes = pl.ds(n * 256, 256)
            PW[first, lanes] = (factor * (SUM[:, lanes] + nn(H[first, late], X[late, lanes]))).astype(BF16)

    def input_piece(c):
        DX[pl.ds(c * 256, 256), :] = tn(
            H[pl.ds(0, 2 * hid), pl.ds(c * 256, 256)], WT[pl.ds(0, 2 * hid), :]
        ).astype(BF16)

    def across(s):
        landing = DS.at[pl.ds(s * block, block)]
        return send(slot(DX, s, block), landing, sibling)

    def across_add(k, s):
        arrived(k, DS.at[pl.ds(s * block, block)])
        GX[pl.ds(s * block, block), :] = (
            DX[pl.ds(s * 2 * block, block), :].astype(F32)
            + DS[pl.ds(s * block, block), :].astype(F32)
        ).astype(BF16)

    blank = PW.shape[0] - 3 * hid
    PW[pl.ds(3 * hid, blank), :] = jnp.zeros((blank, width), BF16)
    first_rows()
    zb[0].start_far()
    weight_piece(2, 0, A[0])
    ya[0].start_far()
    zb[0].start_near()
    weight_piece(1, 0, A[0])
    weight_piece(3, 0, A[0])
    ya[0].start_near()
    weight_rows(a_at[1], A[1])
    weight_rows(b_at[1], B[1])
    ya[1].start_far()
    zb[1].start_far()
    weight_rows(a_at[2], A[2])
    weight_rows(b_at[2], B[2])
    input_piece(2)
    opp = across(OPP)
    zb[0].relay()
    ya[1].start_near()
    input_piece(1)
    near = across(LEFT), across(RIGHT)
    ya[0].relay()
    zb[1].start_near()
    input_piece(0)
    mine = across(SELF)
    weight_piece(0, 0, A[0])
    across_add(opp, OPP)
    xr.start_far()
    ya[2].start_far()
    zb[2].start_far()
    across_add(near[0], LEFT)
    across_add(near[1], RIGHT)
    zb[1].relay()
    ya[1].relay()
    xr.start_near()
    across_add(mine, SELF)
    zb[0].finish(keep(ZB[0]))
    yb[0].start()
    zb[2].start_near()
    ya[2].start_near()
    ya[0].finish(keep(YA[0]))
    za[0].start()
    zb[2].relay()
    ya[2].relay()
    xr.relay()
    ya[1].finish(keep(YA[1]))
    za[1].start()
    zb[1].finish(keep(ZB[1]))
    yb[1].start()
    yb[0].finish(gb[0].row(0))
    gb[0].start()
    za[0].finish(ga[0].row(0))
    ga[0].start()
    zb[2].finish(keep(ZB[2]))
    yb[2].start()
    ya[2].finish(keep(YA[2]))
    za[2].start()
    za[1].finish(ga[1].row(0))
    ga[1].start()
    xr.finish(keep(gin_out))
    yb[1].finish(gb[1].row(0))
    gb[1].start()
    gb[0].finish()
    ga[0].finish()
    yb[2].finish(gb[2].row(0))
    gb[2].start()
    za[2].finish(ga[2].row(0))
    ga[2].start()
    ga[1].finish()
    gb[1].finish()
    gb[2].finish()
    ga[2].finish()
    og_out[...] = OUTT[pl.ds(0, hid), :].astype(F32)
    ou_out[...] = OUTT[pl.ds(hid, hid), :].astype(F32)
    od_out[...] = OUTT[pl.ds(2 * hid, hid), :].astype(F32)

    for copy in pending:
        copy.wait_send()


def writer(*refs):
    sources, targets, sems = refs[:4], refs[4:8], refs[8]
    copies = [pltpu.make_async_copy(a, b, sems.at[i]) for i, (a, b) in enumerate(zip(sources, targets))]
    for copy in copies:
        copy.start()
    for copy in copies:
        copy.wait()


def body(tokens_in, out_grad, gate_weight, up_weight, down_weight):
    block, width = tokens_in.shape
    shard, hid = gate_weight.shape
    devices = lax.axis_size("rep") * lax.axis_size("fs") * lax.axis_size("tp")
    factor = (block * devices) ** (-0.5)
    tokens = block * 8
    A, B = SPLIT
    total_rows = sum(A) + sum(B)

    def ring(count, lanes):
        return [
            pltpu.VMEM((count, lanes // 2), BF16),
            pltpu.VMEM((count, lanes // 2), BF16),
            pltpu.VMEM((count, lanes), BF16),
            pltpu.VMEM((count, lanes), BF16),
        ]

    def exchange(count):
        return [pltpu.VMEM((count // 4, shard), BF16)] * 3

    outs = (
        jax.ShapeDtypeStruct((block, width), BF16),
        jax.ShapeDtypeStruct((hid, shard), F32),
        jax.ShapeDtypeStruct((hid, shard), F32),
        jax.ShapeDtypeStruct((hid, shard), F32),
    )
    arrays = tokens_in, out_grad, gate_weight.T, up_weight.T, down_weight
    results = pl.pallas_call(
        functools.partial(kernel, factor, block, width, hid),
        out_shape=outs,
        in_specs=[pl.BlockSpec(memory_space=pltpu.HBM)] * 5,
        out_specs=[pl.BlockSpec(memory_space=pltpu.VMEM)] * 4,
        scratch_shapes=[
            pltpu.VMEM((tokens, width), BF16),
            pltpu.VMEM((tokens, width), BF16),
            pltpu.VMEM((3 * hid, width), BF16),
            pltpu.VMEM((3 * hid, tokens), BF16),
            pltpu.VMEM((hid, tokens), F32),
            pltpu.VMEM((hid, tokens), F32),
            pltpu.VMEM((B[0], width), F32),
            pltpu.VMEM((total_rows, width), BF16),
            pltpu.VMEM((tokens, width), BF16),
            pltpu.VMEM((tokens // 2, width), BF16),
            pltpu.VMEM((tokens // 2, width), BF16),
            [pltpu.VMEM((n, shard), BF16) for n in A],
            [pltpu.VMEM((n // 4, width), BF16) for n in B],
            pltpu.VMEM((total_rows, shard), BF16),
            [ring(n, shard) for n in A],
            [ring(n // 4, width) for n in B],
            [exchange(n) for n in A],
            [exchange(n) for n in B],
            ring(block, width),
            pltpu.SemaphoreType.DMA((COPIES,)),
            pltpu.SemaphoreType.DMA((COPIES,)),
            pltpu.SemaphoreType.DMA((5,)),
        ],
        compiler_params=pltpu.CompilerParams(
            collective_id=0, has_side_effects=True, vmem_limit_bytes=48 * 1024 * 1024
        ),
    )(*[pltpu.with_memory_space_constraint(a, pltpu.HBM) for a in arrays])
    grad_in, gate_t, up_t, down_t = pl.pallas_call(
        writer,
        out_shape=outs,
        in_specs=[pl.BlockSpec(memory_space=pl.ANY)] * 4,
        out_specs=[pl.BlockSpec(memory_space=pltpu.HBM)] * 4,
        scratch_shapes=[pltpu.SemaphoreType.DMA((4,))],
        compiler_params=pltpu.CompilerParams(vmem_limit_bytes=1024 * 1024),
    )(*results)
    return grad_in, gate_t.T, up_t.T, down_t


def solution(mesh):
    return jax.shard_map(
        body,
        mesh=mesh,
        in_specs=(
            P(("rep", "fs", "tp"), None),
            P(("rep", "fs", "tp"), None),
            P("fs", "tp"),
            P("fs", "tp"),
            P("tp", "fs"),
        ),
        out_specs=(P(("rep", "fs", "tp"), None), P("fs", "tp"), P("fs", "tp"), P("tp", "fs")),
        check_vma=False,
    )
```

```python
import functools

import jax
import jax.numpy as jnp
from jax import lax
from jax.experimental import pallas as pl
from jax.experimental.pallas import tpu as pltpu
from jax.sharding import PartitionSpec as P

BF16 = jnp.bfloat16
F32 = jnp.float32
MESH = pl.DeviceIdType.MESH
COPIES = 144
SPLIT = (192, 192, 192), (128, 256, 128)


def nt(left, right):
    return lax.dot_general(left, right, (((1,), (1,)), ((), ())), preferred_element_type=F32)


def tn(left, right):
    return lax.dot_general(left, right, (((0,), (0,)), ((), ())), preferred_element_type=F32)


def nn(left, right):
    return lax.dot_general(left, right, (((1,), (0,)), ((), ())), preferred_element_type=F32)


def kernel(
    factor, block, width, hid,
    x_in, g_in, wg_in, wu_in, wd_in,
    gin_out, og_out, ou_out, od_out,
    X, G, WT, H, ACT, SLOPE, SUM, PW, DX, DS, GX, YA, ZB, OUTT, YA_BUFS, ZB_BUFS, ZA_BUFS, YB_BUFS, XR_BUFS,
    send_sems, recv_sems, local_sems,
):
    rep = lax.axis_index("rep")
    fs = lax.axis_index("fs")
    tp = lax.axis_index("tp")
    core = lax.rem(tp, 2)
    xpos = tp // 2
    shard = width // 4

    def turn(pos, step):
        return lax.rem(pos + step, 4)

    def at_x(step):
        return {"tp": turn(xpos, step) * 2 + core}

    def at_y(step):
        return {"fs": turn(fs, step)}

    def at_z(step):
        return {"rep": turn(rep, step)}

    sibling = {"tp": tp + 1 - 2 * core}

    def lanes_of(step):
        return pl.ds(pl.multiple_of(turn(fs, step) * shard, shard), shard)

    counter = [0]
    pending = []

    def remote(src, dst, k, where):
        return pltpu.make_async_remote_copy(
            src_ref=src, dst_ref=dst, send_sem=send_sems.at[k], recv_sem=recv_sems.at[k],
            device_id=where, device_id_type=MESH,
        )

    def send(src, dst, where):
        k = counter[0]
        counter[0] += 1
        copy = remote(src, dst, k, where)
        copy.start()
        pending.append(copy)
        return k

    def arrived(k, landing):
        remote(landing, landing, k, sibling).wait_recv()

    barrier = pltpu.get_barrier_semaphore()
    partners = [sibling] + [at(step) for at in (at_x, at_y, at_z) for step in (1, 3)]
    partners += [at_y(2), at_z(2)]
    for where in partners:
        pl.semaphore_signal(barrier, inc=1, device_id=where, device_id_type=MESH)

    own_lanes = lanes_of(0)
    loads = [
        pltpu.make_async_copy(x_in, X.at[pl.ds(0, block)], local_sems.at[0]),
        pltpu.make_async_copy(g_in, G.at[pl.ds(0, block)], local_sems.at[1]),
        pltpu.make_async_copy(wg_in, WT.at[pl.ds(0, hid), own_lanes], local_sems.at[2]),
        pltpu.make_async_copy(wu_in, WT.at[pl.ds(hid, hid), own_lanes], local_sems.at[3]),
        pltpu.make_async_copy(wd_in, WT.at[pl.ds(2 * hid, hid), own_lanes], local_sems.at[4]),
    ]
    for load in loads:
        load.start()

    pl.semaphore_wait(barrier, len(partners))

    half = block // 2
    SELF, LEFT, RIGHT, OPP = 0, 1, 2, 3

    def slot(buf, s, start=0, count=block):
        return buf.at[pl.ds(s * 2 * block + start, count)]

    def forward(buf, s, start=0, count=block):
        landing = (s, block + start, count)
        return send(slot(buf, s, start, count), slot(buf, *landing), sibling), landing

    def forwarded(buf, *states):
        for k, landing in states:
            arrived(k, slot(buf, *landing))

    class Tokens:
        def __init__(self, buf):
            self.buf = buf

        def part(self, s, which):
            return slot(self.buf, s, which * half, half)

        def start_first(self):
            self.r0 = send(self.part(SELF, 0), self.part(LEFT, 0), at_x(1))
            self.l1 = send(self.part(SELF, 1), self.part(RIGHT, 1), at_x(3))

        def start_second(self):
            self.r1 = send(self.part(SELF, 1), self.part(LEFT, 1), at_x(1))
            self.l0 = send(self.part(SELF, 0), self.part(RIGHT, 0), at_x(3))

        def relay(self):
            arrived(self.r0, self.part(LEFT, 0))
            self.r2 = send(self.part(LEFT, 0), self.part(OPP, 0), at_x(1))
            arrived(self.l1, self.part(RIGHT, 1))
            self.l2 = send(self.part(RIGHT, 1), self.part(OPP, 1), at_x(3))

        def near(self):
            arrived(self.r1, self.part(LEFT, 1))
            arrived(self.l0, self.part(RIGHT, 0))
            return forward(self.buf, LEFT), forward(self.buf, RIGHT)

        def far(self):
            arrived(self.r2, self.part(OPP, 0))
            first = forward(self.buf, OPP, 0, half)
            arrived(self.l2, self.part(OPP, 1))
            return first, forward(self.buf, OPP, half, half)

    xt, gt = Tokens(X), Tokens(G)
    loads[0].wait()
    xt.start_first()
    xt.start_second()
    loads[1].wait()
    gt.start_first()
    for load in loads[2:]:
        load.wait()

    direct, spare = 384, 96
    base1, base2 = direct, 2 * hid + spare
    dhalf = direct // 2
    D0, D1 = pl.ds(0, dhalf), pl.ds(dhalf, dhalf)
    D2 = pl.ds(2 * hid, spare)

    def w(rows, step):
        return WT.at[rows, lanes_of(step)]

    def copy_w(rows, step, where):
        return send(w(rows, step), w(rows, step), where)

    class Quarters:
        def __init__(self, base, end):
            self.base, self.part = base, (end - base) // 4
            self.cut = (self.part // 2 + 15) // 16 * 16

        def rows(self, step, which=None):
            start, count = {
                None: (0, self.part), 0: (0, self.cut), 1: (self.cut, self.part - self.cut)
            }[which]
            return pl.ds(pl.multiple_of(self.base + turn(rep, step) * self.part + start, 16), count)

        def start(self):
            self.r, self.l = copy_w(self.rows(0), 0, at_y(1)), copy_w(self.rows(0), 0, at_y(3))
            self.shares = {}

        def relay(self):
            arrived(self.r, w(self.rows(0), 3))
            self.r2 = copy_w(self.rows(0, 0), 3, at_y(1))
            arrived(self.l, w(self.rows(0), 1))
            self.l2 = copy_w(self.rows(0, 1), 1, at_y(3))

        def far(self):
            arrived(self.r2, w(self.rows(0, 0), 2))
            arrived(self.l2, w(self.rows(0, 1), 2))

        def share(self, lane):
            self.shares[lane] = [
                (copy_w(self.rows(0), lane, at_z(step)), 4 - step) for step in (2, 1, 3)
            ]

        def finish(self):
            for lane, keys in self.shares.items():
                for k, step in keys:
                    arrived(k, w(self.rows(step), lane))

    q1, q2 = Quarters(base1, 2 * hid), Quarters(base2, 3 * hid)
    q1.start()
    q2.start()
    d0r = copy_w(D0, 0, at_y(1))
    d1l = copy_w(D1, 0, at_y(3))
    x_own = forward(X, SELF)
    g_own = forward(G, SELF)

    q1.relay()
    q1.share(3)
    q1.share(1)
    q2.relay()
    d1r = copy_w(D1, 0, at_y(1))
    d0l = copy_w(D0, 0, at_y(3))

    xt.relay()
    gt.start_second()
    arrived(d0r, w(D0, 3))
    dc = copy_w(D0, 3, at_y(1))
    arrived(d1l, w(D1, 1))
    dd = copy_w(D1, 1, at_y(3))
    x_near = xt.near()
    q1.far()
    q1.share(2)
    q2.share(3)
    q2.share(1)
    q2.far()
    q2.share(2)
    d2 = [(copy_w(D2, 0, at_y(step)), 4 - step) for step in (2, 1, 3)]
    gt.relay()
    x_far = xt.far()

    forwarded(X, x_own, *x_near)
    arrived(d1r, w(D1, 3))
    arrived(d0l, w(D0, 1))
    q1.finish()
    arrived(dc, w(D0, 2))
    arrived(dd, w(D1, 2))

    rows = hid // 2

    def gate_stage(c):
        cols = pl.ds(c * 256, 256)
        for p in range(2):
            part_rows = pl.ds(p * rows, rows)
            gate = nt(WT[part_rows, :], X[cols, :]).astype(BF16).astype(F32)
            up = nt(WT[pl.ds(hid + p * rows, rows), :], X[cols, :]).astype(BF16).astype(F32)
            sig = jax.nn.sigmoid(gate)
            act = gate * sig
            H[pl.ds(2 * hid + p * rows, rows), cols] = (act * up).astype(BF16)
            ACT[part_rows, cols] = act
            SLOPE[part_rows, cols] = up * sig * (1.0 + gate * (1.0 - sig))

    def grad_stage(c):
        cols = pl.ds(c * 256, 256)
        grad = nt(WT[pl.ds(2 * hid, hid), :], G[cols, :]).astype(BF16).astype(F32)
        H[pl.ds(0, hid), cols] = (grad * SLOPE[:, cols]).astype(BF16)
        H[pl.ds(hid, hid), cols] = (grad * ACT[:, cols]).astype(BF16)

    gate_stage(0)
    gate_stage(1)
    g_near = gt.near()
    forwarded(X, *x_far)
    gate_stage(2)
    q2.finish()
    for k, step in d2:
        arrived(k, w(D2, step))
    forwarded(G, g_own, g_near[0])
    g_far = gt.far()
    grad_stage(0)
    forwarded(G, g_near[1])
    grad_stage(1)
    first = pl.ds(sum(SPLIT[0]), SPLIT[1][0])
    early, late = pl.ds(0, 2 * 256), pl.ds(2 * 256, 256)
    for n in range(4):
        SUM[:, pl.ds(n * 256, 256)] = nn(H[first, early], X[early, pl.ds(n * 256, 256)])
    forwarded(G, *g_far)
    grad_stage(2)

    class Ring:
        def __init__(self, piece, bufs, dest):
            self.piece, self.dest = piece, dest
            self.t0, self.t1, self.fl, self.fr = bufs
            self.h = self.t0.shape[1]

        def side(self, buf, which):
            return buf.at[:, pl.ds(which * self.h, self.h)]

        def start_far(self):
            self.a = send(self.piece(2, 0), self.t0, self.dest(1))
            self.b = send(self.piece(2, 1), self.t1, self.dest(3))

        def start_near(self):
            self.c = send(self.piece(1, 1), self.side(self.fl, 1), self.dest(1))
            self.d = send(self.piece(3, 0), self.side(self.fr, 0), self.dest(3))

        def relay(self):
            arrived(self.a, self.t0)
            self.t0[...] = (self.t0[...].astype(F32) + self.piece(1, 0)[...].astype(F32)).astype(BF16)
            self.e = send(self.t0, self.side(self.fl, 0), self.dest(1))
            arrived(self.b, self.t1)
            self.t1[...] = (self.t1[...].astype(F32) + self.piece(3, 1)[...].astype(F32)).astype(BF16)
            self.f = send(self.t1, self.side(self.fr, 1), self.dest(3))

        def finish(self, store):
            arrived(self.c, self.side(self.fl, 1))
            arrived(self.d, self.side(self.fr, 0))
            arrived(self.e, self.side(self.fl, 0))
            arrived(self.f, self.side(self.fr, 1))
            for which in range(2):
                total = (
                    self.piece(0, which)[...].astype(F32)
                    + self.side(self.fl, which)[...].astype(F32)
                    + self.side(self.fr, which)[...].astype(F32)
                )
                store(which, total.astype(BF16))

    def y_piece(buf, start, count):
        def piece(step, which):
            lane = pl.multiple_of(turn(fs, step) * shard + which * (shard // 2), 128)
            return buf.at[pl.ds(start, count), pl.ds(lane, shard // 2)]
        return piece

    def z_piece(buf, start, count, lanes):
        def piece(step, which):
            row = pl.multiple_of(start + turn(rep, step) * count, 16)
            return buf.at[pl.ds(row, count), pl.ds(which * lanes, lanes)]
        return piece

    def x_piece(step, which):
        s = {0: SELF, 1: RIGHT, 3: LEFT, 2: OPP}[step]
        return GX.at[pl.ds(s * block, block), pl.ds(which * (width // 2), width // 2)]

    def strip(buf, count):
        def piece(step):
            row = pl.multiple_of(turn(rep, step) * (count // 4), 16)
            return buf.at[pl.ds(row, count // 4)]
        return piece

    def column(buf):
        def piece(step):
            return buf.at[:, lanes_of(step)]
        return piece

    class Exchange:
        def __init__(self, piece, bufs, dest):
            self.piece, self.bufs, self.dest = piece, bufs, dest

        def start(self):
            self.keys = [
                (send(self.piece(step), self.bufs[step - 1], self.dest(step)), self.bufs[step - 1])
                for step in (2, 1, 3)
            ]

        def finish(self, start):
            for k, landing in self.keys:
                arrived(k, landing)
            total = self.piece(0)[...].astype(F32)
            for buf in self.bufs:
                total = total + buf[...].astype(F32)
            OUTT[pl.ds(start, total.shape[0]), :] = total.astype(BF16)

    class Gather:
        def __init__(self, base, count):
            self.base, self.count = base, count // 4

        def row(self, step):
            return pl.multiple_of(self.base + turn(rep, step) * self.count, 16)

        def region(self, step):
            return OUTT.at[pl.ds(self.row(step), self.count)]

        def start(self):
            self.keys = [
                (send(self.region(0), self.region(0), at_z(step)), 4 - step) for step in (2, 1, 3)
            ]

        def finish(self):
            for k, step in self.keys:
                arrived(k, self.region(step))

    A, B = SPLIT
    a_at = [sum(A[:i]) for i in range(len(A))]
    b_at = [sum(A) + sum(B[:i]) for i in range(len(B))]
    ya = [Ring(y_piece(PW, r, n), bufs, at_y) for r, n, bufs in zip(a_at, A, YA_BUFS)]
    zb = [Ring(z_piece(PW, r, n // 4, width // 2), bufs, at_z) for r, n, bufs in zip(b_at, B, ZB_BUFS)]
    za = [Exchange(strip(buf, n), bufs, at_z) for buf, n, bufs in zip(YA, A, ZA_BUFS)]
    yb = [Exchange(column(buf), bufs, at_y) for buf, bufs in zip(ZB, YB_BUFS)]
    ga = [Gather(r, n) for r, n in zip(a_at, A)]
    gb = [Gather(r, n) for r, n in zip(b_at, B)]
    xr = Ring(x_piece, XR_BUFS, at_x)

    def keep(buf):
        def store(which, value):
            h = value.shape[1]
            buf[:, pl.ds(which * h, h)] = value
        return store

    def weight_piece(step, start, count):
        lanes = lanes_of(step)
        PW[pl.ds(start, count), lanes] = (
            factor * nn(H[pl.ds(start, count), :], X[:, lanes])
        ).astype(BF16)

    def weight_rows(start, count):
        for lo, hi, tokens in ((start, min(start + count, 2 * hid), X), (max(start, 2 * hid), min(start + count, 3 * hid), G)):
            if lo < hi:
                for n in range(4):
                    PW[pl.ds(lo, hi - lo), pl.ds(n * 256, 256)] = (
                        factor * nn(H[pl.ds(lo, hi - lo), :], tokens[:, pl.ds(n * 256, 256)])
                    ).astype(BF16)

    def first_rows():
        for n in range(4):
            lanes = pl.ds(n * 256, 256)
            PW[first, lanes] = (factor * (SUM[:, lanes] + nn(H[first, late], X[late, lanes]))).astype(BF16)

    def input_piece(c):
        DX[pl.ds(c * 256, 256), :] = tn(
            H[pl.ds(0, 2 * hid), pl.ds(c * 256, 256)], WT[pl.ds(0, 2 * hid), :]
        ).astype(BF16)

    def across(s):
        landing = DS.at[pl.ds(s * block, block)]
        return send(slot(DX, s, block), landing, sibling)

    def across_add(k, s):
        arrived(k, DS.at[pl.ds(s * block, block)])
        GX[pl.ds(s * block, block), :] = (
            DX[pl.ds(s * 2 * block, block), :].astype(F32)
            + DS[pl.ds(s * block, block), :].astype(F32)
        ).astype(BF16)

    blank = PW.shape[0] - 3 * hid
    PW[pl.ds(3 * hid, blank), :] = jnp.zeros((blank, width), BF16)
    first_rows()
    zb[0].start_far()
    zb[0].start_near()
    weight_piece(2, 0, A[0])
    ya[0].start_far()
    weight_rows(b_at[1], B[1])
    zb[1].start_far()
    weight_piece(1, 0, A[0])
    weight_piece(3, 0, A[0])
    ya[0].start_near()
    weight_rows(a_at[1], A[1])
    ya[1].start_far()
    zb[1].start_near()
    weight_rows(b_at[2], B[2])
    zb[2].start_far()
    weight_rows(a_at[2], A[2])
    ya[1].start_near()
    ya[2].start_far()
    input_piece(2)
    opp = across(OPP)
    zb[0].relay()
    input_piece(1)
    near = across(LEFT), across(RIGHT)
    ya[0].relay()
    input_piece(0)
    mine = across(SELF)
    weight_piece(0, 0, A[0])
    across_add(opp, OPP)
    xr.start_far()
    zb[1].relay()
    zb[2].start_near()
    across_add(near[0], LEFT)
    across_add(near[1], RIGHT)
    xr.start_near()
    ya[1].relay()
    ya[2].start_near()
    across_add(mine, SELF)
    zb[2].relay()
    zb[0].finish(keep(ZB[0]))
    yb[0].start()
    ya[2].relay()
    ya[0].finish(keep(YA[0]))
    za[0].start()
    zb[1].finish(keep(ZB[1]))
    yb[1].start()
    ya[1].finish(keep(YA[1]))
    za[1].start()
    zb[2].finish(keep(ZB[2]))
    yb[2].start()
    xr.relay()
    yb[0].finish(gb[0].row(0))
    gb[0].start()
    ya[2].finish(keep(YA[2]))
    za[2].start()
    za[0].finish(ga[0].row(0))
    ga[0].start()
    za[1].finish(ga[1].row(0))
    ga[1].start()
    yb[1].finish(gb[1].row(0))
    gb[1].start()
    yb[2].finish(gb[2].row(0))
    gb[2].start()
    za[2].finish(ga[2].row(0))
    ga[2].start()
    xr.finish(keep(gin_out))
    gb[0].finish()
    ga[0].finish()
    ga[1].finish()
    gb[1].finish()
    gb[2].finish()
    ga[2].finish()
    og_out[...] = OUTT[pl.ds(0, hid), :].astype(F32)
    ou_out[...] = OUTT[pl.ds(hid, hid), :].astype(F32)
    od_out[...] = OUTT[pl.ds(2 * hid, hid), :].astype(F32)

    for copy in pending:
        copy.wait_send()


def writer(*refs):
    sources, targets, sems = refs[:4], refs[4:8], refs[8]
    copies = [pltpu.make_async_copy(a, b, sems.at[i]) for i, (a, b) in enumerate(zip(sources, targets))]
    for copy in copies:
        copy.start()
    for copy in copies:
        copy.wait()


def body(tokens_in, out_grad, gate_weight, up_weight, down_weight):
    block, width = tokens_in.shape
    shard, hid = gate_weight.shape
    devices = lax.axis_size("rep") * lax.axis_size("fs") * lax.axis_size("tp")
    factor = (block * devices) ** (-0.5)
    tokens = block * 8
    A, B = SPLIT
    total_rows = sum(A) + sum(B)

    def ring(count, lanes):
        return [
            pltpu.VMEM((count, lanes // 2), BF16),
            pltpu.VMEM((count, lanes // 2), BF16),
            pltpu.VMEM((count, lanes), BF16),
            pltpu.VMEM((count, lanes), BF16),
        ]

    def exchange(count):
        return [pltpu.VMEM((count // 4, shard), BF16)] * 3

    outs = (
        jax.ShapeDtypeStruct((block, width), BF16),
        jax.ShapeDtypeStruct((hid, shard), F32),
        jax.ShapeDtypeStruct((hid, shard), F32),
        jax.ShapeDtypeStruct((hid, shard), F32),
    )
    arrays = tokens_in, out_grad, gate_weight.T, up_weight.T, down_weight
    results = pl.pallas_call(
        functools.partial(kernel, factor, block, width, hid),
        out_shape=outs,
        in_specs=[pl.BlockSpec(memory_space=pltpu.HBM)] * 5,
        out_specs=[pl.BlockSpec(memory_space=pltpu.VMEM)] * 4,
        scratch_shapes=[
            pltpu.VMEM((tokens, width), BF16),
            pltpu.VMEM((tokens, width), BF16),
            pltpu.VMEM((3 * hid, width), BF16),
            pltpu.VMEM((3 * hid, tokens), BF16),
            pltpu.VMEM((hid, tokens), F32),
            pltpu.VMEM((hid, tokens), F32),
            pltpu.VMEM((B[0], width), F32),
            pltpu.VMEM((total_rows, width), BF16),
            pltpu.VMEM((tokens, width), BF16),
            pltpu.VMEM((tokens // 2, width), BF16),
            pltpu.VMEM((tokens // 2, width), BF16),
            [pltpu.VMEM((n, shard), BF16) for n in A],
            [pltpu.VMEM((n // 4, width), BF16) for n in B],
            pltpu.VMEM((total_rows, shard), BF16),
            [ring(n, shard) for n in A],
            [ring(n // 4, width) for n in B],
            [exchange(n) for n in A],
            [exchange(n) for n in B],
            ring(block, width),
            pltpu.SemaphoreType.DMA((COPIES,)),
            pltpu.SemaphoreType.DMA((COPIES,)),
            pltpu.SemaphoreType.DMA((5,)),
        ],
        compiler_params=pltpu.CompilerParams(
            collective_id=0, has_side_effects=True, vmem_limit_bytes=48 * 1024 * 1024
        ),
    )(*[pltpu.with_memory_space_constraint(a, pltpu.HBM) for a in arrays])
    grad_in, gate_t, up_t, down_t = pl.pallas_call(
        writer,
        out_shape=outs,
        in_specs=[pl.BlockSpec(memory_space=pl.ANY)] * 4,
        out_specs=[pl.BlockSpec(memory_space=pltpu.HBM)] * 4,
        scratch_shapes=[pltpu.SemaphoreType.DMA((4,))],
        compiler_params=pltpu.CompilerParams(vmem_limit_bytes=1024 * 1024),
    )(*results)
    return grad_in, gate_t.T, up_t.T, down_t


def solution(mesh):
    return jax.shard_map(
        body,
        mesh=mesh,
        in_specs=(
            P(("rep", "fs", "tp"), None),
            P(("rep", "fs", "tp"), None),
            P("fs", "tp"),
            P("fs", "tp"),
            P("tp", "fs"),
        ),
        out_specs=(P(("rep", "fs", "tp"), None), P("fs", "tp"), P("fs", "tp"), P("tp", "fs")),
        check_vma=False,
    )
```

```python
import functools

import jax
import jax.numpy as jnp
from jax import lax
from jax.experimental import pallas as pl
from jax.experimental.pallas import tpu as pltpu
from jax.sharding import PartitionSpec as P

BF16 = jnp.bfloat16
F32 = jnp.float32
MESH = pl.DeviceIdType.MESH
COPIES = 144
SPLIT = (128, 256, 192), (128, 192, 192)


def nt(left, right):
    return lax.dot_general(left, right, (((1,), (1,)), ((), ())), preferred_element_type=F32)


def tn(left, right):
    return lax.dot_general(left, right, (((0,), (0,)), ((), ())), preferred_element_type=F32)


def nn(left, right):
    return lax.dot_general(left, right, (((1,), (0,)), ((), ())), preferred_element_type=F32)


def kernel(
    factor, block, width, hid,
    x_in, g_in, wg_in, wu_in, wd_in,
    gin_out, og_out, ou_out, od_out,
    X, G, WT, H, ACT, SLOPE, PW, DX, DS, GX, YA, ZB, OUTT, YA_BUFS, ZB_BUFS, ZA_BUFS, YB_BUFS, XR_BUFS,
    send_sems, recv_sems, local_sems,
):
    rep = lax.axis_index("rep")
    fs = lax.axis_index("fs")
    tp = lax.axis_index("tp")
    core = lax.rem(tp, 2)
    xpos = tp // 2
    shard = width // 4

    def turn(pos, step):
        return lax.rem(pos + step, 4)

    def at_x(step):
        return {"tp": turn(xpos, step) * 2 + core}

    def at_y(step):
        return {"fs": turn(fs, step)}

    def at_z(step):
        return {"rep": turn(rep, step)}

    sibling = {"tp": tp + 1 - 2 * core}

    def lanes_of(step):
        return pl.ds(pl.multiple_of(turn(fs, step) * shard, shard), shard)

    counter = [0]
    pending = []

    def remote(src, dst, k, where):
        return pltpu.make_async_remote_copy(
            src_ref=src, dst_ref=dst, send_sem=send_sems.at[k], recv_sem=recv_sems.at[k],
            device_id=where, device_id_type=MESH,
        )

    def send(src, dst, where):
        k = counter[0]
        counter[0] += 1
        copy = remote(src, dst, k, where)
        copy.start()
        pending.append(copy)
        return k

    def arrived(k, landing):
        remote(landing, landing, k, sibling).wait_recv()

    barrier = pltpu.get_barrier_semaphore()
    partners = [sibling] + [at(step) for at in (at_x, at_y, at_z) for step in (1, 3)]
    partners += [at_y(2), at_z(2)]
    for where in partners:
        pl.semaphore_signal(barrier, inc=1, device_id=where, device_id_type=MESH)

    own_lanes = lanes_of(0)
    loads = [
        pltpu.make_async_copy(x_in, X.at[pl.ds(0, block)], local_sems.at[0]),
        pltpu.make_async_copy(g_in, G.at[pl.ds(0, block)], local_sems.at[1]),
        pltpu.make_async_copy(wg_in, WT.at[pl.ds(0, hid), own_lanes], local_sems.at[2]),
        pltpu.make_async_copy(wu_in, WT.at[pl.ds(hid, hid), own_lanes], local_sems.at[3]),
        pltpu.make_async_copy(wd_in, WT.at[pl.ds(2 * hid, hid), own_lanes], local_sems.at[4]),
    ]
    for load in loads:
        load.start()

    pl.semaphore_wait(barrier, len(partners))

    half = block // 2
    SELF, LEFT, RIGHT, OPP = 0, 1, 2, 3

    def slot(buf, s, start=0, count=block):
        return buf.at[pl.ds(s * 2 * block + start, count)]

    def forward(buf, s, start=0, count=block):
        landing = (s, block + start, count)
        return send(slot(buf, s, start, count), slot(buf, *landing), sibling), landing

    def forwarded(buf, *states):
        for k, landing in states:
            arrived(k, slot(buf, *landing))

    class Tokens:
        def __init__(self, buf):
            self.buf = buf

        def part(self, s, which):
            return slot(self.buf, s, which * half, half)

        def start_first(self):
            self.r0 = send(self.part(SELF, 0), self.part(LEFT, 0), at_x(1))
            self.l1 = send(self.part(SELF, 1), self.part(RIGHT, 1), at_x(3))

        def start_second(self):
            self.r1 = send(self.part(SELF, 1), self.part(LEFT, 1), at_x(1))
            self.l0 = send(self.part(SELF, 0), self.part(RIGHT, 0), at_x(3))

        def relay(self):
            arrived(self.r0, self.part(LEFT, 0))
            self.r2 = send(self.part(LEFT, 0), self.part(OPP, 0), at_x(1))
            arrived(self.l1, self.part(RIGHT, 1))
            self.l2 = send(self.part(RIGHT, 1), self.part(OPP, 1), at_x(3))

        def near(self):
            arrived(self.r1, self.part(LEFT, 1))
            arrived(self.l0, self.part(RIGHT, 0))
            return forward(self.buf, LEFT), forward(self.buf, RIGHT)

        def far(self):
            arrived(self.r2, self.part(OPP, 0))
            first = forward(self.buf, OPP, 0, half)
            arrived(self.l2, self.part(OPP, 1))
            return first, forward(self.buf, OPP, half, half)

    xt, gt = Tokens(X), Tokens(G)
    loads[0].wait()
    xt.start_first()
    xt.start_second()
    loads[1].wait()
    gt.start_first()
    for load in loads[2:]:
        load.wait()

    direct, spare = 384, 96
    base1, base2 = direct, 2 * hid + spare
    dhalf = direct // 2
    D0, D1 = pl.ds(0, dhalf), pl.ds(dhalf, dhalf)
    D2 = pl.ds(2 * hid, spare)

    def w(rows, step):
        return WT.at[rows, lanes_of(step)]

    def copy_w(rows, step, where):
        return send(w(rows, step), w(rows, step), where)

    class Quarters:
        def __init__(self, base, end):
            self.base, self.part = base, (end - base) // 4
            self.cut = (self.part // 2 + 15) // 16 * 16

        def rows(self, step, which=None):
            start, count = {
                None: (0, self.part), 0: (0, self.cut), 1: (self.cut, self.part - self.cut)
            }[which]
            return pl.ds(pl.multiple_of(self.base + turn(rep, step) * self.part + start, 16), count)

        def start(self):
            self.r, self.l = copy_w(self.rows(0), 0, at_y(1)), copy_w(self.rows(0), 0, at_y(3))
            self.shares = {}

        def relay(self):
            arrived(self.r, w(self.rows(0), 3))
            self.r2 = copy_w(self.rows(0, 0), 3, at_y(1))
            arrived(self.l, w(self.rows(0), 1))
            self.l2 = copy_w(self.rows(0, 1), 1, at_y(3))

        def far(self):
            arrived(self.r2, w(self.rows(0, 0), 2))
            arrived(self.l2, w(self.rows(0, 1), 2))

        def share(self, lane):
            self.shares[lane] = [
                (copy_w(self.rows(0), lane, at_z(step)), 4 - step) for step in (2, 1, 3)
            ]

        def finish(self):
            for lane, keys in self.shares.items():
                for k, step in keys:
                    arrived(k, w(self.rows(step), lane))

    q1, q2 = Quarters(base1, 2 * hid), Quarters(base2, 3 * hid)
    q1.start()
    q2.start()
    d0r = copy_w(D0, 0, at_y(1))
    d1l = copy_w(D1, 0, at_y(3))
    x_own = forward(X, SELF)
    g_own = forward(G, SELF)

    q1.relay()
    q1.share(3)
    q1.share(1)
    q2.relay()
    d1r = copy_w(D1, 0, at_y(1))
    d0l = copy_w(D0, 0, at_y(3))

    xt.relay()
    gt.start_second()
    arrived(d0r, w(D0, 3))
    dc = copy_w(D0, 3, at_y(1))
    arrived(d1l, w(D1, 1))
    dd = copy_w(D1, 1, at_y(3))
    x_near = xt.near()
    q1.far()
    q1.share(2)
    q2.share(3)
    q2.share(1)
    q2.far()
    q2.share(2)
    d2 = [(copy_w(D2, 0, at_y(step)), 4 - step) for step in (2, 1, 3)]
    gt.relay()
    x_far = xt.far()

    forwarded(X, x_own, *x_near)
    arrived(d1r, w(D1, 3))
    arrived(d0l, w(D0, 1))
    q1.finish()
    arrived(dc, w(D0, 2))
    arrived(dd, w(D1, 2))

    rows = hid // 2

    def gate_stage(c):
        cols = pl.ds(c * 256, 256)
        for p in range(2):
            part_rows = pl.ds(p * rows, rows)
            gate = nt(WT[part_rows, :], X[cols, :]).astype(BF16).astype(F32)
            up = nt(WT[pl.ds(hid + p * rows, rows), :], X[cols, :]).astype(BF16).astype(F32)
            sig = jax.nn.sigmoid(gate)
            act = gate * sig
            H[pl.ds(2 * hid + p * rows, rows), cols] = (act * up).astype(BF16)
            ACT[part_rows, cols] = act
            SLOPE[part_rows, cols] = up * sig * (1.0 + gate * (1.0 - sig))

    def grad_stage(c):
        cols = pl.ds(c * 256, 256)
        grad = nt(WT[pl.ds(2 * hid, hid), :], G[cols, :]).astype(BF16).astype(F32)
        H[pl.ds(0, hid), cols] = (grad * SLOPE[:, cols]).astype(BF16)
        H[pl.ds(hid, hid), cols] = (grad * ACT[:, cols]).astype(BF16)

    gate_stage(0)
    gate_stage(1)
    g_near = gt.near()
    forwarded(X, *x_far)
    gate_stage(2)
    q2.finish()
    for k, step in d2:
        arrived(k, w(D2, step))
    forwarded(G, g_own, g_near[0])
    g_far = gt.far()
    grad_stage(0)
    forwarded(G, g_near[1])
    grad_stage(1)
    forwarded(G, *g_far)
    grad_stage(2)

    class Ring:
        def __init__(self, piece, bufs, dest):
            self.piece, self.dest = piece, dest
            self.t0, self.t1, self.fl, self.fr = bufs
            self.h = self.t0.shape[1]

        def side(self, buf, which):
            return buf.at[:, pl.ds(which * self.h, self.h)]

        def start_far(self):
            self.a = send(self.piece(2, 0), self.t0, self.dest(1))
            self.b = send(self.piece(2, 1), self.t1, self.dest(3))

        def start_near(self):
            self.c = send(self.piece(1, 1), self.side(self.fl, 1), self.dest(1))
            self.d = send(self.piece(3, 0), self.side(self.fr, 0), self.dest(3))

        def relay(self):
            arrived(self.a, self.t0)
            self.t0[...] = (self.t0[...].astype(F32) + self.piece(1, 0)[...].astype(F32)).astype(BF16)
            self.e = send(self.t0, self.side(self.fl, 0), self.dest(1))
            arrived(self.b, self.t1)
            self.t1[...] = (self.t1[...].astype(F32) + self.piece(3, 1)[...].astype(F32)).astype(BF16)
            self.f = send(self.t1, self.side(self.fr, 1), self.dest(3))

        def finish(self, store):
            arrived(self.c, self.side(self.fl, 1))
            arrived(self.d, self.side(self.fr, 0))
            arrived(self.e, self.side(self.fl, 0))
            arrived(self.f, self.side(self.fr, 1))
            for which in range(2):
                total = (
                    self.piece(0, which)[...].astype(F32)
                    + self.side(self.fl, which)[...].astype(F32)
                    + self.side(self.fr, which)[...].astype(F32)
                )
                store(which, total.astype(BF16))

    def y_piece(buf, start, count):
        def piece(step, which):
            lane = pl.multiple_of(turn(fs, step) * shard + which * (shard // 2), 128)
            return buf.at[pl.ds(start, count), pl.ds(lane, shard // 2)]
        return piece

    def z_piece(buf, start, count, lanes):
        def piece(step, which):
            row = pl.multiple_of(start + turn(rep, step) * count, 16)
            return buf.at[pl.ds(row, count), pl.ds(which * lanes, lanes)]
        return piece

    def x_piece(step, which):
        s = {0: SELF, 1: RIGHT, 3: LEFT, 2: OPP}[step]
        return GX.at[pl.ds(s * block, block), pl.ds(which * (width // 2), width // 2)]

    def strip(buf, count):
        def piece(step):
            row = pl.multiple_of(turn(rep, step) * (count // 4), 16)
            return buf.at[pl.ds(row, count // 4)]
        return piece

    def column(buf):
        def piece(step):
            return buf.at[:, lanes_of(step)]
        return piece

    class Exchange:
        def __init__(self, piece, bufs, dest):
            self.piece, self.bufs, self.dest = piece, bufs, dest

        def start(self):
            self.keys = [
                (send(self.piece(step), self.bufs[step - 1], self.dest(step)), self.bufs[step - 1])
                for step in (2, 1, 3)
            ]

        def finish(self, start):
            for k, landing in self.keys:
                arrived(k, landing)
            total = self.piece(0)[...].astype(F32)
            for buf in self.bufs:
                total = total + buf[...].astype(F32)
            OUTT[pl.ds(start, total.shape[0]), :] = total.astype(BF16)

    class Gather:
        def __init__(self, base, count):
            self.base, self.count = base, count // 4

        def row(self, step):
            return pl.multiple_of(self.base + turn(rep, step) * self.count, 16)

        def region(self, step):
            return OUTT.at[pl.ds(self.row(step), self.count)]

        def start(self):
            self.keys = [
                (send(self.region(0), self.region(0), at_z(step)), 4 - step) for step in (2, 1, 3)
            ]

        def finish(self):
            for k, step in self.keys:
                arrived(k, self.region(step))

    A, B = SPLIT
    a_at = [sum(A[:i]) for i in range(len(A))]
    b_at = [sum(A) + sum(B[:i]) for i in range(len(B))]
    ya = [Ring(y_piece(PW, r, n), bufs, at_y) for r, n, bufs in zip(a_at, A, YA_BUFS)]
    zb = [Ring(z_piece(PW, r, n // 4, width // 2), bufs, at_z) for r, n, bufs in zip(b_at, B, ZB_BUFS)]
    za = [Exchange(strip(buf, n), bufs, at_z) for buf, n, bufs in zip(YA, A, ZA_BUFS)]
    yb = [Exchange(column(buf), bufs, at_y) for buf, bufs in zip(ZB, YB_BUFS)]
    ga = [Gather(r, n) for r, n in zip(a_at, A)]
    gb = [Gather(r, n) for r, n in zip(b_at, B)]
    xr = Ring(x_piece, XR_BUFS, at_x)

    def keep(buf):
        def store(which, value):
            h = value.shape[1]
            buf[:, pl.ds(which * h, h)] = value
        return store

    def weight_piece(step, start, count):
        lanes = lanes_of(step)
        PW[pl.ds(start, count), lanes] = (
            factor * nn(H[pl.ds(start, count), :], X[:, lanes])
        ).astype(BF16)

    def weight_rows(start, count):
        for lo, hi, tokens in ((start, min(start + count, 2 * hid), X), (max(start, 2 * hid), min(start + count, 3 * hid), G)):
            if lo < hi:
                for n in range(4):
                    PW[pl.ds(lo, hi - lo), pl.ds(n * 256, 256)] = (
                        factor * nn(H[pl.ds(lo, hi - lo), :], tokens[:, pl.ds(n * 256, 256)])
                    ).astype(BF16)

    def input_piece(c):
        DX[pl.ds(c * 256, 256), :] = tn(
            H[pl.ds(0, 2 * hid), pl.ds(c * 256, 256)], WT[pl.ds(0, 2 * hid), :]
        ).astype(BF16)

    def across(s):
        landing = DS.at[pl.ds(s * block, block)]
        return send(slot(DX, s, block), landing, sibling)

    def across_add(k, s):
        arrived(k, DS.at[pl.ds(s * block, block)])
        GX[pl.ds(s * block, block), :] = (
            DX[pl.ds(s * 2 * block, block), :].astype(F32)
            + DS[pl.ds(s * block, block), :].astype(F32)
        ).astype(BF16)

    blank = PW.shape[0] - 3 * hid
    PW[pl.ds(3 * hid, blank), :] = jnp.zeros((blank, width), BF16)
    weight_piece(2, 0, A[0])
    ya[0].start_far()
    weight_rows(b_at[0], B[0])
    zb[0].start_far()
    weight_piece(1, 0, A[0])
    weight_piece(3, 0, A[0])
    ya[0].start_near()
    weight_rows(a_at[1], A[1])
    zb[0].start_near()
    weight_rows(b_at[1], B[1])
    ya[1].start_far()
    weight_rows(a_at[2], A[2])
    zb[1].start_far()
    weight_rows(b_at[2], B[2])
    input_piece(2)
    opp = across(OPP)
    ya[1].start_near()
    zb[1].start_near()
    ya[0].relay()
    zb[0].relay()
    input_piece(1)
    near = across(LEFT), across(RIGHT)
    input_piece(0)
    mine = across(SELF)
    weight_piece(0, 0, A[0])
    across_add(opp, OPP)
    xr.start_far()
    zb[2].start_far()
    ya[2].start_far()
    across_add(near[0], LEFT)
    across_add(near[1], RIGHT)
    xr.start_near()
    ya[1].relay()
    zb[1].relay()
    across_add(mine, SELF)
    zb[2].start_near()
    zb[0].finish(keep(ZB[0]))
    yb[0].start()
    ya[0].finish(keep(YA[0]))
    za[0].start()
    ya[2].start_near()
    zb[2].relay()
    ya[2].relay()
    xr.relay()
    zb[1].finish(keep(ZB[1]))
    yb[1].start()
    ya[1].finish(keep(YA[1]))
    za[1].start()
    yb[0].finish(gb[0].row(0))
    gb[0].start()
    za[0].finish(ga[0].row(0))
    ga[0].start()
    zb[2].finish(keep(ZB[2]))
    yb[2].start()
    ya[2].finish(keep(YA[2]))
    za[2].start()
    xr.finish(keep(gin_out))
    yb[1].finish(gb[1].row(0))
    gb[1].start()
    za[1].finish(ga[1].row(0))
    ga[1].start()
    gb[0].finish()
    ga[0].finish()
    yb[2].finish(gb[2].row(0))
    gb[2].start()
    za[2].finish(ga[2].row(0))
    ga[2].start()
    gb[1].finish()
    ga[1].finish()
    gb[2].finish()
    ga[2].finish()
    og_out[...] = OUTT[pl.ds(0, hid), :].astype(F32)
    ou_out[...] = OUTT[pl.ds(hid, hid), :].astype(F32)
    od_out[...] = OUTT[pl.ds(2 * hid, hid), :].astype(F32)

    for copy in pending:
        copy.wait_send()


def writer(*refs):
    sources, targets, sems = refs[:4], refs[4:8], refs[8]
    copies = [pltpu.make_async_copy(a, b, sems.at[i]) for i, (a, b) in enumerate(zip(sources, targets))]
    for copy in copies:
        copy.start()
    for copy in copies:
        copy.wait()


def body(tokens_in, out_grad, gate_weight, up_weight, down_weight):
    block, width = tokens_in.shape
    shard, hid = gate_weight.shape
    devices = lax.axis_size("rep") * lax.axis_size("fs") * lax.axis_size("tp")
    factor = (block * devices) ** (-0.5)
    tokens = block * 8
    A, B = SPLIT
    total_rows = sum(A) + sum(B)

    def ring(count, lanes):
        return [
            pltpu.VMEM((count, lanes // 2), BF16),
            pltpu.VMEM((count, lanes // 2), BF16),
            pltpu.VMEM((count, lanes), BF16),
            pltpu.VMEM((count, lanes), BF16),
        ]

    def exchange(count):
        return [pltpu.VMEM((count // 4, shard), BF16)] * 3

    outs = (
        jax.ShapeDtypeStruct((block, width), BF16),
        jax.ShapeDtypeStruct((hid, shard), F32),
        jax.ShapeDtypeStruct((hid, shard), F32),
        jax.ShapeDtypeStruct((hid, shard), F32),
    )
    arrays = tokens_in, out_grad, gate_weight.T, up_weight.T, down_weight
    results = pl.pallas_call(
        functools.partial(kernel, factor, block, width, hid),
        out_shape=outs,
        in_specs=[pl.BlockSpec(memory_space=pltpu.HBM)] * 5,
        out_specs=[pl.BlockSpec(memory_space=pltpu.VMEM)] * 4,
        scratch_shapes=[
            pltpu.VMEM((tokens, width), BF16),
            pltpu.VMEM((tokens, width), BF16),
            pltpu.VMEM((3 * hid, width), BF16),
            pltpu.VMEM((3 * hid, tokens), BF16),
            pltpu.VMEM((hid, tokens), F32),
            pltpu.VMEM((hid, tokens), F32),
            pltpu.VMEM((total_rows, width), BF16),
            pltpu.VMEM((tokens, width), BF16),
            pltpu.VMEM((tokens // 2, width), BF16),
            pltpu.VMEM((tokens // 2, width), BF16),
            [pltpu.VMEM((n, shard), BF16) for n in A],
            [pltpu.VMEM((n // 4, width), BF16) for n in B],
            pltpu.VMEM((total_rows, shard), BF16),
            [ring(n, shard) for n in A],
            [ring(n // 4, width) for n in B],
            [exchange(n) for n in A],
            [exchange(n) for n in B],
            ring(block, width),
            pltpu.SemaphoreType.DMA((COPIES,)),
            pltpu.SemaphoreType.DMA((COPIES,)),
            pltpu.SemaphoreType.DMA((5,)),
        ],
        compiler_params=pltpu.CompilerParams(
            collective_id=0, has_side_effects=True, vmem_limit_bytes=48 * 1024 * 1024
        ),
    )(*[pltpu.with_memory_space_constraint(a, pltpu.HBM) for a in arrays])
    grad_in, gate_t, up_t, down_t = pl.pallas_call(
        writer,
        out_shape=outs,
        in_specs=[pl.BlockSpec(memory_space=pl.ANY)] * 4,
        out_specs=[pl.BlockSpec(memory_space=pltpu.HBM)] * 4,
        scratch_shapes=[pltpu.SemaphoreType.DMA((4,))],
        compiler_params=pltpu.CompilerParams(vmem_limit_bytes=1024 * 1024),
    )(*results)
    return grad_in, gate_t.T, up_t.T, down_t


def solution(mesh):
    return jax.shard_map(
        body,
        mesh=mesh,
        in_specs=(
            P(("rep", "fs", "tp"), None),
            P(("rep", "fs", "tp"), None),
            P("fs", "tp"),
            P("fs", "tp"),
            P("tp", "fs"),
        ),
        out_specs=(P(("rep", "fs", "tp"), None), P("fs", "tp"), P("fs", "tp"), P("tp", "fs")),
        check_vma=False,
    )
```

```python
import functools

import jax
import jax.numpy as jnp
from jax import lax
from jax.experimental import pallas as pl
from jax.experimental.pallas import tpu as pltpu
from jax.sharding import PartitionSpec as P

BF16 = jnp.bfloat16
F32 = jnp.float32
MESH = pl.DeviceIdType.MESH
COPIES = 144
SPLIT = (128, 256, 192), (128, 192, 192)


def nt(left, right):
    return lax.dot_general(left, right, (((1,), (1,)), ((), ())), preferred_element_type=F32)


def tn(left, right):
    return lax.dot_general(left, right, (((0,), (0,)), ((), ())), preferred_element_type=F32)


def nn(left, right):
    return lax.dot_general(left, right, (((1,), (0,)), ((), ())), preferred_element_type=F32)


def kernel(
    factor, block, width, hid,
    x_in, g_in, wg_in, wu_in, wd_in,
    gin_out, og_out, ou_out, od_out,
    X, G, WT, H, ACT, SLOPE, PW, DX, DS, GX, YA, ZB, OUTT, YA_BUFS, ZB_BUFS, ZA_BUFS, YB_BUFS, XR_BUFS,
    send_sems, recv_sems, local_sems,
):
    rep = lax.axis_index("rep")
    fs = lax.axis_index("fs")
    tp = lax.axis_index("tp")
    core = lax.rem(tp, 2)
    xpos = tp // 2
    shard = width // 4

    def turn(pos, step):
        return lax.rem(pos + step, 4)

    def at_x(step):
        return {"tp": turn(xpos, step) * 2 + core}

    def at_y(step):
        return {"fs": turn(fs, step)}

    def at_z(step):
        return {"rep": turn(rep, step)}

    sibling = {"tp": tp + 1 - 2 * core}

    def lanes_of(step):
        return pl.ds(pl.multiple_of(turn(fs, step) * shard, shard), shard)

    counter = [0]
    pending = []

    def remote(src, dst, k, where):
        return pltpu.make_async_remote_copy(
            src_ref=src, dst_ref=dst, send_sem=send_sems.at[k], recv_sem=recv_sems.at[k],
            device_id=where, device_id_type=MESH,
        )

    def send(src, dst, where):
        k = counter[0]
        counter[0] += 1
        copy = remote(src, dst, k, where)
        copy.start()
        pending.append(copy)
        return k

    def arrived(k, landing):
        remote(landing, landing, k, sibling).wait_recv()

    barrier = pltpu.get_barrier_semaphore()
    partners = [sibling] + [at(step) for at in (at_x, at_y, at_z) for step in (1, 3)]
    partners += [at_y(2), at_z(2)]
    for where in partners:
        pl.semaphore_signal(barrier, inc=1, device_id=where, device_id_type=MESH)

    own_lanes = lanes_of(0)
    loads = [
        pltpu.make_async_copy(x_in, X.at[pl.ds(0, block)], local_sems.at[0]),
        pltpu.make_async_copy(g_in, G.at[pl.ds(0, block)], local_sems.at[1]),
        pltpu.make_async_copy(wg_in, WT.at[pl.ds(0, hid), own_lanes], local_sems.at[2]),
        pltpu.make_async_copy(wu_in, WT.at[pl.ds(hid, hid), own_lanes], local_sems.at[3]),
        pltpu.make_async_copy(wd_in, WT.at[pl.ds(2 * hid, hid), own_lanes], local_sems.at[4]),
    ]
    for load in loads:
        load.start()

    pl.semaphore_wait(barrier, len(partners))

    half = block // 2
    SELF, LEFT, RIGHT, OPP = 0, 1, 2, 3

    def slot(buf, s, start=0, count=block):
        return buf.at[pl.ds(s * 2 * block + start, count)]

    def forward(buf, s, start=0, count=block):
        landing = (s, block + start, count)
        return send(slot(buf, s, start, count), slot(buf, *landing), sibling), landing

    def forwarded(buf, *states):
        for k, landing in states:
            arrived(k, slot(buf, *landing))

    class Tokens:
        def __init__(self, buf):
            self.buf = buf

        def part(self, s, which):
            return slot(self.buf, s, which * half, half)

        def start_first(self):
            self.r0 = send(self.part(SELF, 0), self.part(LEFT, 0), at_x(1))
            self.l1 = send(self.part(SELF, 1), self.part(RIGHT, 1), at_x(3))

        def start_second(self):
            self.r1 = send(self.part(SELF, 1), self.part(LEFT, 1), at_x(1))
            self.l0 = send(self.part(SELF, 0), self.part(RIGHT, 0), at_x(3))

        def relay(self):
            arrived(self.r0, self.part(LEFT, 0))
            self.r2 = send(self.part(LEFT, 0), self.part(OPP, 0), at_x(1))
            arrived(self.l1, self.part(RIGHT, 1))
            self.l2 = send(self.part(RIGHT, 1), self.part(OPP, 1), at_x(3))

        def near(self):
            arrived(self.r1, self.part(LEFT, 1))
            arrived(self.l0, self.part(RIGHT, 0))
            return forward(self.buf, LEFT), forward(self.buf, RIGHT)

        def far(self):
            arrived(self.r2, self.part(OPP, 0))
            first = forward(self.buf, OPP, 0, half)
            arrived(self.l2, self.part(OPP, 1))
            return first, forward(self.buf, OPP, half, half)

    xt, gt = Tokens(X), Tokens(G)
    loads[0].wait()
    xt.start_first()
    xt.start_second()
    loads[1].wait()
    gt.start_first()
    for load in loads[2:]:
        load.wait()

    direct, spare = 384, 96
    base1, base2 = direct, 2 * hid + spare
    dhalf = direct // 2
    D0, D1 = pl.ds(0, dhalf), pl.ds(dhalf, dhalf)
    D2 = pl.ds(2 * hid, spare)

    def w(rows, step):
        return WT.at[rows, lanes_of(step)]

    def copy_w(rows, step, where):
        return send(w(rows, step), w(rows, step), where)

    class Quarters:
        def __init__(self, base, end):
            self.base, self.part = base, (end - base) // 4
            self.cut = (self.part // 2 + 15) // 16 * 16

        def rows(self, step, which=None):
            start, count = {
                None: (0, self.part), 0: (0, self.cut), 1: (self.cut, self.part - self.cut)
            }[which]
            return pl.ds(pl.multiple_of(self.base + turn(rep, step) * self.part + start, 16), count)

        def start(self):
            self.r, self.l = copy_w(self.rows(0), 0, at_y(1)), copy_w(self.rows(0), 0, at_y(3))
            self.shares = {}

        def relay(self):
            arrived(self.r, w(self.rows(0), 3))
            self.r2 = copy_w(self.rows(0, 0), 3, at_y(1))
            arrived(self.l, w(self.rows(0), 1))
            self.l2 = copy_w(self.rows(0, 1), 1, at_y(3))

        def far(self):
            arrived(self.r2, w(self.rows(0, 0), 2))
            arrived(self.l2, w(self.rows(0, 1), 2))

        def share(self, lane):
            self.shares[lane] = [
                (copy_w(self.rows(0), lane, at_z(step)), 4 - step) for step in (2, 1, 3)
            ]

        def finish(self):
            for lane, keys in self.shares.items():
                for k, step in keys:
                    arrived(k, w(self.rows(step), lane))

    q1, q2 = Quarters(base1, 2 * hid), Quarters(base2, 3 * hid)
    q1.start()
    q2.start()
    d0r = copy_w(D0, 0, at_y(1))
    d1l = copy_w(D1, 0, at_y(3))
    x_own = forward(X, SELF)
    g_own = forward(G, SELF)

    q1.relay()
    q1.share(3)
    q1.share(1)
    q2.relay()
    d1r = copy_w(D1, 0, at_y(1))
    d0l = copy_w(D0, 0, at_y(3))

    xt.relay()
    gt.start_second()
    arrived(d0r, w(D0, 3))
    dc = copy_w(D0, 3, at_y(1))
    arrived(d1l, w(D1, 1))
    dd = copy_w(D1, 1, at_y(3))
    x_near = xt.near()
    q1.far()
    q1.share(2)
    q2.share(3)
    q2.share(1)
    q2.far()
    q2.share(2)
    d2 = [(copy_w(D2, 0, at_y(step)), 4 - step) for step in (2, 1, 3)]
    gt.relay()
    x_far = xt.far()

    forwarded(X, x_own, *x_near)
    arrived(d1r, w(D1, 3))
    arrived(d0l, w(D0, 1))
    q1.finish()
    arrived(dc, w(D0, 2))
    arrived(dd, w(D1, 2))

    rows = hid // 2

    def gate_stage(c):
        cols = pl.ds(c * 256, 256)
        for p in range(2):
            part_rows = pl.ds(p * rows, rows)
            gate = nt(WT[part_rows, :], X[cols, :]).astype(BF16).astype(F32)
            up = nt(WT[pl.ds(hid + p * rows, rows), :], X[cols, :]).astype(BF16).astype(F32)
            sig = jax.nn.sigmoid(gate)
            act = gate * sig
            H[pl.ds(2 * hid + p * rows, rows), cols] = (act * up).astype(BF16)
            ACT[part_rows, cols] = act
            SLOPE[part_rows, cols] = up * sig * (1.0 + gate * (1.0 - sig))

    def grad_stage(c):
        cols = pl.ds(c * 256, 256)
        grad = nt(WT[pl.ds(2 * hid, hid), :], G[cols, :]).astype(BF16).astype(F32)
        H[pl.ds(0, hid), cols] = (grad * SLOPE[:, cols]).astype(BF16)
        H[pl.ds(hid, hid), cols] = (grad * ACT[:, cols]).astype(BF16)

    gate_stage(0)
    gate_stage(1)
    g_near = gt.near()
    forwarded(X, *x_far)
    gate_stage(2)
    q2.finish()
    for k, step in d2:
        arrived(k, w(D2, step))
    forwarded(G, g_own, g_near[0])
    g_far = gt.far()
    grad_stage(0)
    forwarded(G, g_near[1])
    grad_stage(1)
    forwarded(G, *g_far)
    grad_stage(2)

    class Ring:
        def __init__(self, piece, bufs, dest):
            self.piece, self.dest = piece, dest
            self.t0, self.t1, self.fl, self.fr = bufs
            self.h = self.t0.shape[1]

        def side(self, buf, which):
            return buf.at[:, pl.ds(which * self.h, self.h)]

        def start_far(self):
            self.a = send(self.piece(2, 0), self.t0, self.dest(1))
            self.b = send(self.piece(2, 1), self.t1, self.dest(3))

        def start_near(self):
            self.c = send(self.piece(1, 1), self.side(self.fl, 1), self.dest(1))
            self.d = send(self.piece(3, 0), self.side(self.fr, 0), self.dest(3))

        def relay(self):
            arrived(self.a, self.t0)
            self.t0[...] = (self.t0[...].astype(F32) + self.piece(1, 0)[...].astype(F32)).astype(BF16)
            self.e = send(self.t0, self.side(self.fl, 0), self.dest(1))
            arrived(self.b, self.t1)
            self.t1[...] = (self.t1[...].astype(F32) + self.piece(3, 1)[...].astype(F32)).astype(BF16)
            self.f = send(self.t1, self.side(self.fr, 1), self.dest(3))

        def finish(self, store):
            arrived(self.c, self.side(self.fl, 1))
            arrived(self.d, self.side(self.fr, 0))
            arrived(self.e, self.side(self.fl, 0))
            arrived(self.f, self.side(self.fr, 1))
            for which in range(2):
                total = (
                    self.piece(0, which)[...].astype(F32)
                    + self.side(self.fl, which)[...].astype(F32)
                    + self.side(self.fr, which)[...].astype(F32)
                )
                store(which, total.astype(BF16))

    def y_piece(buf, start, count):
        def piece(step, which):
            lane = pl.multiple_of(turn(fs, step) * shard + which * (shard // 2), 128)
            return buf.at[pl.ds(start, count), pl.ds(lane, shard // 2)]
        return piece

    def z_piece(buf, start, count, lanes):
        def piece(step, which):
            row = pl.multiple_of(start + turn(rep, step) * count, 16)
            return buf.at[pl.ds(row, count), pl.ds(which * lanes, lanes)]
        return piece

    def x_piece(step, which):
        s = {0: SELF, 1: RIGHT, 3: LEFT, 2: OPP}[step]
        return GX.at[pl.ds(s * block, block), pl.ds(which * (width // 2), width // 2)]

    def strip(buf, count):
        def piece(step):
            row = pl.multiple_of(turn(rep, step) * (count // 4), 16)
            return buf.at[pl.ds(row, count // 4)]
        return piece

    def column(buf):
        def piece(step):
            return buf.at[:, lanes_of(step)]
        return piece

    class Exchange:
        def __init__(self, piece, bufs, dest):
            self.piece, self.bufs, self.dest = piece, bufs, dest

        def start(self):
            self.keys = [
                (send(self.piece(step), self.bufs[step - 1], self.dest(step)), self.bufs[step - 1])
                for step in (2, 1, 3)
            ]

        def finish(self, start):
            for k, landing in self.keys:
                arrived(k, landing)
            total = self.piece(0)[...].astype(F32)
            for buf in self.bufs:
                total = total + buf[...].astype(F32)
            OUTT[pl.ds(start, total.shape[0]), :] = total.astype(BF16)

    class Gather:
        def __init__(self, base, count):
            self.base, self.count = base, count // 4

        def row(self, step):
            return pl.multiple_of(self.base + turn(rep, step) * self.count, 16)

        def region(self, step):
            return OUTT.at[pl.ds(self.row(step), self.count)]

        def start(self):
            self.keys = [
                (send(self.region(0), self.region(0), at_z(step)), 4 - step) for step in (2, 1, 3)
            ]

        def finish(self):
            for k, step in self.keys:
                arrived(k, self.region(step))

    A, B = SPLIT
    a_at = [sum(A[:i]) for i in range(len(A))]
    b_at = [sum(A) + sum(B[:i]) for i in range(len(B))]
    ya = [Ring(y_piece(PW, r, n), bufs, at_y) for r, n, bufs in zip(a_at, A, YA_BUFS)]
    zb = [Ring(z_piece(PW, r, n // 4, width // 2), bufs, at_z) for r, n, bufs in zip(b_at, B, ZB_BUFS)]
    za = [Exchange(strip(buf, n), bufs, at_z) for buf, n, bufs in zip(YA, A, ZA_BUFS)]
    yb = [Exchange(column(buf), bufs, at_y) for buf, bufs in zip(ZB, YB_BUFS)]
    ga = [Gather(r, n) for r, n in zip(a_at, A)]
    gb = [Gather(r, n) for r, n in zip(b_at, B)]
    xr = Ring(x_piece, XR_BUFS, at_x)

    def keep(buf):
        def store(which, value):
            h = value.shape[1]
            buf[:, pl.ds(which * h, h)] = value
        return store

    def weight_piece(step, start, count):
        lanes = lanes_of(step)
        PW[pl.ds(start, count), lanes] = (
            factor * nn(H[pl.ds(start, count), :], X[:, lanes])
        ).astype(BF16)

    def weight_rows(start, count):
        for lo, hi, tokens in ((start, min(start + count, 2 * hid), X), (max(start, 2 * hid), min(start + count, 3 * hid), G)):
            if lo < hi:
                for n in range(4):
                    PW[pl.ds(lo, hi - lo), pl.ds(n * 256, 256)] = (
                        factor * nn(H[pl.ds(lo, hi - lo), :], tokens[:, pl.ds(n * 256, 256)])
                    ).astype(BF16)

    def input_piece(c):
        DX[pl.ds(c * 256, 256), :] = tn(
            H[pl.ds(0, 2 * hid), pl.ds(c * 256, 256)], WT[pl.ds(0, 2 * hid), :]
        ).astype(BF16)

    def across(s):
        landing = DS.at[pl.ds(s * block, block)]
        return send(slot(DX, s, block), landing, sibling)

    def across_add(k, s):
        arrived(k, DS.at[pl.ds(s * block, block)])
        GX[pl.ds(s * block, block), :] = (
            DX[pl.ds(s * 2 * block, block), :].astype(F32)
            + DS[pl.ds(s * block, block), :].astype(F32)
        ).astype(BF16)

    blank = PW.shape[0] - 3 * hid
    PW[pl.ds(3 * hid, blank), :] = jnp.zeros((blank, width), BF16)
    weight_piece(2, 0, A[0])
    ya[0].start_far()
    weight_rows(b_at[0], B[0])
    zb[0].start_far()
    weight_piece(1, 0, A[0])
    weight_piece(3, 0, A[0])
    ya[0].start_near()
    weight_rows(a_at[1], A[1])
    zb[0].start_near()
    weight_rows(b_at[1], B[1])
    ya[1].start_far()
    weight_rows(a_at[2], A[2])
    zb[1].start_far()
    weight_rows(b_at[2], B[2])
    input_piece(2)
    opp = across(OPP)
    ya[1].start_near()
    zb[1].start_near()
    input_piece(1)
    near = across(LEFT), across(RIGHT)
    ya[0].relay()
    input_piece(0)
    mine = across(SELF)
    zb[0].relay()
    weight_piece(0, 0, A[0])
    across_add(opp, OPP)
    xr.start_far()
    zb[2].start_far()
    ya[2].start_far()
    across_add(near[0], LEFT)
    across_add(near[1], RIGHT)
    xr.start_near()
    ya[1].relay()
    zb[1].relay()
    across_add(mine, SELF)
    zb[2].start_near()
    zb[0].finish(keep(ZB[0]))
    yb[0].start()
    ya[0].finish(keep(YA[0]))
    za[0].start()
    ya[2].start_near()
    zb[2].relay()
    ya[2].relay()
    xr.relay()
    zb[1].finish(keep(ZB[1]))
    yb[1].start()
    ya[1].finish(keep(YA[1]))
    za[1].start()
    yb[0].finish(gb[0].row(0))
    gb[0].start()
    za[0].finish(ga[0].row(0))
    ga[0].start()
    zb[2].finish(keep(ZB[2]))
    yb[2].start()
    ya[2].finish(keep(YA[2]))
    za[2].start()
    xr.finish(keep(gin_out))
    yb[1].finish(gb[1].row(0))
    gb[1].start()
    za[1].finish(ga[1].row(0))
    ga[1].start()
    gb[0].finish()
    ga[0].finish()
    yb[2].finish(gb[2].row(0))
    gb[2].start()
    za[2].finish(ga[2].row(0))
    ga[2].start()
    gb[1].finish()
    ga[1].finish()
    gb[2].finish()
    og_out[...] = OUTT[pl.ds(0, hid), :].astype(F32)
    od_out[...] = OUTT[pl.ds(2 * hid, hid), :].astype(F32)
    for copy in pending[:-3]:
        copy.wait_send()
    ga[2].finish()
    ou_out[...] = OUTT[pl.ds(hid, hid), :].astype(F32)
    for copy in pending[-3:]:
        copy.wait_send()


def writer(*refs):
    sources, targets, sems = refs[:4], refs[4:8], refs[8]
    copies = [pltpu.make_async_copy(a, b, sems.at[i]) for i, (a, b) in enumerate(zip(sources, targets))]
    for copy in copies:
        copy.start()
    for copy in copies:
        copy.wait()


def body(tokens_in, out_grad, gate_weight, up_weight, down_weight):
    block, width = tokens_in.shape
    shard, hid = gate_weight.shape
    devices = lax.axis_size("rep") * lax.axis_size("fs") * lax.axis_size("tp")
    factor = (block * devices) ** (-0.5)
    tokens = block * 8
    A, B = SPLIT
    total_rows = sum(A) + sum(B)

    def ring(count, lanes):
        return [
            pltpu.VMEM((count, lanes // 2), BF16),
            pltpu.VMEM((count, lanes // 2), BF16),
            pltpu.VMEM((count, lanes), BF16),
            pltpu.VMEM((count, lanes), BF16),
        ]

    def exchange(count):
        return [pltpu.VMEM((count // 4, shard), BF16)] * 3

    outs = (
        jax.ShapeDtypeStruct((block, width), BF16),
        jax.ShapeDtypeStruct((hid, shard), F32),
        jax.ShapeDtypeStruct((hid, shard), F32),
        jax.ShapeDtypeStruct((hid, shard), F32),
    )
    arrays = tokens_in, out_grad, gate_weight.T, up_weight.T, down_weight
    results = pl.pallas_call(
        functools.partial(kernel, factor, block, width, hid),
        out_shape=outs,
        in_specs=[pl.BlockSpec(memory_space=pltpu.HBM)] * 5,
        out_specs=[pl.BlockSpec(memory_space=pltpu.VMEM)] * 4,
        scratch_shapes=[
            pltpu.VMEM((tokens, width), BF16),
            pltpu.VMEM((tokens, width), BF16),
            pltpu.VMEM((3 * hid, width), BF16),
            pltpu.VMEM((3 * hid, tokens), BF16),
            pltpu.VMEM((hid, tokens), F32),
            pltpu.VMEM((hid, tokens), F32),
            pltpu.VMEM((total_rows, width), BF16),
            pltpu.VMEM((tokens, width), BF16),
            pltpu.VMEM((tokens // 2, width), BF16),
            pltpu.VMEM((tokens // 2, width), BF16),
            [pltpu.VMEM((n, shard), BF16) for n in A],
            [pltpu.VMEM((n // 4, width), BF16) for n in B],
            pltpu.VMEM((total_rows, shard), BF16),
            [ring(n, shard) for n in A],
            [ring(n // 4, width) for n in B],
            [exchange(n) for n in A],
            [exchange(n) for n in B],
            ring(block, width),
            pltpu.SemaphoreType.DMA((COPIES,)),
            pltpu.SemaphoreType.DMA((COPIES,)),
            pltpu.SemaphoreType.DMA((5,)),
        ],
        compiler_params=pltpu.CompilerParams(
            collective_id=0, has_side_effects=True, vmem_limit_bytes=48 * 1024 * 1024
        ),
    )(*[pltpu.with_memory_space_constraint(a, pltpu.HBM) for a in arrays])
    grad_in, gate_t, up_t, down_t = pl.pallas_call(
        writer,
        out_shape=outs,
        in_specs=[pl.BlockSpec(memory_space=pl.ANY)] * 4,
        out_specs=[pl.BlockSpec(memory_space=pltpu.HBM)] * 4,
        scratch_shapes=[pltpu.SemaphoreType.DMA((4,))],
        compiler_params=pltpu.CompilerParams(vmem_limit_bytes=1024 * 1024),
    )(*results)
    return grad_in, gate_t.T, up_t.T, down_t


def solution(mesh):
    return jax.shard_map(
        body,
        mesh=mesh,
        in_specs=(
            P(("rep", "fs", "tp"), None),
            P(("rep", "fs", "tp"), None),
            P("fs", "tp"),
            P("fs", "tp"),
            P("tp", "fs"),
        ),
        out_specs=(P(("rep", "fs", "tp"), None), P("fs", "tp"), P("fs", "tp"), P("tp", "fs")),
        check_vma=False,
    )
```

```python
import functools

import jax
import jax.numpy as jnp
from jax import lax
from jax.experimental import pallas as pl
from jax.experimental.pallas import tpu as pltpu
from jax.sharding import PartitionSpec as P

BF16 = jnp.bfloat16
F32 = jnp.float32
MESH = pl.DeviceIdType.MESH
COPIES = 144
SPLIT = (128, 256, 192), (128, 192, 192)


def nt(left, right):
    return lax.dot_general(left, right, (((1,), (1,)), ((), ())), preferred_element_type=F32)


def tn(left, right):
    return lax.dot_general(left, right, (((0,), (0,)), ((), ())), preferred_element_type=F32)


def nn(left, right):
    return lax.dot_general(left, right, (((1,), (0,)), ((), ())), preferred_element_type=F32)


def kernel(
    factor, block, width, hid,
    x_in, g_in, wg_in, wu_in, wd_in,
    gin_out, og_out, ou_out, od_out,
    X, G, WT, H, ACT, SLOPE, PW, DX, DS, GX, YA, ZB, OUTT, YA_BUFS, ZB_BUFS, ZA_BUFS, YB_BUFS, XR_BUFS,
    send_sems, recv_sems, local_sems,
):
    rep = lax.axis_index("rep")
    fs = lax.axis_index("fs")
    tp = lax.axis_index("tp")
    core = lax.rem(tp, 2)
    xpos = tp // 2
    shard = width // 4

    def turn(pos, step):
        return lax.rem(pos + step, 4)

    def at_x(step):
        return {"tp": turn(xpos, step) * 2 + core}

    def at_y(step):
        return {"fs": turn(fs, step)}

    def at_z(step):
        return {"rep": turn(rep, step)}

    sibling = {"tp": tp + 1 - 2 * core}

    def lanes_of(step):
        return pl.ds(pl.multiple_of(turn(fs, step) * shard, shard), shard)

    counter = [0]
    pending = []

    def remote(src, dst, k, where):
        return pltpu.make_async_remote_copy(
            src_ref=src, dst_ref=dst, send_sem=send_sems.at[k], recv_sem=recv_sems.at[k],
            device_id=where, device_id_type=MESH,
        )

    def send(src, dst, where):
        k = counter[0]
        counter[0] += 1
        copy = remote(src, dst, k, where)
        copy.start()
        pending.append(copy)
        return k

    def arrived(k, landing):
        remote(landing, landing, k, sibling).wait_recv()

    barrier = pltpu.get_barrier_semaphore()
    partners = [sibling] + [at(step) for at in (at_x, at_y, at_z) for step in (1, 3)]
    partners += [at_y(2), at_z(2)]
    for where in partners:
        pl.semaphore_signal(barrier, inc=1, device_id=where, device_id_type=MESH)

    own_lanes = lanes_of(0)
    loads = [
        pltpu.make_async_copy(x_in, X.at[pl.ds(0, block)], local_sems.at[0]),
        pltpu.make_async_copy(g_in, G.at[pl.ds(0, block)], local_sems.at[1]),
        pltpu.make_async_copy(wg_in, WT.at[pl.ds(0, hid), own_lanes], local_sems.at[2]),
        pltpu.make_async_copy(wu_in, WT.at[pl.ds(hid, hid), own_lanes], local_sems.at[3]),
        pltpu.make_async_copy(wd_in, WT.at[pl.ds(2 * hid, hid), own_lanes], local_sems.at[4]),
    ]
    for load in loads:
        load.start()

    pl.semaphore_wait(barrier, len(partners))

    half = block // 2
    SELF, LEFT, RIGHT, OPP = 0, 1, 2, 3

    def slot(buf, s, start=0, count=block):
        return buf.at[pl.ds(s * 2 * block + start, count)]

    def forward(buf, s, start=0, count=block):
        landing = (s, block + start, count)
        return send(slot(buf, s, start, count), slot(buf, *landing), sibling), landing

    def forwarded(buf, *states):
        for k, landing in states:
            arrived(k, slot(buf, *landing))

    class Tokens:
        def __init__(self, buf):
            self.buf = buf

        def part(self, s, which):
            return slot(self.buf, s, which * half, half)

        def start_first(self):
            self.r0 = send(self.part(SELF, 0), self.part(LEFT, 0), at_x(1))
            self.l1 = send(self.part(SELF, 1), self.part(RIGHT, 1), at_x(3))

        def start_second(self):
            self.r1 = send(self.part(SELF, 1), self.part(LEFT, 1), at_x(1))
            self.l0 = send(self.part(SELF, 0), self.part(RIGHT, 0), at_x(3))

        def relay(self):
            arrived(self.r0, self.part(LEFT, 0))
            self.r2 = send(self.part(LEFT, 0), self.part(OPP, 0), at_x(1))
            arrived(self.l1, self.part(RIGHT, 1))
            self.l2 = send(self.part(RIGHT, 1), self.part(OPP, 1), at_x(3))

        def near(self):
            arrived(self.r1, self.part(LEFT, 1))
            arrived(self.l0, self.part(RIGHT, 0))
            return forward(self.buf, LEFT), forward(self.buf, RIGHT)

        def far(self):
            arrived(self.r2, self.part(OPP, 0))
            first = forward(self.buf, OPP, 0, half)
            arrived(self.l2, self.part(OPP, 1))
            return first, forward(self.buf, OPP, half, half)

    xt, gt = Tokens(X), Tokens(G)
    loads[0].wait()
    xt.start_first()
    xt.start_second()
    loads[1].wait()
    gt.start_first()
    for load in loads[2:]:
        load.wait()

    direct, spare = 384, 96
    base1, base2 = direct, 2 * hid + spare
    dhalf = direct // 2
    D0, D1 = pl.ds(0, dhalf), pl.ds(dhalf, dhalf)
    D2 = pl.ds(2 * hid, spare)

    def w(rows, step):
        return WT.at[rows, lanes_of(step)]

    def copy_w(rows, step, where):
        return send(w(rows, step), w(rows, step), where)

    class Quarters:
        def __init__(self, base, end):
            self.base, self.part = base, (end - base) // 4
            self.cut = (self.part // 2 + 15) // 16 * 16

        def rows(self, step, which=None):
            start, count = {
                None: (0, self.part), 0: (0, self.cut), 1: (self.cut, self.part - self.cut)
            }[which]
            return pl.ds(pl.multiple_of(self.base + turn(rep, step) * self.part + start, 16), count)

        def start(self):
            self.r, self.l = copy_w(self.rows(0), 0, at_y(1)), copy_w(self.rows(0), 0, at_y(3))
            self.shares = {}

        def relay(self):
            arrived(self.r, w(self.rows(0), 3))
            self.r2 = copy_w(self.rows(0, 0), 3, at_y(1))
            arrived(self.l, w(self.rows(0), 1))
            self.l2 = copy_w(self.rows(0, 1), 1, at_y(3))

        def far(self):
            arrived(self.r2, w(self.rows(0, 0), 2))
            arrived(self.l2, w(self.rows(0, 1), 2))

        def share(self, lane):
            self.shares[lane] = [
                (copy_w(self.rows(0), lane, at_z(step)), 4 - step) for step in (2, 1, 3)
            ]

        def finish(self):
            for lane, keys in self.shares.items():
                for k, step in keys:
                    arrived(k, w(self.rows(step), lane))

    q1, q2 = Quarters(base1, 2 * hid), Quarters(base2, 3 * hid)
    q1.start()
    q2.start()
    d0r = copy_w(D0, 0, at_y(1))
    d1l = copy_w(D1, 0, at_y(3))
    x_own = forward(X, SELF)
    g_own = forward(G, SELF)

    q1.relay()
    q1.share(3)
    q1.share(1)
    q2.relay()
    d1r = copy_w(D1, 0, at_y(1))
    d0l = copy_w(D0, 0, at_y(3))

    xt.relay()
    gt.start_second()
    arrived(d0r, w(D0, 3))
    dc = copy_w(D0, 3, at_y(1))
    arrived(d1l, w(D1, 1))
    dd = copy_w(D1, 1, at_y(3))
    x_near = xt.near()
    q1.far()
    q1.share(2)
    q2.share(3)
    q2.share(1)
    q2.far()
    q2.share(2)
    d2 = [(copy_w(D2, 0, at_y(step)), 4 - step) for step in (2, 1, 3)]
    gt.relay()
    x_far = xt.far()

    forwarded(X, x_own, *x_near)
    arrived(d1r, w(D1, 3))
    arrived(d0l, w(D0, 1))
    q1.finish()
    arrived(dc, w(D0, 2))
    arrived(dd, w(D1, 2))

    rows = hid // 2

    def gate_stage(c):
        cols = pl.ds(c * 256, 256)
        for p in range(2):
            part_rows = pl.ds(p * rows, rows)
            gate = nt(WT[part_rows, :], X[cols, :]).astype(BF16).astype(F32)
            up = nt(WT[pl.ds(hid + p * rows, rows), :], X[cols, :]).astype(BF16).astype(F32)
            sig = jax.nn.sigmoid(gate)
            act = gate * sig
            H[pl.ds(2 * hid + p * rows, rows), cols] = (act * up).astype(BF16)
            ACT[part_rows, cols] = act
            SLOPE[part_rows, cols] = up * sig * (1.0 + gate * (1.0 - sig))

    def grad_stage(c):
        cols = pl.ds(c * 256, 256)
        grad = nt(WT[pl.ds(2 * hid, hid), :], G[cols, :]).astype(BF16).astype(F32)
        H[pl.ds(0, hid), cols] = (grad * SLOPE[:, cols]).astype(BF16)
        H[pl.ds(hid, hid), cols] = (grad * ACT[:, cols]).astype(BF16)

    gate_stage(0)
    g_near = gt.near()
    gate_stage(1)
    forwarded(X, *x_far)
    gate_stage(2)
    q2.finish()
    for k, step in d2:
        arrived(k, w(D2, step))
    forwarded(G, g_own, g_near[0])
    g_far = gt.far()
    grad_stage(0)
    forwarded(G, g_near[1])
    grad_stage(1)
    forwarded(G, *g_far)
    grad_stage(2)

    class Ring:
        def __init__(self, piece, bufs, dest):
            self.piece, self.dest = piece, dest
            self.t0, self.t1, self.fl, self.fr = bufs
            self.h = self.t0.shape[1]

        def side(self, buf, which):
            return buf.at[:, pl.ds(which * self.h, self.h)]

        def start_far(self):
            self.a = send(self.piece(2, 0), self.t0, self.dest(1))
            self.b = send(self.piece(2, 1), self.t1, self.dest(3))

        def start_near(self):
            self.c = send(self.piece(1, 1), self.side(self.fl, 1), self.dest(1))
            self.d = send(self.piece(3, 0), self.side(self.fr, 0), self.dest(3))

        def relay(self):
            arrived(self.a, self.t0)
            self.t0[...] = (self.t0[...].astype(F32) + self.piece(1, 0)[...].astype(F32)).astype(BF16)
            self.e = send(self.t0, self.side(self.fl, 0), self.dest(1))
            arrived(self.b, self.t1)
            self.t1[...] = (self.t1[...].astype(F32) + self.piece(3, 1)[...].astype(F32)).astype(BF16)
            self.f = send(self.t1, self.side(self.fr, 1), self.dest(3))

        def finish(self, store):
            arrived(self.c, self.side(self.fl, 1))
            arrived(self.d, self.side(self.fr, 0))
            arrived(self.e, self.side(self.fl, 0))
            arrived(self.f, self.side(self.fr, 1))
            for which in range(2):
                total = (
                    self.piece(0, which)[...].astype(F32)
                    + self.side(self.fl, which)[...].astype(F32)
                    + self.side(self.fr, which)[...].astype(F32)
                )
                store(which, total.astype(BF16))

    def y_piece(buf, start, count):
        def piece(step, which):
            lane = pl.multiple_of(turn(fs, step) * shard + which * (shard // 2), 128)
            return buf.at[pl.ds(start, count), pl.ds(lane, shard // 2)]
        return piece

    def z_piece(buf, start, count, lanes):
        def piece(step, which):
            row = pl.multiple_of(start + turn(rep, step) * count, 16)
            return buf.at[pl.ds(row, count), pl.ds(which * lanes, lanes)]
        return piece

    def x_piece(step, which):
        s = {0: SELF, 1: RIGHT, 3: LEFT, 2: OPP}[step]
        return GX.at[pl.ds(s * block, block), pl.ds(which * (width // 2), width // 2)]

    def strip(buf, count):
        def piece(step):
            row = pl.multiple_of(turn(rep, step) * (count // 4), 16)
            return buf.at[pl.ds(row, count // 4)]
        return piece

    def column(buf):
        def piece(step):
            return buf.at[:, lanes_of(step)]
        return piece

    class Exchange:
        def __init__(self, piece, bufs, dest):
            self.piece, self.bufs, self.dest = piece, bufs, dest

        def start(self):
            self.keys = [
                (send(self.piece(step), self.bufs[step - 1], self.dest(step)), self.bufs[step - 1])
                for step in (2, 1, 3)
            ]

        def finish(self, start):
            for k, landing in self.keys:
                arrived(k, landing)
            total = self.piece(0)[...].astype(F32)
            for buf in self.bufs:
                total = total + buf[...].astype(F32)
            OUTT[pl.ds(start, total.shape[0]), :] = total.astype(BF16)

    class Gather:
        def __init__(self, base, count):
            self.base, self.count = base, count // 4

        def row(self, step):
            return pl.multiple_of(self.base + turn(rep, step) * self.count, 16)

        def region(self, step):
            return OUTT.at[pl.ds(self.row(step), self.count)]

        def start(self):
            self.keys = [
                (send(self.region(0), self.region(0), at_z(step)), 4 - step) for step in (2, 1, 3)
            ]

        def finish(self):
            for k, step in self.keys:
                arrived(k, self.region(step))

    A, B = SPLIT
    a_at = [sum(A[:i]) for i in range(len(A))]
    b_at = [sum(A) + sum(B[:i]) for i in range(len(B))]
    ya = [Ring(y_piece(PW, r, n), bufs, at_y) for r, n, bufs in zip(a_at, A, YA_BUFS)]
    zb = [Ring(z_piece(PW, r, n // 4, width // 2), bufs, at_z) for r, n, bufs in zip(b_at, B, ZB_BUFS)]
    za = [Exchange(strip(buf, n), bufs, at_z) for buf, n, bufs in zip(YA, A, ZA_BUFS)]
    yb = [Exchange(column(buf), bufs, at_y) for buf, bufs in zip(ZB, YB_BUFS)]
    ga = [Gather(r, n) for r, n in zip(a_at, A)]
    gb = [Gather(r, n) for r, n in zip(b_at, B)]
    xr = Ring(x_piece, XR_BUFS, at_x)

    def keep(buf):
        def store(which, value):
            h = value.shape[1]
            buf[:, pl.ds(which * h, h)] = value
        return store

    def weight_piece(step, start, count):
        lanes = lanes_of(step)
        PW[pl.ds(start, count), lanes] = (
            factor * nn(H[pl.ds(start, count), :], X[:, lanes])
        ).astype(BF16)

    def weight_rows(start, count):
        for lo, hi, tokens in ((start, min(start + count, 2 * hid), X), (max(start, 2 * hid), min(start + count, 3 * hid), G)):
            if lo < hi:
                for n in range(4):
                    PW[pl.ds(lo, hi - lo), pl.ds(n * 256, 256)] = (
                        factor * nn(H[pl.ds(lo, hi - lo), :], tokens[:, pl.ds(n * 256, 256)])
                    ).astype(BF16)

    def input_piece(c):
        DX[pl.ds(c * 256, 256), :] = tn(
            H[pl.ds(0, 2 * hid), pl.ds(c * 256, 256)], WT[pl.ds(0, 2 * hid), :]
        ).astype(BF16)

    def across(s):
        landing = DS.at[pl.ds(s * block, block)]
        return send(slot(DX, s, block), landing, sibling)

    def across_add(k, s):
        arrived(k, DS.at[pl.ds(s * block, block)])
        GX[pl.ds(s * block, block), :] = (
            DX[pl.ds(s * 2 * block, block), :].astype(F32)
            + DS[pl.ds(s * block, block), :].astype(F32)
        ).astype(BF16)

    blank = PW.shape[0] - 3 * hid
    PW[pl.ds(3 * hid, blank), :] = jnp.zeros((blank, width), BF16)
    weight_piece(2, 0, A[0])
    ya[0].start_far()
    weight_rows(b_at[0], B[0])
    zb[0].start_far()
    weight_piece(1, 0, A[0])
    weight_piece(3, 0, A[0])
    ya[0].start_near()
    weight_rows(a_at[1], A[1])
    zb[0].start_near()
    weight_rows(b_at[1], B[1])
    ya[1].start_far()
    weight_rows(a_at[2], A[2])
    zb[1].start_far()
    weight_rows(b_at[2], B[2])
    input_piece(2)
    opp = across(OPP)
    ya[1].start_near()
    zb[1].start_near()
    input_piece(1)
    near = across(LEFT), across(RIGHT)
    ya[0].relay()
    input_piece(0)
    mine = across(SELF)
    zb[0].relay()
    weight_piece(0, 0, A[0])
    across_add(opp, OPP)
    xr.start_far()
    zb[2].start_far()
    ya[2].start_far()
    across_add(near[0], LEFT)
    across_add(near[1], RIGHT)
    xr.start_near()
    ya[1].relay()
    zb[1].relay()
    across_add(mine, SELF)
    zb[2].start_near()
    zb[0].finish(keep(ZB[0]))
    yb[0].start()
    ya[0].finish(keep(YA[0]))
    za[0].start()
    ya[2].start_near()
    zb[2].relay()
    ya[2].relay()
    xr.relay()
    zb[1].finish(keep(ZB[1]))
    yb[1].start()
    ya[1].finish(keep(YA[1]))
    za[1].start()
    yb[0].finish(gb[0].row(0))
    gb[0].start()
    za[0].finish(ga[0].row(0))
    ga[0].start()
    zb[2].finish(keep(ZB[2]))
    yb[2].start()
    ya[2].finish(keep(YA[2]))
    za[2].start()
    xr.finish(keep(gin_out))
    yb[1].finish(gb[1].row(0))
    gb[1].start()
    za[1].finish(ga[1].row(0))
    ga[1].start()
    gb[0].finish()
    ga[0].finish()
    yb[2].finish(gb[2].row(0))
    gb[2].start()
    za[2].finish(ga[2].row(0))
    ga[2].start()
    gb[1].finish()
    ga[1].finish()
    gb[2].finish()
    og_out[...] = OUTT[pl.ds(0, hid), :].astype(F32)
    od_out[...] = OUTT[pl.ds(2 * hid, hid), :].astype(F32)
    for copy in pending[:-3]:
        copy.wait_send()
    ga[2].finish()
    ou_out[...] = OUTT[pl.ds(hid, hid), :].astype(F32)
    for copy in pending[-3:]:
        copy.wait_send()


def writer(*refs):
    sources, targets, sems = refs[:4], refs[4:8], refs[8]
    copies = [pltpu.make_async_copy(a, b, sems.at[i]) for i, (a, b) in enumerate(zip(sources, targets))]
    for copy in copies:
        copy.start()
    for copy in copies:
        copy.wait()


def body(tokens_in, out_grad, gate_weight, up_weight, down_weight):
    block, width = tokens_in.shape
    shard, hid = gate_weight.shape
    devices = lax.axis_size("rep") * lax.axis_size("fs") * lax.axis_size("tp")
    factor = (block * devices) ** (-0.5)
    tokens = block * 8
    A, B = SPLIT
    total_rows = sum(A) + sum(B)

    def ring(count, lanes):
        return [
            pltpu.VMEM((count, lanes // 2), BF16),
            pltpu.VMEM((count, lanes // 2), BF16),
            pltpu.VMEM((count, lanes), BF16),
            pltpu.VMEM((count, lanes), BF16),
        ]

    def exchange(count):
        return [pltpu.VMEM((count // 4, shard), BF16)] * 3

    outs = (
        jax.ShapeDtypeStruct((block, width), BF16),
        jax.ShapeDtypeStruct((hid, shard), F32),
        jax.ShapeDtypeStruct((hid, shard), F32),
        jax.ShapeDtypeStruct((hid, shard), F32),
    )
    arrays = tokens_in, out_grad, gate_weight.T, up_weight.T, down_weight
    results = pl.pallas_call(
        functools.partial(kernel, factor, block, width, hid),
        out_shape=outs,
        in_specs=[pl.BlockSpec(memory_space=pltpu.HBM)] * 5,
        out_specs=[pl.BlockSpec(memory_space=pltpu.VMEM)] * 4,
        scratch_shapes=[
            pltpu.VMEM((tokens, width), BF16),
            pltpu.VMEM((tokens, width), BF16),
            pltpu.VMEM((3 * hid, width), BF16),
            pltpu.VMEM((3 * hid, tokens), BF16),
            pltpu.VMEM((hid, tokens), F32),
            pltpu.VMEM((hid, tokens), F32),
            pltpu.VMEM((total_rows, width), BF16),
            pltpu.VMEM((tokens, width), BF16),
            pltpu.VMEM((tokens // 2, width), BF16),
            pltpu.VMEM((tokens // 2, width), BF16),
            [pltpu.VMEM((n, shard), BF16) for n in A],
            [pltpu.VMEM((n // 4, width), BF16) for n in B],
            pltpu.VMEM((total_rows, shard), BF16),
            [ring(n, shard) for n in A],
            [ring(n // 4, width) for n in B],
            [exchange(n) for n in A],
            [exchange(n) for n in B],
            ring(block, width),
            pltpu.SemaphoreType.DMA((COPIES,)),
            pltpu.SemaphoreType.DMA((COPIES,)),
            pltpu.SemaphoreType.DMA((5,)),
        ],
        compiler_params=pltpu.CompilerParams(
            collective_id=0, has_side_effects=True, vmem_limit_bytes=48 * 1024 * 1024
        ),
    )(*[pltpu.with_memory_space_constraint(a, pltpu.HBM) for a in arrays])
    grad_in, gate_t, up_t, down_t = pl.pallas_call(
        writer,
        out_shape=outs,
        in_specs=[pl.BlockSpec(memory_space=pl.ANY)] * 4,
        out_specs=[pl.BlockSpec(memory_space=pltpu.HBM)] * 4,
        scratch_shapes=[pltpu.SemaphoreType.DMA((4,))],
        compiler_params=pltpu.CompilerParams(vmem_limit_bytes=1024 * 1024),
    )(*results)
    return grad_in, gate_t.T, up_t.T, down_t


def solution(mesh):
    return jax.shard_map(
        body,
        mesh=mesh,
        in_specs=(
            P(("rep", "fs", "tp"), None),
            P(("rep", "fs", "tp"), None),
            P("fs", "tp"),
            P("fs", "tp"),
            P("tp", "fs"),
        ),
        out_specs=(P(("rep", "fs", "tp"), None), P("fs", "tp"), P("fs", "tp"), P("tp", "fs")),
        check_vma=False,
    )
```

```python
import functools

import jax
import jax.numpy as jnp
from jax import lax
from jax.experimental import pallas as pl
from jax.experimental.pallas import tpu as pltpu
from jax.sharding import PartitionSpec as P

BF16 = jnp.bfloat16
F32 = jnp.float32
MESH = pl.DeviceIdType.MESH
COPIES = 144
SPLIT = (128, 256, 192), (128, 192, 192)


def nt(left, right):
    return lax.dot_general(left, right, (((1,), (1,)), ((), ())), preferred_element_type=F32)


def tn(left, right):
    return lax.dot_general(left, right, (((0,), (0,)), ((), ())), preferred_element_type=F32)


def nn(left, right):
    return lax.dot_general(left, right, (((1,), (0,)), ((), ())), preferred_element_type=F32)


def kernel(
    factor, block, width, hid,
    x_in, g_in, wg_in, wu_in, wd_in,
    gin_out, og_out, ou_out, od_out,
    X, G, WT, H, ACT, SLOPE, PW, DX, DS, GX, YA, ZB, OUTT, YA_BUFS, ZB_BUFS, ZA_BUFS, YB_BUFS, XR_BUFS,
    send_sems, recv_sems, local_sems,
):
    rep = lax.axis_index("rep")
    fs = lax.axis_index("fs")
    tp = lax.axis_index("tp")
    core = lax.rem(tp, 2)
    xpos = tp // 2
    shard = width // 4

    def turn(pos, step):
        return lax.rem(pos + step, 4)

    def at_x(step):
        return {"tp": turn(xpos, step) * 2 + core}

    def at_y(step):
        return {"fs": turn(fs, step)}

    def at_z(step):
        return {"rep": turn(rep, step)}

    sibling = {"tp": tp + 1 - 2 * core}

    def lanes_of(step):
        return pl.ds(pl.multiple_of(turn(fs, step) * shard, shard), shard)

    counter = [0]
    pending = []

    def remote(src, dst, k, where):
        return pltpu.make_async_remote_copy(
            src_ref=src, dst_ref=dst, send_sem=send_sems.at[k], recv_sem=recv_sems.at[k],
            device_id=where, device_id_type=MESH,
        )

    def send(src, dst, where):
        k = counter[0]
        counter[0] += 1
        copy = remote(src, dst, k, where)
        copy.start()
        pending.append(copy)
        return k

    def arrived(k, landing):
        remote(landing, landing, k, sibling).wait_recv()

    barrier = pltpu.get_barrier_semaphore()
    partners = [sibling] + [at(step) for at in (at_x, at_y, at_z) for step in (1, 3)]
    partners += [at_y(2), at_z(2)]
    for where in partners:
        pl.semaphore_signal(barrier, inc=1, device_id=where, device_id_type=MESH)

    own_lanes = lanes_of(0)
    loads = [
        pltpu.make_async_copy(x_in, X.at[pl.ds(0, block)], local_sems.at[0]),
        pltpu.make_async_copy(g_in, G.at[pl.ds(0, block)], local_sems.at[1]),
        pltpu.make_async_copy(wg_in, WT.at[pl.ds(0, hid), own_lanes], local_sems.at[2]),
        pltpu.make_async_copy(wu_in, WT.at[pl.ds(hid, hid), own_lanes], local_sems.at[3]),
        pltpu.make_async_copy(wd_in, WT.at[pl.ds(2 * hid, hid), own_lanes], local_sems.at[4]),
    ]
    for load in loads:
        load.start()

    pl.semaphore_wait(barrier, len(partners))

    half = block // 2
    SELF, LEFT, RIGHT, OPP = 0, 1, 2, 3

    def slot(buf, s, start=0, count=block):
        return buf.at[pl.ds(s * 2 * block + start, count)]

    def forward(buf, s, start=0, count=block):
        landing = (s, block + start, count)
        return send(slot(buf, s, start, count), slot(buf, *landing), sibling), landing

    def forwarded(buf, *states):
        for k, landing in states:
            arrived(k, slot(buf, *landing))

    class Tokens:
        def __init__(self, buf):
            self.buf = buf

        def part(self, s, which):
            return slot(self.buf, s, which * half, half)

        def start_first(self):
            self.r0 = send(self.part(SELF, 0), self.part(LEFT, 0), at_x(1))
            self.l1 = send(self.part(SELF, 1), self.part(RIGHT, 1), at_x(3))

        def start_second(self):
            self.r1 = send(self.part(SELF, 1), self.part(LEFT, 1), at_x(1))
            self.l0 = send(self.part(SELF, 0), self.part(RIGHT, 0), at_x(3))

        def relay(self):
            arrived(self.r0, self.part(LEFT, 0))
            self.r2 = send(self.part(LEFT, 0), self.part(OPP, 0), at_x(1))
            arrived(self.l1, self.part(RIGHT, 1))
            self.l2 = send(self.part(RIGHT, 1), self.part(OPP, 1), at_x(3))

        def near(self):
            arrived(self.r1, self.part(LEFT, 1))
            arrived(self.l0, self.part(RIGHT, 0))
            return forward(self.buf, LEFT), forward(self.buf, RIGHT)

        def far(self):
            arrived(self.r2, self.part(OPP, 0))
            first = forward(self.buf, OPP, 0, half)
            arrived(self.l2, self.part(OPP, 1))
            return first, forward(self.buf, OPP, half, half)

    xt, gt = Tokens(X), Tokens(G)
    loads[0].wait()
    xt.start_first()
    xt.start_second()
    loads[1].wait()
    gt.start_first()
    for load in loads[2:]:
        load.wait()

    direct, spare = 384, 96
    base1, base2 = direct, 2 * hid + spare
    dhalf = direct // 2
    D0, D1 = pl.ds(0, dhalf), pl.ds(dhalf, dhalf)
    D2 = pl.ds(2 * hid, spare)

    def w(rows, step):
        return WT.at[rows, lanes_of(step)]

    def copy_w(rows, step, where):
        return send(w(rows, step), w(rows, step), where)

    class Quarters:
        def __init__(self, base, end):
            self.base, self.part = base, (end - base) // 4
            self.cut = (self.part // 2 + 15) // 16 * 16

        def rows(self, step, which=None):
            start, count = {
                None: (0, self.part), 0: (0, self.cut), 1: (self.cut, self.part - self.cut)
            }[which]
            return pl.ds(pl.multiple_of(self.base + turn(rep, step) * self.part + start, 16), count)

        def start(self):
            self.r, self.l = copy_w(self.rows(0), 0, at_y(1)), copy_w(self.rows(0), 0, at_y(3))
            self.shares = {}

        def relay(self):
            arrived(self.r, w(self.rows(0), 3))
            self.r2 = copy_w(self.rows(0, 0), 3, at_y(1))
            arrived(self.l, w(self.rows(0), 1))
            self.l2 = copy_w(self.rows(0, 1), 1, at_y(3))

        def far(self):
            arrived(self.r2, w(self.rows(0, 0), 2))
            arrived(self.l2, w(self.rows(0, 1), 2))

        def share(self, lane):
            self.shares[lane] = [
                (copy_w(self.rows(0), lane, at_z(step)), 4 - step) for step in (2, 1, 3)
            ]

        def finish(self):
            for lane, keys in self.shares.items():
                for k, step in keys:
                    arrived(k, w(self.rows(step), lane))

    q1, q2 = Quarters(base1, 2 * hid), Quarters(base2, 3 * hid)
    q1.start()
    q2.start()
    d0r = copy_w(D0, 0, at_y(1))
    d1l = copy_w(D1, 0, at_y(3))
    x_own = forward(X, SELF)
    g_own = forward(G, SELF)

    q1.relay()
    q1.share(3)
    q1.share(1)
    q2.relay()
    d1r = copy_w(D1, 0, at_y(1))
    d0l = copy_w(D0, 0, at_y(3))

    xt.relay()
    gt.start_second()
    arrived(d0r, w(D0, 3))
    dc = copy_w(D0, 3, at_y(1))
    arrived(d1l, w(D1, 1))
    dd = copy_w(D1, 1, at_y(3))
    x_near = xt.near()
    q1.far()
    q1.share(2)
    q2.share(3)
    q2.share(1)
    q2.far()
    q2.share(2)
    d2 = [(copy_w(D2, 0, at_y(step)), 4 - step) for step in (2, 1, 3)]
    gt.relay()
    x_far = xt.far()

    forwarded(X, x_own, *x_near)
    arrived(d1r, w(D1, 3))
    arrived(d0l, w(D0, 1))
    q1.finish()
    arrived(dc, w(D0, 2))
    arrived(dd, w(D1, 2))

    rows = hid // 2

    def gate_stage(c):
        cols = pl.ds(c * 256, 256)
        for p in range(2):
            part_rows = pl.ds(p * rows, rows)
            gate = nt(WT[part_rows, :], X[cols, :]).astype(BF16).astype(F32)
            up = nt(WT[pl.ds(hid + p * rows, rows), :], X[cols, :]).astype(BF16).astype(F32)
            sig = jax.nn.sigmoid(gate)
            act = gate * sig
            H[pl.ds(2 * hid + p * rows, rows), cols] = (act * up).astype(BF16)
            ACT[part_rows, cols] = act
            SLOPE[part_rows, cols] = up * sig * (1.0 + gate * (1.0 - sig))

    def grad_stage(c):
        cols = pl.ds(c * 256, 256)
        grad = nt(WT[pl.ds(2 * hid, hid), :], G[cols, :]).astype(BF16).astype(F32)
        H[pl.ds(0, hid), cols] = (grad * SLOPE[:, cols]).astype(BF16)
        H[pl.ds(hid, hid), cols] = (grad * ACT[:, cols]).astype(BF16)

    gate_stage(0)
    gate_stage(1)
    g_near = gt.near()
    forwarded(X, *x_far)
    gate_stage(2)
    q2.finish()
    for k, step in d2:
        arrived(k, w(D2, step))
    forwarded(G, g_own, g_near[0])
    grad_stage(0)
    g_far = gt.far()
    forwarded(G, g_near[1])
    grad_stage(1)
    forwarded(G, *g_far)
    grad_stage(2)

    class Ring:
        def __init__(self, piece, bufs, dest):
            self.piece, self.dest = piece, dest
            self.t0, self.t1, self.fl, self.fr = bufs
            self.h = self.t0.shape[1]

        def side(self, buf, which):
            return buf.at[:, pl.ds(which * self.h, self.h)]

        def start_far(self):
            self.a = send(self.piece(2, 0), self.t0, self.dest(1))
            self.b = send(self.piece(2, 1), self.t1, self.dest(3))

        def start_near(self):
            self.c = send(self.piece(1, 1), self.side(self.fl, 1), self.dest(1))
            self.d = send(self.piece(3, 0), self.side(self.fr, 0), self.dest(3))

        def relay(self):
            arrived(self.a, self.t0)
            self.t0[...] = (self.t0[...].astype(F32) + self.piece(1, 0)[...].astype(F32)).astype(BF16)
            self.e = send(self.t0, self.side(self.fl, 0), self.dest(1))
            arrived(self.b, self.t1)
            self.t1[...] = (self.t1[...].astype(F32) + self.piece(3, 1)[...].astype(F32)).astype(BF16)
            self.f = send(self.t1, self.side(self.fr, 1), self.dest(3))

        def finish(self, store):
            arrived(self.c, self.side(self.fl, 1))
            arrived(self.d, self.side(self.fr, 0))
            arrived(self.e, self.side(self.fl, 0))
            arrived(self.f, self.side(self.fr, 1))
            for which in range(2):
                total = (
                    self.piece(0, which)[...].astype(F32)
                    + self.side(self.fl, which)[...].astype(F32)
                    + self.side(self.fr, which)[...].astype(F32)
                )
                store(which, total.astype(BF16))

    def y_piece(buf, start, count):
        def piece(step, which):
            lane = pl.multiple_of(turn(fs, step) * shard + which * (shard // 2), 128)
            return buf.at[pl.ds(start, count), pl.ds(lane, shard // 2)]
        return piece

    def z_piece(buf, start, count, lanes):
        def piece(step, which):
            row = pl.multiple_of(start + turn(rep, step) * count, 16)
            return buf.at[pl.ds(row, count), pl.ds(which * lanes, lanes)]
        return piece

    def x_piece(step, which):
        s = {0: SELF, 1: RIGHT, 3: LEFT, 2: OPP}[step]
        return GX.at[pl.ds(s * block, block), pl.ds(which * (width // 2), width // 2)]

    def strip(buf, count):
        def piece(step):
            row = pl.multiple_of(turn(rep, step) * (count // 4), 16)
            return buf.at[pl.ds(row, count // 4)]
        return piece

    def column(buf):
        def piece(step):
            return buf.at[:, lanes_of(step)]
        return piece

    class Exchange:
        def __init__(self, piece, bufs, dest):
            self.piece, self.bufs, self.dest = piece, bufs, dest

        def start(self):
            self.keys = [
                (send(self.piece(step), self.bufs[step - 1], self.dest(step)), self.bufs[step - 1])
                for step in (2, 1, 3)
            ]

        def finish(self, start):
            for k, landing in self.keys:
                arrived(k, landing)
            total = self.piece(0)[...].astype(F32)
            for buf in self.bufs:
                total = total + buf[...].astype(F32)
            OUTT[pl.ds(start, total.shape[0]), :] = total.astype(BF16)

    class Gather:
        def __init__(self, base, count):
            self.base, self.count = base, count // 4

        def row(self, step):
            return pl.multiple_of(self.base + turn(rep, step) * self.count, 16)

        def region(self, step):
            return OUTT.at[pl.ds(self.row(step), self.count)]

        def start(self):
            self.keys = [
                (send(self.region(0), self.region(0), at_z(step)), 4 - step) for step in (2, 1, 3)
            ]

        def finish(self):
            for k, step in self.keys:
                arrived(k, self.region(step))

    A, B = SPLIT
    a_at = [sum(A[:i]) for i in range(len(A))]
    b_at = [sum(A) + sum(B[:i]) for i in range(len(B))]
    ya = [Ring(y_piece(PW, r, n), bufs, at_y) for r, n, bufs in zip(a_at, A, YA_BUFS)]
    zb = [Ring(z_piece(PW, r, n // 4, width // 2), bufs, at_z) for r, n, bufs in zip(b_at, B, ZB_BUFS)]
    za = [Exchange(strip(buf, n), bufs, at_z) for buf, n, bufs in zip(YA, A, ZA_BUFS)]
    yb = [Exchange(column(buf), bufs, at_y) for buf, bufs in zip(ZB, YB_BUFS)]
    ga = [Gather(r, n) for r, n in zip(a_at, A)]
    gb = [Gather(r, n) for r, n in zip(b_at, B)]
    xr = Ring(x_piece, XR_BUFS, at_x)

    def keep(buf):
        def store(which, value):
            h = value.shape[1]
            buf[:, pl.ds(which * h, h)] = value
        return store

    def weight_piece(step, start, count):
        lanes = lanes_of(step)
        PW[pl.ds(start, count), lanes] = (
            factor * nn(H[pl.ds(start, count), :], X[:, lanes])
        ).astype(BF16)

    def weight_rows(start, count):
        for lo, hi, tokens in ((start, min(start + count, 2 * hid), X), (max(start, 2 * hid), min(start + count, 3 * hid), G)):
            if lo < hi:
                for n in range(4):
                    PW[pl.ds(lo, hi - lo), pl.ds(n * 256, 256)] = (
                        factor * nn(H[pl.ds(lo, hi - lo), :], tokens[:, pl.ds(n * 256, 256)])
                    ).astype(BF16)

    def input_piece(c):
        DX[pl.ds(c * 256, 256), :] = tn(
            H[pl.ds(0, 2 * hid), pl.ds(c * 256, 256)], WT[pl.ds(0, 2 * hid), :]
        ).astype(BF16)

    def across(s):
        landing = DS.at[pl.ds(s * block, block)]
        return send(slot(DX, s, block), landing, sibling)

    def across_add(k, s):
        arrived(k, DS.at[pl.ds(s * block, block)])
        GX[pl.ds(s * block, block), :] = (
            DX[pl.ds(s * 2 * block, block), :].astype(F32)
            + DS[pl.ds(s * block, block), :].astype(F32)
        ).astype(BF16)

    blank = PW.shape[0] - 3 * hid
    PW[pl.ds(3 * hid, blank), :] = jnp.zeros((blank, width), BF16)
    weight_piece(2, 0, A[0])
    ya[0].start_far()
    weight_rows(b_at[0], B[0])
    zb[0].start_far()
    weight_piece(1, 0, A[0])
    weight_piece(3, 0, A[0])
    ya[0].start_near()
    weight_rows(a_at[1], A[1])
    zb[0].start_near()
    weight_rows(b_at[1], B[1])
    ya[1].start_far()
    weight_rows(a_at[2], A[2])
    zb[1].start_far()
    weight_rows(b_at[2], B[2])
    input_piece(2)
    opp = across(OPP)
    ya[1].start_near()
    zb[1].start_near()
    input_piece(1)
    near = across(LEFT), across(RIGHT)
    ya[0].relay()
    input_piece(0)
    mine = across(SELF)
    zb[0].relay()
    weight_piece(0, 0, A[0])
    across_add(opp, OPP)
    xr.start_far()
    zb[2].start_far()
    ya[2].start_far()
    across_add(near[0], LEFT)
    across_add(near[1], RIGHT)
    xr.start_near()
    ya[1].relay()
    zb[1].relay()
    across_add(mine, SELF)
    zb[2].start_near()
    zb[0].finish(keep(ZB[0]))
    yb[0].start()
    ya[0].finish(keep(YA[0]))
    za[0].start()
    ya[2].start_near()
    zb[2].relay()
    ya[2].relay()
    xr.relay()
    zb[1].finish(keep(ZB[1]))
    yb[1].start()
    ya[1].finish(keep(YA[1]))
    za[1].start()
    yb[0].finish(gb[0].row(0))
    gb[0].start()
    za[0].finish(ga[0].row(0))
    ga[0].start()
    zb[2].finish(keep(ZB[2]))
    yb[2].start()
    ya[2].finish(keep(YA[2]))
    za[2].start()
    xr.finish(keep(gin_out))
    yb[1].finish(gb[1].row(0))
    gb[1].start()
    za[1].finish(ga[1].row(0))
    ga[1].start()
    gb[0].finish()
    ga[0].finish()
    yb[2].finish(gb[2].row(0))
    gb[2].start()
    za[2].finish(ga[2].row(0))
    ga[2].start()
    gb[1].finish()
    ga[1].finish()
    gb[2].finish()
    og_out[...] = OUTT[pl.ds(0, hid), :].astype(F32)
    od_out[...] = OUTT[pl.ds(2 * hid, hid), :].astype(F32)
    for copy in pending[:-3]:
        copy.wait_send()
    ga[2].finish()
    ou_out[...] = OUTT[pl.ds(hid, hid), :].astype(F32)
    for copy in pending[-3:]:
        copy.wait_send()


def writer(*refs):
    sources, targets, sems = refs[:4], refs[4:8], refs[8]
    copies = [pltpu.make_async_copy(a, b, sems.at[i]) for i, (a, b) in enumerate(zip(sources, targets))]
    for copy in copies:
        copy.start()
    for copy in copies:
        copy.wait()


def body(tokens_in, out_grad, gate_weight, up_weight, down_weight):
    block, width = tokens_in.shape
    shard, hid = gate_weight.shape
    devices = lax.axis_size("rep") * lax.axis_size("fs") * lax.axis_size("tp")
    factor = (block * devices) ** (-0.5)
    tokens = block * 8
    A, B = SPLIT
    total_rows = sum(A) + sum(B)

    def ring(count, lanes):
        return [
            pltpu.VMEM((count, lanes // 2), BF16),
            pltpu.VMEM((count, lanes // 2), BF16),
            pltpu.VMEM((count, lanes), BF16),
            pltpu.VMEM((count, lanes), BF16),
        ]

    def exchange(count):
        return [pltpu.VMEM((count // 4, shard), BF16)] * 3

    outs = (
        jax.ShapeDtypeStruct((block, width), BF16),
        jax.ShapeDtypeStruct((hid, shard), F32),
        jax.ShapeDtypeStruct((hid, shard), F32),
        jax.ShapeDtypeStruct((hid, shard), F32),
    )
    arrays = tokens_in, out_grad, gate_weight.T, up_weight.T, down_weight
    results = pl.pallas_call(
        functools.partial(kernel, factor, block, width, hid),
        out_shape=outs,
        in_specs=[pl.BlockSpec(memory_space=pltpu.HBM)] * 5,
        out_specs=[pl.BlockSpec(memory_space=pltpu.VMEM)] * 4,
        scratch_shapes=[
            pltpu.VMEM((tokens, width), BF16),
            pltpu.VMEM((tokens, width), BF16),
            pltpu.VMEM((3 * hid, width), BF16),
            pltpu.VMEM((3 * hid, tokens), BF16),
            pltpu.VMEM((hid, tokens), F32),
            pltpu.VMEM((hid, tokens), F32),
            pltpu.VMEM((total_rows, width), BF16),
            pltpu.VMEM((tokens, width), BF16),
            pltpu.VMEM((tokens // 2, width), BF16),
            pltpu.VMEM((tokens // 2, width), BF16),
            [pltpu.VMEM((n, shard), BF16) for n in A],
            [pltpu.VMEM((n // 4, width), BF16) for n in B],
            pltpu.VMEM((total_rows, shard), BF16),
            [ring(n, shard) for n in A],
            [ring(n // 4, width) for n in B],
            [exchange(n) for n in A],
            [exchange(n) for n in B],
            ring(block, width),
            pltpu.SemaphoreType.DMA((COPIES,)),
            pltpu.SemaphoreType.DMA((COPIES,)),
            pltpu.SemaphoreType.DMA((5,)),
        ],
        compiler_params=pltpu.CompilerParams(
            collective_id=0, has_side_effects=True, vmem_limit_bytes=48 * 1024 * 1024
        ),
    )(*[pltpu.with_memory_space_constraint(a, pltpu.HBM) for a in arrays])
    grad_in, gate_t, up_t, down_t = pl.pallas_call(
        writer,
        out_shape=outs,
        in_specs=[pl.BlockSpec(memory_space=pl.ANY)] * 4,
        out_specs=[pl.BlockSpec(memory_space=pltpu.HBM)] * 4,
        scratch_shapes=[pltpu.SemaphoreType.DMA((4,))],
        compiler_params=pltpu.CompilerParams(vmem_limit_bytes=1024 * 1024),
    )(*results)
    return grad_in, gate_t.T, up_t.T, down_t


def solution(mesh):
    return jax.shard_map(
        body,
        mesh=mesh,
        in_specs=(
            P(("rep", "fs", "tp"), None),
            P(("rep", "fs", "tp"), None),
            P("fs", "tp"),
            P("fs", "tp"),
            P("tp", "fs"),
        ),
        out_specs=(P(("rep", "fs", "tp"), None), P("fs", "tp"), P("fs", "tp"), P("tp", "fs")),
        check_vma=False,
    )
```
